256 devices in a mesh: sp: 32 (over z, y), tp: 8 (over x, core).
Axes of the slice: x: 4, y: 4, z: 8, core: 2. Of those that a mesh axis runs over, the one named last changes fastest.
Arguments:
- latent: bfloat16 [8192, 2048], P('sp'), may hold values from -6 to 6
- context: bfloat16 [1024, 2048], P('sp'), may hold values from -6 to 6
- condition: bfloat16 [2048], replicated, may hold values from -6 to 6
- context_condition: bfloat16 [2048], replicated, may hold values from -6 to 6
- gain_pre: float32 [2048], replicated, may hold values from 0.1 to 1.9
- gain_post: float32 [2048], replicated, may hold values from 0.1 to 1.9
- w_shift: bfloat16 [2048, 2048], P('sp', 'tp'), may hold values from -0.125 to 0.125
- w_scale: bfloat16 [2048, 2048], P('sp', 'tp'), may hold values from -0.125 to 0.125
- w_gate: bfloat16 [2048, 2048], P('sp', 'tp'), may hold values from -0.125 to 0.125
- w_query: bfloat16 [2048, 2048], P(None, 'tp'), may hold values from -0.13258252 to 0.13258252
- w_key: bfloat16 [2048, 2048], P(None, 'tp'), may hold values from -6.629126 to 6.629126
- w_value: bfloat16 [2048, 2048], P(None, 'tp'), may hold values from -0.125 to 0.125
- w_silu: bfloat16 [2048, 2048], P(None, 'tp'), may hold values from -0.125 to 0.125
- offset_bias: float32 [32, 15, 31], P('tp'), may hold values from 1.5 to 3.5
- w_out: bfloat16 [2048, 2048], P('tp'), may hold values from -0.125 to 0.125
Outputs:
- updated: bfloat16 [8192, 2048], P(('sp', 'tp'))
The draws below stay inside these ranges and needn't reach their ends.
All inputs are finite; a program needn't handle non-finite values.
Results may differ from the reference program's by a relative error of at most 0.01.
Values may be sent and summed in bfloat16 or wider, within the bound.
A program may use at most 64 MiB of HBM per device.

```python
import jax
import jax.numpy as jnp
from jax import lax

D = 2048
HEADS = 32
HEAD_DIM = 64
GRID_W = 64
WIN_ROWS = 8
WIN_COLS = 16
CTX = 1024
TOKENS = 8192
N_TP = 8


def query_key_pair(key):
    base = jax.random.fold_in(key, 7)
    first, second, third = jax.random.split(base, 3)
    spread = D ** (-0.5)
    weight_query = jnp.clip(jax.random.normal(first, (D, D), jnp.float32), -6.0, 6.0) * spread
    weight_key = jnp.clip(jax.random.normal(second, (D, D), jnp.float32), -6.0, 6.0) * spread
    return (weight_query, weight_key)


def draw_w_query(key, part):
    return query_key_pair(key)[0].astype(jnp.bfloat16)


def draw_w_key(key, part):
    return query_key_pair(key)[1].astype(jnp.bfloat16)


def steps_of(key, dims, pieces, smallest, high):
    def one(dim, shards_of):
        steps = jax.random.uniform(jax.random.fold_in(jax.random.fold_in(key, 6), dim), (shards_of,), jnp.float32, smallest / len(pieces), high / len(pieces))
        return jnp.repeat(jnp.exp(steps), dims[dim] // shards_of).reshape((-1,) + (1,) * (len(dims) - dim - 1))

    factor_of = one(*pieces[0])
    for cut in pieces[1:]:
        factor_of = factor_of * one(*cut)
    return factor_of


def scatter_about(stream_key, dims, scale, reach, cuts=(), kind=jnp.bfloat16):
    factor_of = steps_of(stream_key, dims, cuts, -0.22, 0.18) if cuts else 1.0
    values = jax.random.normal(stream_key, dims, jnp.float32) * scale * factor_of
    return jnp.minimum(jnp.maximum(values, -reach), reach).astype(kind)


def setup_inputs(seed: int = 0) -> dict:
    streams_of = jax.random.split(jax.random.key(seed), 16)
    latent = scatter_about(streams_of[0], (TOKENS, D), 1.0, 6.0, ((0, 32),))
    context = scatter_about(streams_of[1], (CTX, D), 1.0, 6.0, ((0, 32),))
    condition = scatter_about(streams_of[2], (D,), 1.0, 6.0)
    context_condition = scatter_about(streams_of[3], (D,), 1.0, 6.0)
    gain_pre = jnp.clip(1.0 + 0.18 * jax.random.normal(streams_of[4], (D,), jnp.float32), 0.1, 1.9)
    gain_post = jnp.clip(1.0 + 0.18 * jax.random.normal(streams_of[5], (D,), jnp.float32), 0.1, 1.9)
    w_shift = scatter_about(streams_of[6], (D, D), D ** -0.5, 0.125, ((0, 32), (1, 8)))
    w_scale = scatter_about(streams_of[7], (D, D), D ** -0.5, 0.125, ((0, 32), (1, 8)))
    w_gate = scatter_about(streams_of[8], (D, D), D ** -0.5, 0.125, ((0, 32), (1, 8)))
    w_query = draw_w_query(jax.random.fold_in(streams_of[15], 71), 0)
    w_key = draw_w_key(jax.random.fold_in(streams_of[15], 71), 0)
    w_value = scatter_about(streams_of[11], (D, D), D ** -0.5, 0.125, ((1, 8),))
    w_silu = scatter_about(streams_of[12], (D, D), D ** -0.5, 0.125, ((1, 8),))
    offset_bias = jnp.clip(1.5 + 2.0 * jax.random.uniform(streams_of[13], (HEADS, 2 * WIN_ROWS - 1, 2 * WIN_COLS - 1), jnp.float32) ** steps_of(streams_of[13], (HEADS, 2 * WIN_ROWS - 1, 2 * WIN_COLS - 1), ((0, 8),), -0.2, 0.2), 1.5, 3.5)
    w_out = scatter_about(streams_of[14], (D, D), D ** -0.5, 0.125, ((0, 8),))
    return {"latent": latent, "context": context, "condition": condition, "context_condition": context_condition, "gain_pre": gain_pre, "gain_post": gain_post, "w_shift": w_shift, "w_scale": w_scale, "w_gate": w_gate, "w_query": w_query, "w_key": w_key, "w_value": w_value, "w_silu": w_silu, "offset_bias": offset_bias, "w_out": w_out}


EPSILON = 1e-06

def rounded(values):
    return lax.optimization_barrier(values.astype(jnp.bfloat16))

def normalize(row_block, gain_row):
    values = row_block.astype(jnp.float32)
    return values * lax.rsqrt(lax.optimization_barrier(jnp.mean(values * values, axis=-1, keepdims=True)) + EPSILON) * gain_row

def project(row_block, weight):
    return rounded(jnp.dot(row_block, weight, preferred_element_type=jnp.float32))

def reference(latent, context, condition, context_condition, gain_pre, gain_post, w_shift, w_scale, w_gate, w_query, w_key, w_value, w_silu, offset_bias, w_out):
    active = jax.nn.silu(jnp.stack([condition, context_condition]).astype(jnp.float32)).astype(jnp.bfloat16)
    shifts = jnp.dot(active, w_shift, preferred_element_type=jnp.float32)
    scales = jnp.dot(active, w_scale, preferred_element_type=jnp.float32)
    gating = jnp.dot(active, w_gate, preferred_element_type=jnp.float32)
    hidden = rounded(normalize(latent, gain_pre) * (1.0 + scales[0]) + shifts[0])
    context_hidden = rounded(normalize(context, gain_pre) * (1.0 + scales[1]) + shifts[1])
    queries = project(hidden, w_query)
    keys_latent = project(hidden, w_key)
    values_latent = project(hidden, w_value)
    silu_gate = project(hidden, w_silu)
    context_keys = project(context_hidden, w_key).reshape(-1, HEADS, HEAD_DIM).astype(jnp.float32)
    context_values = project(context_hidden, w_value).reshape(-1, HEADS, HEAD_DIM).astype(jnp.float32)
    tokens, model_width = latent.shape
    grid_rows = tokens // GRID_W
    score_scale = HEAD_DIM ** (-0.5)
    query_grid = queries.reshape(grid_rows, GRID_W, HEADS, HEAD_DIM)
    key_grid = keys_latent.reshape(grid_rows, GRID_W, HEADS, HEAD_DIM)
    value_grid = values_latent.reshape(grid_rows, GRID_W, HEADS, HEAD_DIM)
    columns = jnp.arange(GRID_W, dtype=jnp.int32)
    col_start = jnp.clip(columns - WIN_COLS // 2, 0, GRID_W - WIN_COLS)
    col_inside = (columns[None, :] >= col_start[:, None]) & (columns[None, :] < col_start[:, None] + WIN_COLS)
    col_offset = jnp.clip(columns[None, :] - columns[:, None] + WIN_COLS - 1, 0, 2 * WIN_COLS - 2)

    def row_step(row_index):
        row_first = jnp.clip(row_index - WIN_ROWS // 2, 0, grid_rows - WIN_ROWS)
        query_row = lax.dynamic_index_in_dim(query_grid, row_index, 0, keepdims=False).astype(jnp.float32)
        key_band = lax.dynamic_slice_in_dim(key_grid, row_first, WIN_ROWS, 0).astype(jnp.float32)
        value_band = lax.dynamic_slice_in_dim(value_grid, row_first, WIN_ROWS, 0).astype(jnp.float32)
        row_offset = row_first + jnp.arange(WIN_ROWS, dtype=jnp.int32) - row_index + WIN_ROWS - 1
        offset_terms = offset_bias[:, row_offset[:, None, None], col_offset[None, :, :]]
        window_scores = jnp.einsum('qhd,vkhd->hqvk', query_row, key_band) * score_scale + jnp.transpose(offset_terms, (0, 2, 1, 3))
        window_scores = jnp.where(col_inside[None, :, None, :], window_scores, -jnp.inf)
        context_scores = jnp.einsum('qhd,jhd->hqj', query_row, context_keys) * score_scale
        maximum = jnp.maximum(lax.optimization_barrier(jnp.max(window_scores, axis=(2, 3))), lax.optimization_barrier(jnp.max(context_scores, axis=2)))
        window_exp = jnp.exp(window_scores - maximum[:, :, None, None])
        context_exp = jnp.exp(context_scores - maximum[:, :, None])
        denominator = lax.optimization_barrier(jnp.sum(window_exp, axis=(2, 3))) + lax.optimization_barrier(jnp.sum(context_exp, axis=2))
        window_weights = rounded(window_exp / denominator[:, :, None, None]).astype(jnp.float32)
        context_weights = rounded(context_exp / denominator[:, :, None]).astype(jnp.float32)
        return jnp.einsum('hqvk,vkhd->qhd', window_weights, value_band) + jnp.einsum('hqj,jhd->qhd', context_weights, context_values)
    attended = lax.map(row_step, jnp.arange(grid_rows, dtype=jnp.int32)).reshape(tokens, model_width)
    gated_heads = rounded(jax.nn.silu(silu_gate.astype(jnp.float32)) * attended)
    group_width = model_width // N_TP
    branch_sum = jnp.zeros((tokens, model_width), jnp.float32)
    for group_index in range(N_TP):
        first_col = group_index * group_width
        term = jnp.dot(gated_heads[:, first_col:first_col + group_width], w_out[first_col:first_col + group_width], preferred_element_type=jnp.float32)
        branch_sum = branch_sum + rounded(term).astype(jnp.float32)
    branch = rounded(branch_sum)
    updated = latent.astype(jnp.float32) + gating[0] * normalize(branch, gain_post)
    return updated.astype(jnp.bfloat16)
```

```python
import functools

import jax
import jax.numpy as jnp
from jax import lax
from jax.experimental import pallas as pl
from jax.experimental.pallas import tpu as pltpu
from jax.sharding import PartitionSpec as P

GRID_W = 64
WIN_ROWS = 8
WIN_COLS = 16
EPSILON = 1e-06
NZ, NY, NX, NC = 8, 4, 4, 2
NTP = NX * NC
D = 2048
HD = 64
TOK = 256
CTXL = 32
CTX = 1024
OUTR = TOK // NTP
LAST_START = NZ * NY * TOK // GRID_W - WIN_ROWS
SPECIAL = (0, 1, 2, 6, 7)
F32 = jnp.float32
BF16 = jnp.bfloat16
NT = (((1,), (1,)), ((), ()))


def dot(a, b):
    return jnp.dot(a, b, preferred_element_type=F32)


def dot_nt(a, b):
    return lax.dot_general(a, b, NT, preferred_element_type=F32)


def remote(src, dst, ssem, rsem, sp, tp):
    return pltpu.make_async_remote_copy(
        src_ref=src,
        dst_ref=dst,
        send_sem=ssem,
        recv_sem=rsem,
        device_id=(sp, tp),
        device_id_type=pl.DeviceIdType.MESH,
    )


def half_swap(v):
    return pltpu.roll(v, 64, 1)


def kernel(
    act_ref,
    biasx_ref,
    gpre_ref,
    gpost_ref,
    lat_h,
    ctx_h,
    wsh_h,
    wsc_h,
    wga_h,
    wq_h,
    wk_h,
    wv_h,
    wg_h,
    wo_h,
    out_ref,
    wmod,
    lat,
    ctx,
    wkv,
    wqg,
    wo,
    wo2,
    zsend,
    zrecv,
    msend,
    mrecv,
    mod,
    btab,
    hid,
    hidc,
    rsl,
    rsc,
    csend,
    ctxkv,
    kvsend,
    kvext,
    qsend,
    qrecv,
    sg,
    rsend,
    rrecv,
    gated,
    grecv,
    psend,
    precv,
    lsem,
    zs,
    zr,
    ms,
    mr,
    ws,
    wr,
    cs,
    cr,
    ks,
    kr,
    qs,
    qr,
    hs,
    hr,
    rs,
    rr,
    gs,
    gr,
    ps,
    pr,
):
    sp = lax.axis_index("sp")
    tp = lax.axis_index("tp")
    z, y = lax.div(sp, NY), lax.rem(sp, NY)
    x, core = lax.div(tp, NC), lax.rem(tp, NC)
    partner = x * NC + (1 - core)
    group = y * NTP + tp
    lane = lax.broadcasted_iota(jnp.int32, (1, 128), 1)
    low = lane < 64

    barrier = pltpu.get_barrier_semaphore()

    def greet(dsp, dtp):
        pl.semaphore_signal(
            barrier, inc=1, device_id=(dsp, dtp), device_id_type=pl.DeviceIdType.MESH
        )

    def greet_z(k, c):
        greet(lax.rem(z + k, NZ) * NY + y, tp)
        return c

    def greet_g(k, c):
        g = lax.rem(group + k, NY * NTP)
        greet(z * NY + lax.div(g, NTP), lax.rem(g, NTP))
        return c

    lax.fori_loop(1, NZ, greet_z, 0)
    lax.fori_loop(1, NY * NTP, greet_g, 0)

    loads = [
        (wsh_h, wmod.at[0]),
        (wsc_h, wmod.at[1]),
        (wga_h, wmod.at[2]),
        (ctx_h, ctx),
        (lat_h, lat),
        (wo_h, wo),
        (wk_h, wkv.at[:, pl.ds(0, TOK)]),
        (wv_h, wkv.at[:, pl.ds(TOK, TOK)]),
        (wq_h, wqg.at[:, pl.ds(0, TOK)]),
        (wg_h, wqg.at[:, pl.ds(TOK, TOK)]),
    ]
    loads = [pltpu.make_async_copy(a, b, lsem.at[i]) for i, (a, b) in enumerate(loads)]
    for c in loads:
        c.start()

    for c in loads[:3]:
        c.wait()
    act = act_ref[...]
    sh = dot(act, wmod[0])
    sc = dot(act, wmod[1])
    ga = dot(act, wmod[2])
    zsend[0:2] = sh[0:2, :128]
    zsend[2:4] = sc[0:2, :128]
    zsend[4:6] = sh[0:2, 128:]
    zsend[6:8] = sc[0:2, 128:]
    zsend[8:10] = ga[0:2, :128]
    zsend[10:12] = ga[0:2, 128:]
    zsend[12:16] = jnp.zeros((4, 128), F32)
    zrecv[z] = zsend[...]

    pl.semaphore_wait(barrier, NZ - 1 + NY * NTP - 1)

    def z_copy(k):
        dz = lax.rem(z + k, NZ)
        return remote(zsend, zrecv.at[z], zs.at[dz], zr.at[z], dz * NY + y, tp)

    def z_in(k):
        dz = lax.rem(z + k, NZ)
        return remote(zsend, zrecv.at[dz], zs.at[dz], zr.at[dz], dz * NY + y, tp)

    for k in (4, 3, 5, 2, 6, 1, 7):
        z_copy(k).start()

    loads[5].wait()
    w_copy = remote(wo, wo2, ws, wr, sp, partner)

    loads[3].wait()
    v = ctx[...].astype(F32)
    r = lax.rsqrt(jnp.mean(v * v, axis=1, keepdims=True) + EPSILON)
    rsc[...] = jnp.broadcast_to(r, (CTXL, 128))
    loads[4].wait()

    def lat_stats(i, c):
        rows = pl.ds(pl.multiple_of(i * 32, 32), 32)
        v = lat[rows, :].astype(F32)
        r = lax.rsqrt(jnp.mean(v * v, axis=1, keepdims=True) + EPSILON)
        rsl[rows, :] = jnp.broadcast_to(r, (32, 128))
        return c

    lax.fori_loop(0, TOK // 32, lat_stats, 0)

    for k in range(1, NZ):
        z_in(k).wait_recv()
    total = zrecv[0]
    for k in range(1, NZ):
        total = total + zrecv[k]
    msend[...] = total
    mrecv[y, tp] = total

    def m_copy(k):
        g = lax.rem(group + k, NY * NTP)
        dy, dt = lax.div(g, NTP), lax.rem(g, NTP)
        return remote(msend, mrecv.at[y, tp], ms.at[g], mr.at[group], z * NY + dy, dt)

    def m_in(k):
        g = lax.rem(group + k, NY * NTP)
        dy, dt = lax.div(g, NTP), lax.rem(g, NTP)
        return remote(msend, mrecv.at[dy, dt], ms.at[g], mr.at[g], z * NY + dy, dt)

    def m_start(k, c):
        m_copy(k).start()
        return c

    lax.fori_loop(1, NY * NTP, m_start, 0)
    w_copy.start()

    col = lax.rem(lax.broadcasted_iota(jnp.int32, (64, 128), 1), 64)
    right = lax.div(lax.broadcasted_iota(jnp.int32, (64, 128), 1), 64)
    qcol = lax.broadcasted_iota(jnp.int32, (64, 128), 0)
    first_col = jnp.clip(qcol - WIN_COLS // 2, 0, GRID_W - WIN_COLS)
    in_cols = (col >= first_col) & (col < first_col + WIN_COLS)
    row0 = z * 16

    def table(t, c):
        p = jnp.where(t < 3, t, t + 3)
        base = jnp.clip(row0 + 2 * p - 4, 0, LAST_START)
        for a in range(2):
            row = row0 + 2 * p + a
            off = jnp.clip(row - 4, 0, LAST_START) - base
            d0 = base - row + 7
            for m in range(5):
                line = biasx_ref[y, pl.ds(d0 + 2 * m, 1), :]
                tile = pltpu.roll(
                    jnp.broadcast_to(line, (64, 128)), 113, 1, stride=1, stride_axis=0
                )
                krow = right + 2 * m
                ok = in_cols & (krow >= off) & (krow < off + WIN_ROWS)
                btab[t, a * 64 : a * 64 + 64, m * 128 : m * 128 + 128] = jnp.where(
                    ok, tile, -jnp.inf
                )
        return c

    lax.fori_loop(0, len(SPECIAL), table, 0)

    @pl.when(z == 0)
    def _():
        kvext[0:TOK] = jnp.zeros((TOK, 128), BF16)

    @pl.when(z == NZ - 1)
    def _():
        kvext[5 * TOK : 6 * TOK] = jnp.zeros((TOK, 128), BF16)

    def m_wait(k, c):
        m_in(k).wait_recv()
        return c

    lax.fori_loop(1, NY * NTP, m_wait, 0)
    for t in range(NTP):
        total = mrecv[0, t] + mrecv[1, t] + mrecv[2, t] + mrecv[3, t]
        lo, hi = 256 * t, 256 * t + 128
        mod[0:4, lo : lo + 128] = total[0:4]
        mod[0:4, hi : hi + 128] = total[4:8]
        mod[4:5, lo : lo + 128] = total[8:9]
        mod[4:5, hi : hi + 128] = total[10:11]
    gpre = gpre_ref[...]

    v = ctx[...].astype(F32) * rsc[:, 0:1]
    hidc[...] = (v * (gpre * (1.0 + mod[3:4, :])) + mod[1:2, :]).astype(BF16)
    loads[6].wait()
    loads[7].wait()
    kv = dot(hidc[...], wkv[...])
    for q in range(2):
        kt = kv[:, 128 * q : 128 * q + 128]
        vt = kv[:, 256 + 128 * q : 256 + 128 * q + 128]
        csend[2 * q] = jnp.where(low, kt, half_swap(vt)).astype(BF16)
        csend[2 * q + 1] = jnp.where(low, half_swap(kt), vt).astype(BF16)
    here = pl.ds(pl.multiple_of(sp * CTXL, CTXL), CTXL)
    ctxkv[here, :] = csend[y]

    def c_copy(k):
        d = lax.rem(sp + k, NZ * NY)
        return remote(csend.at[lax.rem(d, NY)], ctxkv.at[here, :], cs.at[d], cr.at[sp], d, tp)

    def c_in(k):
        d = lax.rem(sp + k, NZ * NY)
        there = pl.ds(pl.multiple_of(d * CTXL, CTXL), CTXL)
        return remote(csend.at[y], ctxkv.at[there, :], cs.at[d], cr.at[d], d, tp)

    def c_start(k, c):
        c_copy(k).start()
        return c

    lax.fori_loop(1, NZ * NY, c_start, 0)

    scale = gpre * (1.0 + mod[2:3, :])
    shift = mod[0:1, :]

    def lat_hidden(i, c):
        rows = pl.ds(pl.multiple_of(i * 32, 32), 32)
        v = lat[rows, :].astype(F32) * rsl[rows, 0:1]
        hid[rows, :] = (v * scale + shift).astype(BF16)
        return c

    lax.fori_loop(0, TOK // 32, lat_hidden, 0)
    kv = dot(hid[...], wkv[...])
    for q in range(2):
        kt = kv[:, 128 * q : 128 * q + 128]
        vt = kv[:, 256 + 128 * q : 256 + 128 * q + 128]
        kvsend[2 * q] = jnp.where(low, kt, half_swap(vt)).astype(BF16)
        kvsend[2 * q + 1] = jnp.where(low, half_swap(kt), vt).astype(BF16)
    mine = pl.ds(pl.multiple_of((1 + y) * TOK, TOK), TOK)
    kvext[mine, :] = kvsend[y]

    def k_copy(k):
        dy = lax.rem(y + k, NY)
        return remote(kvsend.at[dy], kvext.at[mine, :], ks.at[dy], kr.at[y], z * NY + dy, tp)

    def k_in(dy):
        rows = pl.ds(pl.multiple_of((1 + dy) * TOK, TOK), TOK)
        return remote(kvsend.at[y], kvext.at[rows, :], ks.at[dy], kr.at[dy], z * NY + dy, tp)

    for k in (2, 1, 3):
        k_copy(k).start()

    loads[8].wait()
    loads[9].wait()
    qg = dot(hid[...], wqg[...])
    for q in range(2):
        qt = qg[:, 128 * q : 128 * q + 128] * (HD**-0.5)
        up, dn = qt[0:128], qt[128:256]
        qsend[2 * q] = jnp.where(low, up, half_swap(dn)).astype(BF16)
        qsend[2 * q + 1] = jnp.where(low, half_swap(up), dn).astype(BF16)
    qrecv[y] = qsend[y]

    def q_copy(k):
        dy = lax.rem(y + k, NY)
        return remote(qsend.at[dy], qrecv.at[y], qs.at[dy], qr.at[y], z * NY + dy, tp)

    def q_in(k):
        dy = lax.rem(y + k, NY)
        return remote(qsend.at[dy], qrecv.at[dy], qs.at[dy], qr.at[dy], z * NY + dy, tp)

    for k in (2, 1, 3):
        q_copy(k).start()
    g = qg[:, 256:].astype(BF16).astype(F32)
    sg[...] = g * (1.0 / (1.0 + jnp.exp(-g)))

    up_src = kvext.at[pl.ds(4 * TOK, TOK), :]
    dn_src = kvext.at[pl.ds(TOK, TOK), :]
    up_dst = kvext.at[pl.ds(0, TOK), :]
    dn_dst = kvext.at[pl.ds(5 * TOK, TOK), :]
    up_copy = remote(up_src, up_dst, hs.at[0], hr.at[0], jnp.minimum(z + 1, NZ - 1) * NY + y, tp)
    dn_copy = remote(dn_src, dn_dst, hs.at[1], hr.at[1], jnp.maximum(z - 1, 0) * NY + y, tp)

    @pl.when(y != 3)
    def _():
        k_in(3).wait_recv()

    @pl.when(z < NZ - 1)
    def _():
        up_copy.start()

    @pl.when(y != 0)
    def _():
        k_in(0).wait_recv()

    @pl.when(z > 0)
    def _():
        dn_copy.start()

    @pl.when(y != 1)
    def _():
        k_in(1).wait_recv()

    @pl.when(y != 2)
    def _():
        k_in(2).wait_recv()

    for k in (1, 2, 3):
        q_in(k).wait_recv()

    def c_wait(k, c):
        c_in(k).wait_recv()
        return c

    lax.fori_loop(1, NZ * NY, c_wait, 0)

    @pl.when(z > 0)
    def _():
        up_copy.wait_recv()

    @pl.when(z < NZ - 1)
    def _():
        dn_copy.wait_recv()

    def r_copy(dy):
        return remote(rsend.at[dy], rrecv.at[y], rs.at[dy], rr.at[y], z * NY + dy, tp)

    def r_in(dy):
        return remote(rsend.at[dy], rrecv.at[dy], rs.at[dy], rr.at[dy], z * NY + dy, tp)

    def block(k, c):
        b = lax.rem(y + k, NY)
        xq = qrecv[b].astype(F32)
        outs = []
        for a in range(2):
            p = 2 * b + a
            xa = xq if a == 0 else half_swap(xq)
            qp = jnp.where(low, xa, 0.0).astype(BF16)
            base = jnp.clip(row0 + 2 * p - 4, 0, LAST_START) - row0 + 4
            rows = pl.ds(pl.multiple_of(base * GRID_W, GRID_W), 10 * GRID_W)
            t = jnp.where(p < 2, p, jnp.where(p < 6, 2, p - 3))
            sc_ctx = dot_nt(qp, ctxkv[...])
            kvw = kvext[rows, :]
            sc_win = dot_nt(qp, kvw) + btab[t]
            top = jnp.maximum(
                jnp.max(sc_ctx, axis=1, keepdims=True), jnp.max(sc_win, axis=1, keepdims=True)
            )
            e_ctx = jnp.exp(sc_ctx - top)
            e_win = jnp.exp(sc_win - top)
            den = jnp.sum(e_ctx, axis=1, keepdims=True) + jnp.sum(e_win, axis=1, keepdims=True)
            o = dot(e_ctx.astype(BF16), ctxkv[...]) + dot(e_win.astype(BF16), kvw)
            outs.append(o * (1.0 / den))
        rsend[b] = jnp.where(low, half_swap(outs[0]), outs[1]).astype(BF16)

        @pl.when(k < NY)
        def _():
            r_copy(b).start()

        @pl.when(k == NY)
        def _():
            rrecv[b] = rsend[b]

        return c

    lax.fori_loop(1, NY + 1, block, 0)
    for k in (1, 2, 3):
        r_in(lax.rem(y + k, NY)).wait_recv()

    for q in range(2):
        x0, x1 = rrecv[2 * q].astype(F32), rrecv[2 * q + 1].astype(F32)
        up = jnp.where(low, x0, half_swap(x1)) * sg[0:128, 128 * q : 128 * q + 128]
        dn = jnp.where(low, half_swap(x0), x1) * sg[128:256, 128 * q : 128 * q + 128]
        cols = slice(128 * q, 128 * q + 128)
        for i in range(2):
            for h in range(2):
                lo = 64 * i + 32 * h
                gated[i, h, :, cols] = up[lo : lo + 32].astype(BF16)
                gated[2 + i, h, :, cols] = dn[lo : lo + 32].astype(BF16)
    g_copy = remote(gated.at[:, 1 - core], grecv, gs, gr, sp, partner)
    g_copy.start()
    w_copy.wait_recv()
    g_copy.wait_recv()
    g_own = gated[:, core].reshape(NX * OUTR, TOK)
    g_other = grecv[...].reshape(NX * OUTR, TOK)
    for n in range(4):
        cols = slice(512 * n, 512 * n + 512)
        term = dot(g_own, wo[:, cols]) + dot(g_other, wo2[:, cols])
        psend[:, :, cols] = term.reshape(NX, OUTR, 512).astype(BF16)

    def p_copy(k):
        dx = lax.rem(x + k, NX)
        return remote(psend.at[dx], precv.at[x], ps.at[dx], pr.at[x], sp, dx * NC + core)

    def p_in(k):
        dx = lax.rem(x + k, NX)
        return remote(psend.at[dx], precv.at[dx], ps.at[dx], pr.at[dx], sp, dx * NC + core)

    for k in (2, 1, 3):
        p_copy(k).start()
    for k in (1, 3, 2):
        p_in(k).wait_recv()
    branch = psend[x].astype(F32)
    for k in (1, 2, 3):
        branch = branch + precv[lax.rem(x + k, NX)].astype(F32)
    branch = branch.astype(BF16).astype(F32)
    normed = branch * lax.rsqrt(jnp.mean(branch * branch, axis=1, keepdims=True) + EPSILON)
    own = lat[pl.ds(pl.multiple_of(tp * OUTR, OUTR), OUTR), :].astype(F32)
    out_ref[...] = (own + mod[4:5, :] * (normed * gpost_ref[...])).astype(BF16)

    for k in range(1, NZ):
        z_copy(k).wait_send()

    def sent(k, c):
        m_copy(k).wait_send()
        c_copy(k).wait_send()
        return c

    lax.fori_loop(1, NY * NTP, sent, 0)
    w_copy.wait_send()
    g_copy.wait_send()
    for k in (1, 2, 3):
        k_copy(k).wait_send()
        q_copy(k).wait_send()
        r_copy(lax.rem(y + k, NY)).wait_send()
        p_copy(k).wait_send()

    @pl.when(z < NZ - 1)
    def _():
        up_copy.wait_send()

    @pl.when(z > 0)
    def _():
        dn_copy.wait_send()


def shards(
    latent,
    context,
    condition,
    context_condition,
    gain_pre,
    gain_post,
    w_shift,
    w_scale,
    w_gate,
    w_query,
    w_key,
    w_value,
    w_silu,
    offset_bias,
    w_out,
):
    sp_index = lax.axis_index("sp")
    in_rows = w_shift.shape[0]
    own = lax.dynamic_slice_in_dim(
        jnp.stack([condition, context_condition]), sp_index * in_rows, in_rows, 1
    )
    act = jnp.pad(jax.nn.silu(own.astype(F32)).astype(BF16), ((0, 6), (0, 0)))
    lines = jnp.pad(offset_bias, ((0, 0), (0, 2), (0, 33)))
    biasx = jnp.concatenate([lines[:, :16], lines[:, 1:17]], axis=2)
    vmem = pl.BlockSpec(memory_space=pltpu.VMEM)
    hbm = pl.BlockSpec(memory_space=pl.ANY)
    dma = pltpu.SemaphoreType.DMA
    return pl.pallas_call(
        kernel,
        name="whole",
        out_shape=jax.ShapeDtypeStruct((OUTR, D), BF16),
        in_specs=[vmem] * 4 + [hbm] * 10,
        out_specs=vmem,
        scratch_shapes=[
            pltpu.VMEM((3, in_rows, TOK), BF16),
            pltpu.VMEM((TOK, D), BF16),
            pltpu.VMEM((CTXL, D), BF16),
            pltpu.VMEM((D, 2 * TOK), BF16),
            pltpu.VMEM((D, 2 * TOK), BF16),
            pltpu.VMEM((TOK, D), BF16),
            pltpu.VMEM((TOK, D), BF16),
            pltpu.VMEM((16, 128), F32),
            pltpu.VMEM((NZ, 16, 128), F32),
            pltpu.VMEM((16, 128), F32),
            pltpu.VMEM((NY, NTP, 16, 128), F32),
            pltpu.VMEM((8, D), F32),
            pltpu.VMEM((len(SPECIAL), 128, 640), F32),
            pltpu.VMEM((TOK, D), BF16),
            pltpu.VMEM((CTXL, D), BF16),
            pltpu.VMEM((TOK, 128), F32),
            pltpu.VMEM((CTXL, 128), F32),
            pltpu.VMEM((NY, CTXL, 128), BF16),
            pltpu.VMEM((CTX, 128), BF16),
            pltpu.VMEM((NY, TOK, 128), BF16),
            pltpu.VMEM((6 * TOK, 128), BF16),
            pltpu.VMEM((NY, 128, 128), BF16),
            pltpu.VMEM((NY, 128, 128), BF16),
            pltpu.VMEM((TOK, TOK), F32),
            pltpu.VMEM((NY, 128, 128), BF16),
            pltpu.VMEM((NY, 128, 128), BF16),
            pltpu.VMEM((NX, NC, OUTR, TOK), BF16),
            pltpu.VMEM((NX, OUTR, TOK), BF16),
            pltpu.VMEM((NX, OUTR, D), BF16),
            pltpu.VMEM((NX, OUTR, D), BF16),
            dma((10,)),
            dma((NZ,)),
            dma((NZ,)),
            dma((NY * NTP,)),
            dma((NY * NTP,)),
            dma,
            dma,
            dma((NZ * NY,)),
            dma((NZ * NY,)),
            dma((NY,)),
            dma((NY,)),
            dma((NY,)),
            dma((NY,)),
            dma((2,)),
            dma((2,)),
            dma((NY,)),
            dma((NY,)),
            dma,
            dma,
            dma((NX,)),
            dma((NX,)),
        ],
        compiler_params=pltpu.CompilerParams(
            collective_id=0, has_side_effects=True, vmem_limit_bytes=48 << 20
        ),
    )(
        act,
        biasx,
        gain_pre.reshape(1, D),
        gain_post.reshape(1, D),
        latent,
        context,
        w_shift,
        w_scale,
        w_gate,
        w_query,
        w_key,
        w_value,
        w_silu,
        w_out,
    )


def solution(mesh):
    in_specs = (
        P("sp", None),
        P("sp", None),
        P(),
        P(),
        P(),
        P(),
        P("sp", "tp"),
        P("sp", "tp"),
        P("sp", "tp"),
        P(None, "tp"),
        P(None, "tp"),
        P(None, "tp"),
        P(None, "tp"),
        P("tp", None, None),
        P("tp", None),
    )
    out_specs = P(("sp", "tp"), None)
    return jax.shard_map(shards, mesh=mesh, in_specs=in_specs, out_specs=out_specs, check_vma=False)
```

```python
import functools

import jax
import jax.numpy as jnp
from jax import lax
from jax.experimental import pallas as pl
from jax.experimental.pallas import tpu as pltpu
from jax.sharding import PartitionSpec as P

GRID_W = 64
WIN_ROWS = 8
WIN_COLS = 16
EPSILON = 1e-06
NZ, NY, NX, NC = 8, 4, 4, 2
NTP = NX * NC
D = 2048
HD = 64
TOK = 256
CTXL = 32
CTX = 1024
OUTR = TOK // NTP
LAST_START = NZ * NY * TOK // GRID_W - WIN_ROWS
SPECIAL = (0, 1, 2, 6, 7)
F32 = jnp.float32
BF16 = jnp.bfloat16
NT = (((1,), (1,)), ((), ()))


def dot(a, b):
    return jnp.dot(a, b, preferred_element_type=F32)


def dot_nt(a, b):
    return lax.dot_general(a, b, NT, preferred_element_type=F32)


def remote(src, dst, ssem, rsem, sp, tp):
    return pltpu.make_async_remote_copy(
        src_ref=src,
        dst_ref=dst,
        send_sem=ssem,
        recv_sem=rsem,
        device_id=(sp, tp),
        device_id_type=pl.DeviceIdType.MESH,
    )


class Phases:
    def __init__(self):
        self.scope = None

    def __call__(self, name):
        if self.scope is not None:
            self.scope.__exit__(None, None, None)
        self.scope = None
        if name:
            self.scope = jax.named_scope(name)
            self.scope.__enter__()


def half_swap(v):
    return pltpu.roll(v, 64, 1)


def kernel(
    cond_h,
    cond2_h,
    gpre_h,
    gpost_h,
    bias_h,
    lat_h,
    ctx_h,
    wsh_h,
    wsc_h,
    wga_h,
    wq_h,
    wk_h,
    wv_h,
    wg_h,
    wo_h,
    out_ref,
    conds,
    condf,
    gains,
    bias,
    biasx,
    wmod,
    lat,
    wkv,
    wqg,
    wo,
    wo2,
    zsend,
    zrecv,
    msend,
    mrecv,
    zgsend,
    zgrecv,
    mgsend,
    mgrecv,
    mod,
    btab,
    hid,
    rsl,
    csend,
    ctxkv,
    kvsend,
    kvext,
    qsend,
    qrecv,
    sg,
    rsend,
    rrecv,
    gated,
    grecv,
    psend,
    precv,
    lsem,
    zs,
    zr,
    ms,
    mr,
    zgs,
    zgr,
    mgs,
    mgr,
    ws,
    wr,
    cs,
    cr,
    ks,
    kr,
    qs,
    qr,
    hs,
    hr,
    rs,
    rr,
    gs,
    gr,
    ps,
    pr,
):
    sp = lax.axis_index("sp")
    tp = lax.axis_index("tp")
    z, y = lax.div(sp, NY), lax.rem(sp, NY)
    x, core = lax.div(tp, NC), lax.rem(tp, NC)
    partner = x * NC + (1 - core)
    group = y * NTP + tp
    lane = lax.broadcasted_iota(jnp.int32, (1, 128), 1)
    low = lane < 64

    phase = Phases()
    phase("loads")
    loads = [
        (cond_h, conds.at[0]),
        (cond2_h, conds.at[1]),
        (wsh_h, wmod.at[0]),
        (wsc_h, wmod.at[1]),
        (wga_h, wmod.at[2]),
        (ctx_h, lat.at[pl.ds(TOK, CTXL), :]),
        (lat_h, lat.at[pl.ds(0, TOK), :]),
        (gpre_h, gains.at[0]),
        (gpost_h, gains.at[1]),
        (bias_h, bias),
        (wo_h, wo),
        (wk_h, wkv.at[:, pl.ds(0, TOK)]),
        (wv_h, wkv.at[:, pl.ds(TOK, TOK)]),
        (wq_h, wqg.at[:, pl.ds(0, TOK)]),
        (wg_h, wqg.at[:, pl.ds(TOK, TOK)]),
    ]
    loads = [pltpu.make_async_copy(a, b, lsem.at[i]) for i, (a, b) in enumerate(loads)]
    for c in loads:
        c.start()

    phase("greet")
    barrier = pltpu.get_barrier_semaphore()

    def greet(dsp, dtp):
        pl.semaphore_signal(
            barrier, inc=1, device_id=(dsp, dtp), device_id_type=pl.DeviceIdType.MESH
        )

    def greet_z(k, c):
        greet(lax.rem(z + k, NZ) * NY + y, tp)
        return c

    def greet_g(k, c):
        g = lax.rem(group + k, NY * NTP)
        greet(z * NY + lax.div(g, NTP), lax.rem(g, NTP))
        return c

    lax.fori_loop(1, NZ, greet_z, 0)
    lax.fori_loop(1, NY * NTP, greet_g, 0)

    phase("partial")
    for c in loads[:2]:
        c.wait()
    v = conds[...].astype(F32)
    condf[...] = v * (1.0 / (1.0 + jnp.exp(-v)))
    line = jnp.concatenate([condf[i, pl.ds(lax.div(sp, 2), 1), :] for i in range(2)], axis=0)
    line = jnp.where(lax.rem(sp, 2) == 1, half_swap(line), line)[:, :64]
    act = jnp.concatenate([line, jnp.zeros((6, 64), F32)], axis=0).astype(BF16)
    for c in loads[2:5]:
        c.wait()
    sh = dot(act, wmod[0])
    sc = dot(act, wmod[1])
    ga = dot(act, wmod[2])
    zsend[0:2] = sh[0:2, :128]
    zsend[2:4] = sc[0:2, :128]
    zsend[4:6] = sh[0:2, 128:]
    zsend[6:8] = sc[0:2, 128:]
    zgsend[0:1] = ga[0:1, :128]
    zgsend[1:2] = ga[0:1, 128:]
    zrecv[z] = zsend[...]
    zgrecv[z] = zgsend[...]

    phase("barrier")
    pl.semaphore_wait(barrier, NZ - 1 + NY * NTP - 1)

    phase("z_start")
    def z_copy(k):
        dz = lax.rem(z + k, NZ)
        return remote(zsend, zrecv.at[z], zs.at[dz], zr.at[z], dz * NY + y, tp)

    def z_in(k):
        dz = lax.rem(z + k, NZ)
        return remote(zsend, zrecv.at[dz], zs.at[dz], zr.at[dz], dz * NY + y, tp)

    def zg_copy(k):
        dz = lax.rem(z + k, NZ)
        return remote(zgsend, zgrecv.at[z], zgs.at[dz], zgr.at[z], dz * NY + y, tp)

    def zg_in(k):
        dz = lax.rem(z + k, NZ)
        return remote(zgsend, zgrecv.at[dz], zgs.at[dz], zgr.at[dz], dz * NY + y, tp)

    far_first = (4, 3, 5, 2, 6, 1, 7)
    for k in far_first:
        z_copy(k).start()
    for k in far_first:
        zg_copy(k).start()

    phase("stats")
    w_copy = remote(wo, wo2, ws, wr, sp, partner)

    loads[5].wait()
    loads[6].wait()

    def row_stats(i, c):
        rows = pl.ds(pl.multiple_of(i * 32, 32), 32)
        v = lat[rows, :].astype(F32)
        r = lax.rsqrt(jnp.mean(v * v, axis=1, keepdims=True) + EPSILON)
        rsl[rows, :] = jnp.broadcast_to(r, (32, 128))
        return c

    lax.fori_loop(0, (TOK + CTXL) // 32, row_stats, 0)
    loads[7].wait()
    loads[8].wait()
    for t in range(16):
        mod[5:6, 128 * t : 128 * t + 128] = gains[0, t : t + 1, :]
        mod[6:7, 128 * t : 128 * t + 128] = gains[1, t : t + 1, :]
    loads[9].wait()
    biasx[...] = jnp.zeros((16, 128), F32)
    for d in range(2 * WIN_ROWS - 1):
        line = bias[d, pl.ds(y, 1), :]
        biasx[d : d + 1, 0:31] = line
        if d > 0:
            biasx[d - 1 : d, 64:95] = line
    loads[10].wait()

    phase("z_wait")
    for k in range(1, NZ):
        z_in(k).wait_recv()
    phase("m_start")
    total = zrecv[0]
    for k in range(1, NZ):
        total = total + zrecv[k]
    msend[...] = total
    mrecv[y, tp] = total

    def m_copy(k):
        g = lax.rem(group + k, NY * NTP)
        dy, dt = lax.div(g, NTP), lax.rem(g, NTP)
        return remote(msend, mrecv.at[y, tp], ms.at[g], mr.at[group], z * NY + dy, dt)

    def m_in(k):
        g = lax.rem(group + k, NY * NTP)
        dy, dt = lax.div(g, NTP), lax.rem(g, NTP)
        return remote(msend, mrecv.at[dy, dt], ms.at[g], mr.at[g], z * NY + dy, dt)

    def m_start(k, c):
        m_copy(k).start()
        return c

    lax.fori_loop(1, NY * NTP, m_start, 0)
    w_copy.start()

    phase("tables")
    col = lax.rem(lax.broadcasted_iota(jnp.int32, (64, 128), 1), 64)
    right = lax.div(lax.broadcasted_iota(jnp.int32, (64, 128), 1), 64)
    qcol = lax.broadcasted_iota(jnp.int32, (64, 128), 0)
    first_col = jnp.clip(qcol - WIN_COLS // 2, 0, GRID_W - WIN_COLS)
    in_cols = (col >= first_col) & (col < first_col + WIN_COLS)
    row0 = z * 16

    def table(t, c):
        p = jnp.where(t < 3, t, t + 3)
        base = jnp.clip(row0 + 2 * p - 4, 0, LAST_START)
        for a in range(2):
            row = row0 + 2 * p + a
            off = jnp.clip(row - 4, 0, LAST_START) - base
            d0 = base - row + 7
            for m in range(5):
                line = biasx[pl.ds(d0 + 2 * m, 1), :]
                tile = pltpu.roll(
                    jnp.broadcast_to(line, (64, 128)), 113, 1, stride=1, stride_axis=0
                )
                krow = right + 2 * m
                ok = in_cols & (krow >= off) & (krow < off + WIN_ROWS)
                btab[t, a * 64 : a * 64 + 64, m * 128 : m * 128 + 128] = jnp.where(
                    ok, tile, -jnp.inf
                )
        return c

    lax.fori_loop(0, len(SPECIAL), table, 0)

    @pl.when(z == 0)
    def _():
        kvext[0:TOK] = jnp.zeros((TOK, 128), BF16)

    @pl.when(z == NZ - 1)
    def _():
        kvext[5 * TOK : 6 * TOK] = jnp.zeros((TOK, 128), BF16)

    def m_wait(k, c):
        m_in(k).wait_recv()
        return c

    phase("m_wait")
    lax.fori_loop(1, NY * NTP, m_wait, 0)
    phase("mod")
    for t in range(NTP):
        total = mrecv[0, t] + mrecv[1, t] + mrecv[2, t] + mrecv[3, t]
        lo, hi = 256 * t, 256 * t + 128
        mod[0:4, lo : lo + 128] = total[0:4]
        mod[0:4, hi : hi + 128] = total[4:8]
    mod[2:3, :] = mod[5:6, :] * (1.0 + mod[2:3, :])
    mod[3:4, :] = mod[5:6, :] * (1.0 + mod[3:4, :])

    phase("hidden")
    def hidden(rows, which):
        v = lat[rows, :].astype(F32) * rsl[rows, 0:1]
        hid[rows, :] = (v * mod[2 + which : 3 + which, :] + mod[which : 1 + which, :]).astype(BF16)

    def lat_hidden(i, c):
        hidden(pl.ds(pl.multiple_of(i * 32, 32), 32), 0)
        return c

    hidden(pl.ds(TOK, CTXL), 1)
    lax.fori_loop(0, TOK // 32, lat_hidden, 0)
    phase("kv")
    loads[11].wait()
    loads[12].wait()
    kv_all = dot(hid[...], wkv[...])
    kv = kv_all[TOK:]
    for q in range(2):
        kt = kv[:, 128 * q : 128 * q + 128]
        vt = kv[:, 256 + 128 * q : 256 + 128 * q + 128]
        csend[2 * q] = jnp.where(low, kt, half_swap(vt)).astype(BF16)
        csend[2 * q + 1] = jnp.where(low, half_swap(kt), vt).astype(BF16)
    here = pl.ds(pl.multiple_of(sp * CTXL, CTXL), CTXL)
    ctxkv[here, :] = csend[y]

    def c_copy(k):
        d = lax.rem(sp + k, NZ * NY)
        return remote(csend.at[lax.rem(d, NY)], ctxkv.at[here, :], cs.at[d], cr.at[sp], d, tp)

    def c_in(k):
        d = lax.rem(sp + k, NZ * NY)
        there = pl.ds(pl.multiple_of(d * CTXL, CTXL), CTXL)
        return remote(csend.at[y], ctxkv.at[there, :], cs.at[d], cr.at[d], d, tp)

    def c_start(k, c):
        c_copy(k).start()
        return c

    lax.fori_loop(1, NZ * NY, c_start, 0)

    kv = kv_all[:TOK]
    for q in range(2):
        kt = kv[:, 128 * q : 128 * q + 128]
        vt = kv[:, 256 + 128 * q : 256 + 128 * q + 128]
        kvsend[2 * q] = jnp.where(low, kt, half_swap(vt)).astype(BF16)
        kvsend[2 * q + 1] = jnp.where(low, half_swap(kt), vt).astype(BF16)
    mine = pl.ds(pl.multiple_of((1 + y) * TOK, TOK), TOK)
    kvext[mine, :] = kvsend[y]

    def k_copy(k):
        dy = lax.rem(y + k, NY)
        return remote(kvsend.at[dy], kvext.at[mine, :], ks.at[dy], kr.at[y], z * NY + dy, tp)

    def k_in(dy):
        rows = pl.ds(pl.multiple_of((1 + dy) * TOK, TOK), TOK)
        return remote(kvsend.at[y], kvext.at[rows, :], ks.at[dy], kr.at[dy], z * NY + dy, tp)

    for k in (2, 1, 3):
        k_copy(k).start()

    phase("qg")
    loads[13].wait()
    qg = dot(hid[0:TOK, :], wqg[:, 0:TOK])
    for q in range(2):
        qt = qg[:, 128 * q : 128 * q + 128] * (HD**-0.5)
        up, dn = qt[0:128], qt[128:256]
        qsend[2 * q] = jnp.where(low, up, half_swap(dn)).astype(BF16)
        qsend[2 * q + 1] = jnp.where(low, half_swap(up), dn).astype(BF16)
    qrecv[y] = qsend[y]

    def q_copy(k):
        dy = lax.rem(y + k, NY)
        return remote(qsend.at[dy], qrecv.at[y], qs.at[dy], qr.at[y], z * NY + dy, tp)

    def q_in(k):
        dy = lax.rem(y + k, NY)
        return remote(qsend.at[dy], qrecv.at[dy], qs.at[dy], qr.at[dy], z * NY + dy, tp)

    for k in (2, 1, 3):
        q_copy(k).start()
    phase("g")
    loads[14].wait()
    g = dot(hid[0:TOK, :], wqg[:, TOK:]).astype(BF16).astype(F32)
    sg[...] = g * (1.0 / (1.0 + jnp.exp(-g)))

    phase("kq_wait")
    for k in range(1, NZ):
        zg_in(k).wait_recv()
    total = zgrecv[0]
    for k in range(1, NZ):
        total = total + zgrecv[k]
    mgsend[...] = total
    mgrecv[y, tp] = total

    def mg_copy(k):
        g = lax.rem(group + k, NY * NTP)
        dy, dt = lax.div(g, NTP), lax.rem(g, NTP)
        return remote(mgsend, mgrecv.at[y, tp], mgs.at[g], mgr.at[group], z * NY + dy, dt)

    def mg_in(k):
        g = lax.rem(group + k, NY * NTP)
        dy, dt = lax.div(g, NTP), lax.rem(g, NTP)
        return remote(mgsend, mgrecv.at[dy, dt], mgs.at[g], mgr.at[g], z * NY + dy, dt)

    def mg_start(k, c):
        mg_copy(k).start()
        return c

    lax.fori_loop(1, NY * NTP, mg_start, 0)

    up_src = kvext.at[pl.ds(4 * TOK, TOK), :]
    dn_src = kvext.at[pl.ds(TOK, TOK), :]
    up_dst = kvext.at[pl.ds(0, TOK), :]
    dn_dst = kvext.at[pl.ds(5 * TOK, TOK), :]
    up_copy = remote(up_src, up_dst, hs.at[0], hr.at[0], jnp.minimum(z + 1, NZ - 1) * NY + y, tp)
    dn_copy = remote(dn_src, dn_dst, hs.at[1], hr.at[1], jnp.maximum(z - 1, 0) * NY + y, tp)

    @pl.when(y != 3)
    def _():
        k_in(3).wait_recv()

    @pl.when(z < NZ - 1)
    def _():
        up_copy.start()

    @pl.when(y != 0)
    def _():
        k_in(0).wait_recv()

    @pl.when(z > 0)
    def _():
        dn_copy.start()

    @pl.when(y != 1)
    def _():
        k_in(1).wait_recv()

    @pl.when(y != 2)
    def _():
        k_in(2).wait_recv()

    for k in (1, 2, 3):
        q_in(k).wait_recv()

    phase("c_wait")
    def c_wait(k, c):
        c_in(k).wait_recv()
        return c

    lax.fori_loop(1, NZ * NY, c_wait, 0)

    phase("h_wait")
    @pl.when(z > 0)
    def _():
        up_copy.wait_recv()

    @pl.when(z < NZ - 1)
    def _():
        dn_copy.wait_recv()

    phase("attention")
    def r_copy(dy):
        return remote(rsend.at[dy], rrecv.at[y], rs.at[dy], rr.at[y], z * NY + dy, tp)

    def r_in(dy):
        return remote(rsend.at[dy], rrecv.at[dy], rs.at[dy], rr.at[dy], z * NY + dy, tp)

    def block(k, c):
        b = lax.rem(y + k, NY)
        xq = qrecv[b].astype(F32)
        outs = []
        for a in range(2):
            p = 2 * b + a
            xa = xq if a == 0 else half_swap(xq)
            qp = jnp.where(low, xa, 0.0).astype(BF16)
            base = jnp.clip(row0 + 2 * p - 4, 0, LAST_START) - row0 + 4
            rows = pl.ds(pl.multiple_of(base * GRID_W, GRID_W), 10 * GRID_W)
            t = jnp.where(p < 2, p, jnp.where(p < 6, 2, p - 3))
            sc_ctx = dot_nt(qp, ctxkv[...])
            kvw = kvext[rows, :]
            sc_win = dot_nt(qp, kvw) + btab[t]
            top = jnp.maximum(
                jnp.max(sc_ctx, axis=1, keepdims=True), jnp.max(sc_win, axis=1, keepdims=True)
            )
            e_ctx = jnp.exp(sc_ctx - top)
            e_win = jnp.exp(sc_win - top)
            den = jnp.sum(e_ctx, axis=1, keepdims=True) + jnp.sum(e_win, axis=1, keepdims=True)
            o = dot(e_ctx.astype(BF16), ctxkv[...]) + dot(e_win.astype(BF16), kvw)
            outs.append(o * (1.0 / den))
        rsend[b] = jnp.where(low, half_swap(outs[0]), outs[1]).astype(BF16)

        @pl.when(k < NY)
        def _():
            r_copy(b).start()

        @pl.when(k == NY)
        def _():
            rrecv[b] = rsend[b]

        return c

    lax.fori_loop(1, NY + 1, block, 0)
    phase("r_wait")
    for k in (1, 2, 3):
        r_in(lax.rem(y + k, NY)).wait_recv()

    phase("gate")
    for q in range(2):
        x0, x1 = rrecv[2 * q].astype(F32), rrecv[2 * q + 1].astype(F32)
        up = jnp.where(low, x0, half_swap(x1)) * sg[0:128, 128 * q : 128 * q + 128]
        dn = jnp.where(low, half_swap(x0), x1) * sg[128:256, 128 * q : 128 * q + 128]
        cols = slice(128 * q, 128 * q + 128)
        for i in range(2):
            for h in range(2):
                lo = 64 * i + 32 * h
                gated[i, h, :, cols] = up[lo : lo + 32].astype(BF16)
                gated[2 + i, h, :, cols] = dn[lo : lo + 32].astype(BF16)
    g_copy = remote(gated.at[:, 1 - core], grecv, gs, gr, sp, partner)
    g_copy.start()
    phase("g_wait")
    w_copy.wait_recv()
    g_copy.wait_recv()
    phase("project")
    g_own = gated[:, core].reshape(NX * OUTR, TOK)
    g_other = grecv[...].reshape(NX * OUTR, TOK)
    for n in range(4):
        cols = slice(512 * n, 512 * n + 512)
        term = dot(g_own, wo[:, cols]) + dot(g_other, wo2[:, cols])
        psend[:, :, cols] = term.reshape(NX, OUTR, 512).astype(BF16)

    def p_copy(k):
        dx = lax.rem(x + k, NX)
        return remote(psend.at[dx], precv.at[x], ps.at[dx], pr.at[x], sp, dx * NC + core)

    def p_in(k):
        dx = lax.rem(x + k, NX)
        return remote(psend.at[dx], precv.at[dx], ps.at[dx], pr.at[dx], sp, dx * NC + core)

    for k in (2, 1, 3):
        p_copy(k).start()
    phase("sent1")
    for k in range(1, NZ):
        z_copy(k).wait_send()
        zg_copy(k).wait_send()

    def sent(k, c):
        m_copy(k).wait_send()
        mg_copy(k).wait_send()
        c_copy(k).wait_send()
        mg_in(k).wait_recv()
        return c

    lax.fori_loop(1, NY * NTP, sent, 0)
    w_copy.wait_send()
    g_copy.wait_send()
    for k in (1, 2, 3):
        k_copy(k).wait_send()
        q_copy(k).wait_send()
        r_copy(lax.rem(y + k, NY)).wait_send()

    @pl.when(z < NZ - 1)
    def _():
        up_copy.wait_send()

    @pl.when(z > 0)
    def _():
        dn_copy.wait_send()

    for t in range(NTP):
        total = mgrecv[0, t] + mgrecv[1, t] + mgrecv[2, t] + mgrecv[3, t]
        mod[4:5, 256 * t : 256 * t + 128] = total[0:1]
        mod[4:5, 256 * t + 128 : 256 * t + 256] = total[1:2]
    phase("p_wait1")
    p_in(1).wait_recv()
    phase("p_wait3")
    p_in(3).wait_recv()
    phase("p_wait2")
    p_in(2).wait_recv()
    phase("final")
    branch = psend[x].astype(F32)
    for k in (1, 2, 3):
        branch = branch + precv[lax.rem(x + k, NX)].astype(F32)
    branch = branch.astype(BF16).astype(F32)
    normed = branch * lax.rsqrt(jnp.mean(branch * branch, axis=1, keepdims=True) + EPSILON)
    own = lat[pl.ds(pl.multiple_of(tp * OUTR, OUTR), OUTR), :].astype(F32)
    out_ref[...] = (own + mod[4:5, :] * (normed * mod[6:7, :])).astype(BF16)

    phase("sent")
    for k in (1, 2, 3):
        p_copy(k).wait_send()
    phase(None)


def shards(
    latent,
    context,
    condition,
    context_condition,
    gain_pre,
    gain_post,
    w_shift,
    w_scale,
    w_gate,
    w_query,
    w_key,
    w_value,
    w_silu,
    offset_bias,
    w_out,
):
    in_rows = w_shift.shape[0]
    vmem = pl.BlockSpec(memory_space=pltpu.VMEM)
    hbm = pl.BlockSpec(memory_space=pltpu.HBM)
    dma = pltpu.SemaphoreType.DMA
    return pl.pallas_call(
        kernel,
        name="whole",
        out_shape=jax.ShapeDtypeStruct((OUTR, D), BF16),
        in_specs=[hbm] * 15,
        out_specs=vmem,
        scratch_shapes=[
            pltpu.VMEM((2, 16, 128), BF16),
            pltpu.VMEM((2, 16, 128), F32),
            pltpu.VMEM((2, 16, 128), F32),
            pltpu.VMEM((2 * WIN_ROWS - 1, NY, 2 * WIN_COLS - 1), F32),
            pltpu.VMEM((16, 128), F32),
            pltpu.VMEM((3, in_rows, TOK), BF16),
            pltpu.VMEM((TOK + CTXL, D), BF16),
            pltpu.VMEM((D, 2 * TOK), BF16),
            pltpu.VMEM((D, 2 * TOK), BF16),
            pltpu.VMEM((TOK, D), BF16),
            pltpu.VMEM((TOK, D), BF16),
            pltpu.VMEM((8, 128), F32),
            pltpu.VMEM((NZ, 8, 128), F32),
            pltpu.VMEM((8, 128), F32),
            pltpu.VMEM((NY, NTP, 8, 128), F32),
            pltpu.VMEM((2, 128), F32),
            pltpu.VMEM((NZ, 2, 128), F32),
            pltpu.VMEM((2, 128), F32),
            pltpu.VMEM((NY, NTP, 2, 128), F32),
            pltpu.VMEM((8, D), F32),
            pltpu.VMEM((len(SPECIAL), 128, 640), F32),
            pltpu.VMEM((TOK + CTXL, D), BF16),
            pltpu.VMEM((TOK + CTXL, 128), F32),
            pltpu.VMEM((NY, CTXL, 128), BF16),
            pltpu.VMEM((CTX, 128), BF16),
            pltpu.VMEM((NY, TOK, 128), BF16),
            pltpu.VMEM((6 * TOK, 128), BF16),
            pltpu.VMEM((NY, 128, 128), BF16),
            pltpu.VMEM((NY, 128, 128), BF16),
            pltpu.VMEM((TOK, TOK), F32),
            pltpu.VMEM((NY, 128, 128), BF16),
            pltpu.VMEM((NY, 128, 128), BF16),
            pltpu.VMEM((NX, NC, OUTR, TOK), BF16),
            pltpu.VMEM((NX, OUTR, TOK), BF16),
            pltpu.VMEM((NX, OUTR, D), BF16),
            pltpu.VMEM((NX, OUTR, D), BF16),
            dma((15,)),
            dma((NZ,)),
            dma((NZ,)),
            dma((NY * NTP,)),
            dma((NY * NTP,)),
            dma((NZ,)),
            dma((NZ,)),
            dma((NY * NTP,)),
            dma((NY * NTP,)),
            dma,
            dma,
            dma((NZ * NY,)),
            dma((NZ * NY,)),
            dma((NY,)),
            dma((NY,)),
            dma((NY,)),
            dma((NY,)),
            dma((2,)),
            dma((2,)),
            dma((NY,)),
            dma((NY,)),
            dma,
            dma,
            dma((NX,)),
            dma((NX,)),
        ],
        compiler_params=pltpu.CompilerParams(
            collective_id=0, has_side_effects=True, vmem_limit_bytes=67043328
        ),
    )(
        condition.reshape(16, 128),
        context_condition.reshape(16, 128),
        gain_pre.reshape(16, 128),
        gain_post.reshape(16, 128),
        jnp.transpose(offset_bias, (1, 0, 2)),
        latent,
        context,
        w_shift,
        w_scale,
        w_gate,
        w_query,
        w_key,
        w_value,
        w_silu,
        w_out,
    )


def solution(mesh):
    in_specs = (
        P("sp", None),
        P("sp", None),
        P(),
        P(),
        P(),
        P(),
        P("sp", "tp"),
        P("sp", "tp"),
        P("sp", "tp"),
        P(None, "tp"),
        P(None, "tp"),
        P(None, "tp"),
        P(None, "tp"),
        P("tp", None, None),
        P("tp", None),
    )
    out_specs = P(("sp", "tp"), None)
    return jax.shard_map(shards, mesh=mesh, in_specs=in_specs, out_specs=out_specs, check_vma=False)
```

```python
import functools

import jax
import jax.numpy as jnp
from jax import lax
from jax.experimental import pallas as pl
from jax.experimental.pallas import tpu as pltpu
from jax.sharding import PartitionSpec as P

GRID_W = 64
WIN_ROWS = 8
WIN_COLS = 16
EPSILON = 1e-06
NZ, NY, NX, NC = 8, 4, 4, 2
NTP = NX * NC
D = 2048
HD = 64
TOK = 256
CTXL = 32
CTX = 1024
OUTR = TOK // NTP
LAST_START = NZ * NY * TOK // GRID_W - WIN_ROWS
SPECIAL = (0, 1, 2, 6, 7)
F32 = jnp.float32
BF16 = jnp.bfloat16
NT = (((1,), (1,)), ((), ()))


def dot(a, b):
    return jnp.dot(a, b, preferred_element_type=F32)


def dot_nt(a, b):
    return lax.dot_general(a, b, NT, preferred_element_type=F32)


def remote(src, dst, ssem, rsem, sp, tp):
    return pltpu.make_async_remote_copy(
        src_ref=src,
        dst_ref=dst,
        send_sem=ssem,
        recv_sem=rsem,
        device_id=(sp, tp),
        device_id_type=pl.DeviceIdType.MESH,
    )


class Phases:
    def __init__(self):
        self.scope = None

    def __call__(self, name):
        if self.scope is not None:
            self.scope.__exit__(None, None, None)
        self.scope = None
        if name:
            self.scope = jax.named_scope(name)
            self.scope.__enter__()


def drain(ref, sem):
    pltpu.make_async_copy(ref, ref, sem).wait()


def half_swap(v):
    return pltpu.roll(v, 64, 1)


def kernel(
    cond_h,
    cond2_h,
    gpre_h,
    gpost_h,
    bias_h,
    lat_h,
    ctx_h,
    wsh_h,
    wsc_h,
    wga_h,
    wq_h,
    wk_h,
    wv_h,
    wg_h,
    wo_h,
    out_ref,
    conds,
    condf,
    gains,
    bias,
    biasx,
    wmod,
    lat,
    wkv,
    wqg,
    wo,
    wo2,
    zsend,
    zrecv,
    msend,
    mrecv,
    zgsend,
    zgrecv,
    mgsend,
    mgrecv,
    mod,
    btab,
    hid,
    rsl,
    csend,
    ctxkv,
    kvsend,
    kvext,
    qsend,
    qrecv,
    gbuf,
    gother,
    sgate,
    rsend,
    rrecv,
    gated,
    psend,
    precv,
    lsem,
    zs,
    zr,
    ms,
    mr,
    zgs,
    zgr,
    mgs,
    mgr,
    ws,
    wr,
    cs,
    cr,
    ks,
    kr,
    qs,
    qr,
    hs,
    hr,
    rs,
    rr,
    gs,
    gr,
    ps,
    pr,
):
    sp = lax.axis_index("sp")
    tp = lax.axis_index("tp")
    z, y = lax.div(sp, NY), lax.rem(sp, NY)
    x, core = lax.div(tp, NC), lax.rem(tp, NC)
    partner = x * NC + (1 - core)
    group = y * NTP + tp
    lane = lax.broadcasted_iota(jnp.int32, (1, 128), 1)
    low = lane < 64

    phase = Phases()
    phase("loads")
    def load(sem, *moves):
        for a, b in moves:
            pltpu.make_async_copy(a, b, lsem.at[sem]).start()

    load(0, (cond_h, conds.at[0]), (cond2_h, conds.at[1]))
    load(1, (wsh_h, wmod.at[0]), (wsc_h, wmod.at[1]), (wga_h, wmod.at[2]))
    load(2, (ctx_h, lat.at[pl.ds(TOK, CTXL), :]), (lat_h, lat.at[pl.ds(0, TOK), :]))
    load(3, (gpre_h, gains.at[0]), (gpost_h, gains.at[1]))
    load(4, (bias_h, bias))
    load(5, (wo_h, wo))
    load(6, (wk_h, wkv.at[:, pl.ds(0, TOK)]), (wv_h, wkv.at[:, pl.ds(TOK, TOK)]))
    load(7, (wq_h, wqg.at[:, pl.ds(0, TOK)]), (wg_h, wqg.at[:, pl.ds(TOK, TOK)]))

    phase("greet")
    barrier = pltpu.get_barrier_semaphore()

    def greet(dsp, dtp):
        pl.semaphore_signal(
            barrier, inc=1, device_id=(dsp, dtp), device_id_type=pl.DeviceIdType.MESH
        )

    def greet_z(k, c):
        greet(lax.rem(z + k, NZ) * NY + y, tp)
        return c

    def greet_g(k, c):
        g = lax.rem(group + k, NY * NTP)
        greet(z * NY + lax.div(g, NTP), lax.rem(g, NTP))
        return c

    lax.fori_loop(1, NZ, greet_z, 0)
    lax.fori_loop(1, NY * NTP, greet_g, 0)

    phase("partial")
    drain(conds, lsem.at[0])
    v = conds[...].astype(F32)
    condf[...] = v * (1.0 / (1.0 + jnp.exp(-v)))
    line = jnp.concatenate([condf[i, pl.ds(lax.div(sp, 2), 1), :] for i in range(2)], axis=0)
    line = jnp.where(lax.rem(sp, 2) == 1, half_swap(line), line)[:, :64]
    act = jnp.concatenate([line, jnp.zeros((6, 64), F32)], axis=0).astype(BF16)
    drain(wmod, lsem.at[1])
    sh = dot(act, wmod[0])
    sc = dot(act, wmod[1])
    ga = dot(act, wmod[2])
    zsend[0:2] = sh[0:2, :128]
    zsend[2:4] = sc[0:2, :128]
    zsend[4:6] = sh[0:2, 128:]
    zsend[6:8] = sc[0:2, 128:]
    zgsend[0:1] = ga[0:1, :128]
    zgsend[1:2] = ga[0:1, 128:]
    zrecv[z] = zsend[...]
    zgrecv[z] = zgsend[...]

    phase("barrier")
    pl.semaphore_wait(barrier, NZ - 1 + NY * NTP - 1)

    phase("z_start")
    def z_copy(k):
        dz = lax.rem(z + k, NZ)
        return remote(zsend, zrecv.at[z], zs, zr, dz * NY + y, tp)

    def zg_copy(k):
        dz = lax.rem(z + k, NZ)
        return remote(zgsend, zgrecv.at[z], zgs, zgr, dz * NY + y, tp)

    far_first = (4, 3, 5, 2, 6, 1, 7)
    for k in far_first:
        z_copy(k).start()
    for k in far_first:
        zg_copy(k).start()

    phase("stats")
    w_copy = remote(wo, wo2, ws, wr, sp, partner)

    drain(lat, lsem.at[2])

    def row_stats(i, c):
        rows = pl.ds(pl.multiple_of(i * 32, 32), 32)
        v = lat[rows, :].astype(F32)
        r = lax.rsqrt(jnp.mean(v * v, axis=1, keepdims=True) + EPSILON)
        rsl[rows, :] = jnp.broadcast_to(r, (32, 128))
        return c

    lax.fori_loop(0, (TOK + CTXL) // 32, row_stats, 0)
    drain(gains, lsem.at[3])
    for t in range(16):
        mod[5:6, 128 * t : 128 * t + 128] = gains[0, t : t + 1, :]
        mod[6:7, 128 * t : 128 * t + 128] = gains[1, t : t + 1, :]
    drain(bias, lsem.at[4])
    biasx[...] = jnp.zeros((16, 128), F32)
    for d in range(2 * WIN_ROWS - 1):
        line = bias[d, pl.ds(y, 1), :]
        biasx[d : d + 1, 0:31] = line
        if d > 0:
            biasx[d - 1 : d, 64:95] = line
    drain(wo, lsem.at[5])

    phase("z_wait")
    drain(zrecv.at[pl.ds(0, NZ - 1)], zr)
    phase("m_start")
    total = zrecv[0]
    for k in range(1, NZ):
        total = total + zrecv[k]
    msend[...] = total
    mrecv[group] = total

    def m_copy(k):
        g = lax.rem(group + k, NY * NTP)
        dy, dt = lax.div(g, NTP), lax.rem(g, NTP)
        return remote(msend, mrecv.at[group], ms, mr, z * NY + dy, dt)

    def m_start(k, c):
        m_copy(k).start()
        return c

    lax.fori_loop(1, NY * NTP, m_start, 0)
    w_copy.start()

    phase("tables")
    col = lax.rem(lax.broadcasted_iota(jnp.int32, (64, 128), 1), 64)
    right = lax.div(lax.broadcasted_iota(jnp.int32, (64, 128), 1), 64)
    qcol = lax.broadcasted_iota(jnp.int32, (64, 128), 0)
    first_col = jnp.clip(qcol - WIN_COLS // 2, 0, GRID_W - WIN_COLS)
    in_cols = (col >= first_col) & (col < first_col + WIN_COLS)
    row0 = z * 16

    def table(t, c):
        p = jnp.where(t < 3, t, t + 3)
        base = jnp.clip(row0 + 2 * p - 4, 0, LAST_START)
        for a in range(2):
            row = row0 + 2 * p + a
            off = jnp.clip(row - 4, 0, LAST_START) - base
            d0 = base - row + 7
            for m in range(5):
                line = biasx[pl.ds(d0 + 2 * m, 1), :]
                tile = pltpu.roll(
                    jnp.broadcast_to(line, (64, 128)), 113, 1, stride=1, stride_axis=0
                )
                krow = right + 2 * m
                ok = in_cols & (krow >= off) & (krow < off + WIN_ROWS)
                btab[t, a * 64 : a * 64 + 64, m * 128 : m * 128 + 128] = jnp.where(
                    ok, tile, -jnp.inf
                )
        return c

    lax.fori_loop(0, len(SPECIAL), table, 0)

    @pl.when(z == 0)
    def _():
        kvext[0:TOK] = jnp.zeros((TOK, 128), BF16)

    @pl.when(z == NZ - 1)
    def _():
        kvext[5 * TOK : 6 * TOK] = jnp.zeros((TOK, 128), BF16)

    phase("m_wait")
    drain(mrecv.at[pl.ds(0, NY * NTP - 1)], mr)
    phase("mod")
    for t in range(NTP):
        total = mrecv[t] + mrecv[NTP + t] + mrecv[2 * NTP + t] + mrecv[3 * NTP + t]
        lo, hi = 256 * t, 256 * t + 128
        mod[0:4, lo : lo + 128] = total[0:4]
        mod[0:4, hi : hi + 128] = total[4:8]
    mod[2:3, :] = mod[5:6, :] * (1.0 + mod[2:3, :])
    mod[3:4, :] = mod[5:6, :] * (1.0 + mod[3:4, :])

    phase("hidden")
    def hidden(rows, which):
        v = lat[rows, :].astype(F32) * rsl[rows, 0:1]
        hid[rows, :] = (v * mod[2 + which : 3 + which, :] + mod[which : 1 + which, :]).astype(BF16)

    def lat_hidden(i, c):
        hidden(pl.ds(pl.multiple_of(i * 32, 32), 32), 0)
        return c

    hidden(pl.ds(TOK, CTXL), 1)
    lax.fori_loop(0, TOK // 32, lat_hidden, 0)
    phase("kv")
    drain(wkv, lsem.at[6])
    kv_all = dot(hid[...], wkv[...])
    kv = kv_all[TOK:]
    for q in range(2):
        kt = kv[:, 128 * q : 128 * q + 128]
        vt = kv[:, 256 + 128 * q : 256 + 128 * q + 128]
        csend[2 * q] = jnp.where(low, kt, half_swap(vt)).astype(BF16)
        csend[2 * q + 1] = jnp.where(low, half_swap(kt), vt).astype(BF16)
    here = pl.ds(pl.multiple_of(sp * CTXL, CTXL), CTXL)
    ctxkv[here, :] = csend[y]

    def c_copy(k):
        d = lax.rem(sp + k, NZ * NY)
        return remote(csend.at[lax.rem(d, NY)], ctxkv.at[here, :], cs, cr, d, tp)

    def c_start(k, c):
        c_copy(k).start()
        return c

    lax.fori_loop(1, NZ * NY, c_start, 0)

    kv = kv_all[:TOK]
    for q in range(2):
        kt = kv[:, 128 * q : 128 * q + 128]
        vt = kv[:, 256 + 128 * q : 256 + 128 * q + 128]
        kvsend[2 * q] = jnp.where(low, kt, half_swap(vt)).astype(BF16)
        kvsend[2 * q + 1] = jnp.where(low, half_swap(kt), vt).astype(BF16)
    mine = pl.ds(pl.multiple_of((1 + y) * TOK, TOK), TOK)
    kvext[mine, :] = kvsend[y]

    def k_copy(k):
        dy = lax.rem(y + k, NY)
        return remote(kvsend.at[dy], kvext.at[mine, :], ks, kr.at[y], z * NY + dy, tp)

    def k_in(dy):
        rows = pl.ds(pl.multiple_of((1 + dy) * TOK, TOK), TOK)
        return remote(kvsend.at[y], kvext.at[rows, :], ks, kr.at[dy], z * NY + dy, tp)

    for k in (2, 1, 3):
        k_copy(k).start()

    phase("qg")
    drain(wqg, lsem.at[7])
    qg = dot(hid[0:TOK, :], wqg[:, 0:TOK])
    for q in range(2):
        qt = qg[:, 128 * q : 128 * q + 128] * (HD**-0.5)
        up, dn = qt[0:128], qt[128:256]
        qsend[2 * q] = jnp.where(low, up, half_swap(dn)).astype(BF16)
        qsend[2 * q + 1] = jnp.where(low, half_swap(up), dn).astype(BF16)
    qrecv[y] = qsend[y]

    def q_copy(k):
        dy = lax.rem(y + k, NY)
        return remote(qsend.at[dy], qrecv.at[y], qs, qr, z * NY + dy, tp)

    for k in (2, 1, 3):
        q_copy(k).start()
    phase("g")
    g = dot(hid[0:TOK, :], wqg[:, TOK:])
    gbuf[...] = g.astype(BF16).reshape(NX, NC, OUTR, TOK)
    g_copy = remote(gbuf.at[:, 1 - core], gother, gs, gr, sp, partner)
    g_copy.start()

    phase("kq_wait")
    drain(zgrecv.at[pl.ds(0, NZ - 1)], zgr)
    total = zgrecv[0]
    for k in range(1, NZ):
        total = total + zgrecv[k]
    mgsend[...] = total
    mgrecv[group] = total

    def mg_copy(k):
        g = lax.rem(group + k, NY * NTP)
        dy, dt = lax.div(g, NTP), lax.rem(g, NTP)
        return remote(mgsend, mgrecv.at[group], mgs, mgr, z * NY + dy, dt)

    def mg_start(k, c):
        mg_copy(k).start()
        return c

    lax.fori_loop(1, NY * NTP, mg_start, 0)

    up_src = kvext.at[pl.ds(4 * TOK, TOK), :]
    dn_src = kvext.at[pl.ds(TOK, TOK), :]
    up_dst = kvext.at[pl.ds(0, TOK), :]
    dn_dst = kvext.at[pl.ds(5 * TOK, TOK), :]
    up_copy = remote(up_src, up_dst, hs.at[0], hr.at[0], jnp.minimum(z + 1, NZ - 1) * NY + y, tp)
    dn_copy = remote(dn_src, dn_dst, hs.at[1], hr.at[1], jnp.maximum(z - 1, 0) * NY + y, tp)

    @pl.when(y != 3)
    def _():
        k_in(3).wait_recv()

    @pl.when(z < NZ - 1)
    def _():
        up_copy.start()

    @pl.when(y != 0)
    def _():
        k_in(0).wait_recv()

    @pl.when(z > 0)
    def _():
        dn_copy.start()

    @pl.when(y != 1)
    def _():
        k_in(1).wait_recv()

    @pl.when(y != 2)
    def _():
        k_in(2).wait_recv()

    phase("gates")
    g_copy.wait_recv()
    for part in range(2):
        g = (gbuf[:, core] if part == 0 else gother[...]).astype(F32)
        sgate[:, :, TOK * part : TOK * part + TOK] = g * (1.0 / (1.0 + jnp.exp(-g)))
    phase("q_wait")
    drain(qrecv.at[pl.ds(0, NY - 1)], qr)
    phase("c_wait")
    drain(ctxkv.at[pl.ds(0, CTX - CTXL)], cr)
    phase("h_wait")
    @pl.when(z > 0)
    def _():
        up_copy.wait_recv()

    @pl.when(z < NZ - 1)
    def _():
        dn_copy.wait_recv()

    phase("attention")
    first = 1 - lax.div(x, 2)
    beside = x + 1 - 2 * lax.rem(x, 2)
    source = core * NY + y

    def r_copy(a, b, h):
        return remote(
            rsend.at[a, b, h], rrecv.at[a, source], rs, rr.at[a], z * NY + b, x * NC + h
        )

    def pair(a, k):
        b = lax.rem(y + k, NY)
        p = 2 * b + a
        xq = qrecv[b].astype(F32)
        qp = jnp.where(low, jnp.where(a == 1, half_swap(xq), xq), 0.0).astype(BF16)
        base = jnp.clip(row0 + 2 * p - 4, 0, LAST_START) - row0 + 4
        rows = pl.ds(pl.multiple_of(base * GRID_W, GRID_W), 10 * GRID_W)
        t = jnp.where(p < 2, p, jnp.where(p < 6, 2, p - 3))
        sc_ctx = dot_nt(qp, ctxkv[...])
        kvw = kvext[rows, :]
        sc_win = dot_nt(qp, kvw) + btab[t]
        top = jnp.maximum(
            jnp.max(sc_ctx, axis=1, keepdims=True), jnp.max(sc_win, axis=1, keepdims=True)
        )
        e_ctx = jnp.exp(sc_ctx - top)
        e_win = jnp.exp(sc_win - top)
        den = jnp.sum(e_ctx, axis=1, keepdims=True) + jnp.sum(e_win, axis=1, keepdims=True)
        o = dot(e_ctx.astype(BF16), ctxkv[...]) + dot(e_win.astype(BF16), kvw)
        o = o * (1.0 / den)
        for h in range(NC):
            r0, r1 = o[OUTR * h : OUTR * h + OUTR], o[64 + OUTR * h : 64 + OUTR * h + OUTR]
            rsend[a, b, h] = jnp.where(low, half_swap(r0), r1).astype(BF16)

    def send_back(a, k):
        b = lax.rem(y + k, NY)
        for h in range(NC):
            r_copy(a, b, h).start()

    def far_pairs(a):
        pair(a, 1)
        pair(a, 2)
        send_back(a, 1)
        send_back(a, 2)

    def near_pairs(a):
        pair(a, 3)
        pair(a, 0)
        send_back(a, 3)
        r_copy(a, y, 1 - core).start()
        rrecv[a, source] = rsend[a, y, core]

    def p_copy(i):
        return remote(psend.at[i], precv.at[x], ps, pr, sp, i * NC + core)

    def finish(a):
        phase("r_wait")
        drain(rrecv.at[a, pl.ds(0, NC * NY - 1)], rr.at[a])
        phase("project")
        for part in range(2):
            src = (core if part == 0 else 1 - core) * NY
            for q in range(2):
                x0, x1 = rrecv[a, src + 2 * q].astype(F32), rrecv[a, src + 2 * q + 1].astype(F32)
                cols = slice(TOK * part + 128 * q, TOK * part + 128 * q + 128)
                up = jnp.where(low, x0, half_swap(x1)) * sgate[2 * a, :, cols]
                dn = jnp.where(low, half_swap(x0), x1) * sgate[2 * a + 1, :, cols]
                gated[0:OUTR, cols] = up.astype(BF16)
                gated[OUTR : 2 * OUTR, cols] = dn.astype(BF16)
        for n in range(4):
            cols = slice(512 * n, 512 * n + 512)
            term = dot(gated[:, :TOK], wo[:, cols]) + dot(gated[:, TOK:], wo2[:, cols])
            psend[2 * a, :, cols] = term[:OUTR].astype(BF16)
            psend[2 * a + 1, :, cols] = term[OUTR:].astype(BF16)

    far_pairs(first)
    near_pairs(first)
    phase("attention2")
    far_pairs(1 - first)
    near_pairs(1 - first)
    phase("w_wait")
    w_copy.wait_recv()
    finish(first)
    p_copy(lax.rem(x + 2, NX)).start()
    p_copy(lax.rem(beside + 2, NX)).start()
    finish(1 - first)
    p_copy(beside).start()

    phase("sent1")
    drain(zrecv.at[pl.ds(0, NZ - 1)], zs)
    drain(zgrecv.at[pl.ds(0, NZ - 1)], zgs)
    drain(mrecv.at[pl.ds(0, NY * NTP - 1)], ms)
    drain(mgrecv.at[pl.ds(0, NY * NTP - 1)], mgs)
    drain(mgrecv.at[pl.ds(0, NY * NTP - 1)], mgr)
    drain(ctxkv.at[pl.ds(0, CTX - CTXL)], cs)
    drain(kvext.at[pl.ds(0, (NY - 1) * TOK)], ks)
    drain(qrecv.at[pl.ds(0, NY - 1)], qs)
    w_copy.wait_send()
    g_copy.wait_send()
    for a in range(2):
        drain(rrecv.at[a, pl.ds(0, NC * NY - 1)], rs)

    @pl.when(z < NZ - 1)
    def _():
        up_copy.wait_send()

    @pl.when(z > 0)
    def _():
        dn_copy.wait_send()

    for t in range(NTP):
        total = mgrecv[t] + mgrecv[NTP + t] + mgrecv[2 * NTP + t] + mgrecv[3 * NTP + t]
        mod[4:5, 256 * t : 256 * t + 128] = total[0:1]
        mod[4:5, 256 * t + 128 : 256 * t + 256] = total[1:2]
    phase("p_wait")
    drain(precv.at[pl.ds(0, NX - 1)], pr)
    phase("final")
    branch = psend[x].astype(F32)
    for k in (1, 2, 3):
        branch = branch + precv[lax.rem(x + k, NX)].astype(F32)
    branch = branch.astype(BF16).astype(F32)
    normed = branch * lax.rsqrt(jnp.mean(branch * branch, axis=1, keepdims=True) + EPSILON)
    own = lat[pl.ds(pl.multiple_of(tp * OUTR, OUTR), OUTR), :].astype(F32)
    out_ref[...] = (own + mod[4:5, :] * (normed * mod[6:7, :])).astype(BF16)

    phase("sent")
    drain(precv.at[pl.ds(0, NX - 1)], ps)
    phase(None)


def shards(
    latent,
    context,
    condition,
    context_condition,
    gain_pre,
    gain_post,
    w_shift,
    w_scale,
    w_gate,
    w_query,
    w_key,
    w_value,
    w_silu,
    offset_bias,
    w_out,
):
    in_rows = w_shift.shape[0]
    vmem = pl.BlockSpec(memory_space=pltpu.VMEM)
    hbm = pl.BlockSpec(memory_space=pltpu.HBM)
    dma = pltpu.SemaphoreType.DMA
    operands = (
        condition.reshape(16, 128),
        context_condition.reshape(16, 128),
        gain_pre.reshape(16, 128),
        gain_post.reshape(16, 128),
        jnp.transpose(offset_bias, (1, 0, 2)),
        latent,
        context,
        w_shift,
        w_scale,
        w_gate,
        w_query,
        w_key,
        w_value,
        w_silu,
        w_out,
    )
    operands = [pltpu.with_memory_space_constraint(a, pltpu.HBM) for a in operands]
    return pl.pallas_call(
        kernel,
        name="whole",
        out_shape=jax.ShapeDtypeStruct((OUTR, D), BF16),
        in_specs=[hbm] * 15,
        out_specs=vmem,
        scratch_shapes=[
            pltpu.VMEM((2, 16, 128), BF16),
            pltpu.VMEM((2, 16, 128), F32),
            pltpu.VMEM((2, 16, 128), F32),
            pltpu.VMEM((2 * WIN_ROWS - 1, NY, 2 * WIN_COLS - 1), F32),
            pltpu.VMEM((16, 128), F32),
            pltpu.VMEM((3, in_rows, TOK), BF16),
            pltpu.VMEM((TOK + CTXL, D), BF16),
            pltpu.VMEM((D, 2 * TOK), BF16),
            pltpu.VMEM((D, 2 * TOK), BF16),
            pltpu.VMEM((TOK, D), BF16),
            pltpu.VMEM((TOK, D), BF16),
            pltpu.VMEM((8, 128), F32),
            pltpu.VMEM((NZ, 8, 128), F32),
            pltpu.VMEM((8, 128), F32),
            pltpu.VMEM((NY * NTP, 8, 128), F32),
            pltpu.VMEM((2, 128), F32),
            pltpu.VMEM((NZ, 2, 128), F32),
            pltpu.VMEM((2, 128), F32),
            pltpu.VMEM((NY * NTP, 2, 128), F32),
            pltpu.VMEM((8, D), F32),
            pltpu.VMEM((len(SPECIAL), 128, 640), F32),
            pltpu.VMEM((TOK + CTXL, D), BF16),
            pltpu.VMEM((TOK + CTXL, 128), F32),
            pltpu.VMEM((NY, CTXL, 128), BF16),
            pltpu.VMEM((CTX, 128), BF16),
            pltpu.VMEM((NY, TOK, 128), BF16),
            pltpu.VMEM((6 * TOK, 128), BF16),
            pltpu.VMEM((NY, 128, 128), BF16),
            pltpu.VMEM((NY, 128, 128), BF16),
            pltpu.VMEM((NX, NC, OUTR, TOK), BF16),
            pltpu.VMEM((NX, OUTR, TOK), BF16),
            pltpu.VMEM((NX, OUTR, NC * TOK), F32),
            pltpu.VMEM((2, NY, NC, OUTR, 128), BF16),
            pltpu.VMEM((2, NC * NY, OUTR, 128), BF16),
            pltpu.VMEM((2 * OUTR, NC * TOK), BF16),
            pltpu.VMEM((NX, OUTR, D), BF16),
            pltpu.VMEM((NX, OUTR, D), BF16),
            dma((8,)),
            dma,
            dma,
            dma,
            dma,
            dma,
            dma,
            dma,
            dma,
            dma,
            dma,
            dma,
            dma,
            dma,
            dma((NY,)),
            dma,
            dma,
            dma((2,)),
            dma((2,)),
            dma,
            dma((2,)),
            dma,
            dma,
            dma,
            dma,
        ],
        compiler_params=pltpu.CompilerParams(
            collective_id=0, has_side_effects=True, vmem_limit_bytes=48 << 20
        ),
    )(*operands)


def solution(mesh):
    in_specs = (
        P("sp", None),
        P("sp", None),
        P(),
        P(),
        P(),
        P(),
        P("sp", "tp"),
        P("sp", "tp"),
        P("sp", "tp"),
        P(None, "tp"),
        P(None, "tp"),
        P(None, "tp"),
        P(None, "tp"),
        P("tp", None, None),
        P("tp", None),
    )
    out_specs = P(("sp", "tp"), None)
    return jax.shard_map(shards, mesh=mesh, in_specs=in_specs, out_specs=out_specs, check_vma=False)
```

```python
import functools

import jax
import jax.numpy as jnp
from jax import lax
from jax.experimental import pallas as pl
from jax.experimental.pallas import tpu as pltpu
from jax.sharding import PartitionSpec as P

GRID_W = 64
WIN_ROWS = 8
WIN_COLS = 16
EPSILON = 1e-06
NZ, NY, NX, NC = 8, 4, 4, 2
NTP = NX * NC
D = 2048
HD = 64
TOK = 256
CTXL = 32
CTX = 1024
OUTR = TOK // NTP
LAST_START = NZ * NY * TOK // GRID_W - WIN_ROWS
SPECIAL = (0, 1, 2, 6, 7)
F32 = jnp.float32
BF16 = jnp.bfloat16
NT = (((1,), (1,)), ((), ()))


def dot(a, b):
    return jnp.dot(a, b, preferred_element_type=F32)


def dot_nt(a, b):
    return lax.dot_general(a, b, NT, preferred_element_type=F32)


def remote(src, dst, ssem, rsem, sp, tp):
    return pltpu.make_async_remote_copy(
        src_ref=src,
        dst_ref=dst,
        send_sem=ssem,
        recv_sem=rsem,
        device_id=(sp, tp),
        device_id_type=pl.DeviceIdType.MESH,
    )


class Phases:
    def __init__(self):
        self.scope = None

    def __call__(self, name):
        if self.scope is not None:
            self.scope.__exit__(None, None, None)
        self.scope = None
        if name:
            self.scope = jax.named_scope(name)
            self.scope.__enter__()


def drain(ref, sem):
    pltpu.make_async_copy(ref, ref, sem).wait()


def half_swap(v):
    return pltpu.roll(v, 64, 1)


def kernel(
    cond_h,
    cond2_h,
    gpre_h,
    gpost_h,
    bias_h,
    lat_h,
    ctx_h,
    wsh_h,
    wsc_h,
    wga_h,
    wq_h,
    wk_h,
    wv_h,
    wg_h,
    wo_h,
    out_ref,
    conds,
    condf,
    gains,
    bias,
    biasx,
    wmod,
    lat,
    ctx,
    wkv,
    wy,
    wqg,
    wo,
    wo2,
    zsend,
    zrecv,
    msend,
    mrecv,
    zgsend,
    zgrecv,
    mgsend,
    mgrecv,
    mod,
    spread,
    btab,
    hid,
    hidc,
    rsl,
    rsc,
    ctxkv,
    kvsend,
    kvext,
    qsend,
    qrecv,
    gbuf,
    gother,
    sgate,
    rsend,
    rrecv,
    gated,
    psend,
    precv,
    lsem,
    zs,
    zr,
    ms,
    mr,
    zgs,
    zgr,
    mgs,
    mgr,
    xs,
    xr,
    xps,
    xpr,
    ws,
    wr,
    cs,
    cr,
    ks,
    kr,
    qs,
    qr,
    hs,
    hr,
    rs,
    rr,
    gs,
    gr,
    ps,
    pr,
):
    sp = lax.axis_index("sp")
    tp = lax.axis_index("tp")
    z, y = lax.div(sp, NY), lax.rem(sp, NY)
    x, core = lax.div(tp, NC), lax.rem(tp, NC)
    partner = x * NC + (1 - core)
    group = y * NTP + tp
    lane = lax.broadcasted_iota(jnp.int32, (1, 128), 1)
    low = lane < 64

    phase = Phases()
    phase("loads")
    def load(sem, *moves):
        for a, b in moves:
            pltpu.make_async_copy(a, b, lsem.at[sem]).start()

    load(0, (cond_h, conds.at[0]), (cond2_h, conds.at[1]))
    load(1, (wsh_h, wmod.at[0]), (wsc_h, wmod.at[1]), (wga_h, wmod.at[2]))
    half = CTXL // NC
    load(8, *((ctx_h.at[pl.ds(half * h, half), :], ctx.at[y, h]) for h in range(NC)))
    load(2, (lat_h, lat))
    load(3, (gpre_h, gains.at[0]), (gpost_h, gains.at[1]))
    load(4, (bias_h, bias))
    load(5, (wo_h, wo))
    load(6, (wk_h, wkv.at[:, pl.ds(0, TOK)]), (wv_h, wkv.at[:, pl.ds(TOK, TOK)]))
    load(7, (wq_h, wqg.at[:, pl.ds(0, TOK)]), (wg_h, wqg.at[:, pl.ds(TOK, TOK)]))

    phase("greet")
    barrier = pltpu.get_barrier_semaphore()

    def greet(dsp, dtp):
        pl.semaphore_signal(
            barrier, inc=1, device_id=(dsp, dtp), device_id_type=pl.DeviceIdType.MESH
        )

    def greet_z(k, c):
        greet(lax.rem(z + k, NZ) * NY + y, tp)
        return c

    def greet_g(k, c):
        g = lax.rem(group + k, NY * NTP)
        greet(z * NY + lax.div(g, NTP), lax.rem(g, NTP))
        return c

    lax.fori_loop(1, NZ, greet_z, 0)
    lax.fori_loop(1, NY * NTP, greet_g, 0)

    phase("partial")
    drain(conds, lsem.at[0])
    v = conds[...].astype(F32)
    condf[...] = v * (1.0 / (1.0 + jnp.exp(-v)))
    line = jnp.concatenate([condf[i, pl.ds(lax.div(sp, 2), 1), :] for i in range(2)], axis=0)
    line = jnp.where(lax.rem(sp, 2) == 1, half_swap(line), line)[:, :64]
    act = jnp.concatenate([line, jnp.zeros((6, 64), F32)], axis=0).astype(BF16)
    drain(wmod, lsem.at[1])
    sh = dot(act, wmod[0])
    sc = dot(act, wmod[1])
    ga = dot(act, wmod[2])
    zsend[0:2] = sh[0:2, :128]
    zsend[2:4] = sc[0:2, :128]
    zsend[4:6] = sh[0:2, 128:]
    zsend[6:8] = sc[0:2, 128:]
    zgsend[0:1] = ga[0:1, :128]
    zgsend[1:2] = ga[0:1, 128:]
    zrecv[z] = zsend[...]
    zgrecv[z] = zgsend[...]

    phase("barrier")
    pl.semaphore_wait(barrier, NZ - 1 + NY * NTP - 1)

    phase("z_start")
    def z_copy(k):
        dz = lax.rem(z + k, NZ)
        return remote(zsend, zrecv.at[z], zs, zr, dz * NY + y, tp)

    def zg_copy(k):
        dz = lax.rem(z + k, NZ)
        return remote(zgsend, zgrecv.at[z], zgs, zgr, dz * NY + y, tp)

    far_first = (4, 3, 5, 2, 6, 1, 7)
    for k in far_first:
        z_copy(k).start()
    for k in far_first:
        zg_copy(k).start()

    def x_copy(k):
        dy = lax.rem(y + k, NY)
        return remote(ctx.at[y, core], ctx.at[y, core], xs, xr, z * NY + dy, tp)

    def x_pass(k):
        rows = ctx.at[lax.rem(y + k, NY), core]
        return remote(rows, rows, xps, xpr, sp, partner)

    drain(ctx.at[0], lsem.at[8])
    for k in (2, 1, 3):
        x_copy(k).start()

    phase("stats")
    drain(lat, lsem.at[2])

    def stats(v):
        r = lax.rsqrt(jnp.mean(v * v, axis=1, keepdims=True) + EPSILON)
        return jnp.broadcast_to(r, (v.shape[0], 128))

    def row_stats(i, c):
        rows = pl.ds(pl.multiple_of(i * 32, 32), 32)
        rsl[rows, :] = stats(lat[rows, :].astype(F32))
        return c

    lax.fori_loop(0, TOK // 32, row_stats, 0)
    drain(gains, lsem.at[3])
    for t in range(16):
        mod[5:6, 128 * t : 128 * t + 128] = gains[0, t : t + 1, :]
        mod[6:7, 128 * t : 128 * t + 128] = gains[1, t : t + 1, :]
    drain(bias, lsem.at[4])
    biasx[...] = jnp.zeros((16, 128), F32)
    for d in range(2 * WIN_ROWS - 1):
        line = bias[d, pl.ds(y, 1), :]
        biasx[d : d + 1, 0:31] = line
        if d > 0:
            biasx[d - 1 : d, 64:95] = line

    phase("z_wait")
    drain(zrecv.at[pl.ds(0, NZ - 1)], zr)
    phase("m_start")
    total = zrecv[0]
    for k in range(1, NZ):
        total = total + zrecv[k]
    msend[...] = total
    mrecv[group] = total

    def m_copy(k):
        g = lax.rem(group + k, NY * NTP)
        dy, dt = lax.div(g, NTP), lax.rem(g, NTP)
        return remote(msend, mrecv.at[group], ms, mr, z * NY + dy, dt)

    def m_start(k, c):
        m_copy(k).start()
        return c

    lax.fori_loop(1, NY * NTP, m_start, 0)

    phase("tables")
    col = lax.rem(lax.broadcasted_iota(jnp.int32, (64, 128), 1), 64)
    right = lax.div(lax.broadcasted_iota(jnp.int32, (64, 128), 1), 64)
    qcol = lax.broadcasted_iota(jnp.int32, (64, 128), 0)
    first_col = jnp.clip(qcol - WIN_COLS // 2, 0, GRID_W - WIN_COLS)
    in_cols = (col >= first_col) & (col < first_col + WIN_COLS)
    row0 = z * 16

    def table(t, c):
        p = jnp.where(t < 3, t, t + 3)
        base = jnp.clip(row0 + 2 * p - 4, 0, LAST_START)
        for a in range(2):
            row = row0 + 2 * p + a
            off = jnp.clip(row - 4, 0, LAST_START) - base
            d0 = base - row + 7
            for m in range(5):
                line = biasx[pl.ds(d0 + 2 * m, 1), :]
                tile = pltpu.roll(
                    jnp.broadcast_to(line, (64, 128)), 113, 1, stride=1, stride_axis=0
                )
                krow = right + 2 * m
                ok = in_cols & (krow >= off) & (krow < off + WIN_ROWS)
                btab[t, a * 64 : a * 64 + 64, m * 128 : m * 128 + 128] = jnp.where(
                    ok, tile, -jnp.inf
                )
        return c

    lax.fori_loop(0, len(SPECIAL), table, 0)

    @pl.when(z == 0)
    def _():
        kvext[0:TOK] = jnp.zeros((TOK, 128), BF16)

    @pl.when(z == NZ - 1)
    def _():
        kvext[5 * TOK : 6 * TOK] = jnp.zeros((TOK, 128), BF16)

    phase("x_wait")
    drain(ctx.at[pl.ds(0, NY - 1), 0], xr)
    for k in (1, 2, 3):
        x_pass(k).start()

    phase("wy")
    drain(wkv, lsem.at[6])

    def head_columns(i, c):
        rows = pl.ds(pl.multiple_of(i * 256, 256), 256)
        at = 128 * lax.div(y, 2)
        kt = wkv[rows, pl.ds(pl.multiple_of(at, 128), 128)].astype(F32)
        vt = wkv[rows, pl.ds(pl.multiple_of(TOK + at, 128), 128)].astype(F32)
        odd = lax.rem(y, 2) == 1
        wy[rows, :] = jnp.where(
            low, jnp.where(odd, half_swap(kt), kt), jnp.where(odd, vt, half_swap(vt))
        ).astype(BF16)
        return c

    lax.fori_loop(0, D // 256, head_columns, 0)
    phase("x_wait2")
    drain(ctx.at[pl.ds(0, NY - 1), 0], xpr)
    for b in range(NY):
        rows = slice(CTXL * b, CTXL * b + CTXL)
        rsc[rows, :] = stats(ctx[b].reshape(CTXL, D).astype(F32))

    phase("m_wait")
    drain(mrecv.at[pl.ds(0, NY * NTP - 1)], mr)
    phase("mod")
    for t in range(NTP):
        total = mrecv[t] + mrecv[NTP + t] + mrecv[2 * NTP + t] + mrecv[3 * NTP + t]
        lo, hi = 256 * t, 256 * t + 128
        mod[0:4, lo : lo + 128] = total[0:4]
        mod[0:4, hi : hi + 128] = total[4:8]
    mod[2:3, :] = mod[5:6, :] * (1.0 + mod[2:3, :])
    mod[3:4, :] = mod[5:6, :] * (1.0 + mod[3:4, :])

    for i in range(4):
        spread[i] = jnp.broadcast_to(mod[i : i + 1, :], (8, D))

    def hidden(v, r, which):
        n = v.shape[0] // 8
        r = r.reshape(n, 8, 128)
        parts = []
        for t in range(D // 128):
            cols = slice(128 * t, 128 * t + 128)
            u = v[:, cols].astype(F32).reshape(n, 8, 128) * r
            u = u * spread[2 + which, :, cols] + spread[which, :, cols]
            parts.append(u.reshape(8 * n, 128).astype(BF16))
        return jnp.concatenate(parts, axis=1)

    phase("ctx_hidden")
    for b in range(NY):
        rows = slice(CTXL * b, CTXL * b + CTXL)
        hidc[rows, :] = hidden(ctx[b].reshape(CTXL, D), rsc[rows, :], 1)
    phase("ctx_kv")
    here = pl.ds(pl.multiple_of(z * NY * CTXL, NY * CTXL), NY * CTXL)
    ctxkv[here, :] = dot(hidc[...], wy[...]).astype(BF16)

    def c_copy(k):
        dz = lax.rem(z + k, NZ)
        return remote(ctxkv.at[here, :], ctxkv.at[here, :], cs, cr, dz * NY + y, tp)

    for k in far_first:
        c_copy(k).start()

    phase("hidden_kv")
    for i in range(2):
        rows = slice(128 * i, 128 * i + 128)
        for n in range(4):
            r32 = slice(128 * i + 32 * n, 128 * i + 32 * n + 32)
            hid[r32, :] = hidden(lat[r32, :], rsl[r32, :], 0)
        kv = dot(hid[rows, :], wkv[...])
        for q in range(2):
            kt = kv[:, 128 * q : 128 * q + 128]
            vt = kv[:, 256 + 128 * q : 256 + 128 * q + 128]
            kvsend[2 * q, rows] = jnp.where(low, kt, half_swap(vt)).astype(BF16)
            kvsend[2 * q + 1, rows] = jnp.where(low, half_swap(kt), vt).astype(BF16)
    mine = pl.ds(pl.multiple_of((1 + y) * TOK, TOK), TOK)
    kvext[mine, :] = kvsend[y]

    def k_copy(k):
        dy = lax.rem(y + k, NY)
        return remote(kvsend.at[dy], kvext.at[mine, :], ks, kr.at[y], z * NY + dy, tp)

    def k_in(dy):
        rows = pl.ds(pl.multiple_of((1 + dy) * TOK, TOK), TOK)
        return remote(kvsend.at[y], kvext.at[rows, :], ks, kr.at[dy], z * NY + dy, tp)

    for k in (2, 1, 3):
        k_copy(k).start()

    phase("qg")
    drain(wqg, lsem.at[7])
    qg = dot(hid[0:TOK, :], wqg[:, 0:TOK])
    for q in range(2):
        qt = qg[:, 128 * q : 128 * q + 128] * (HD**-0.5)
        up, dn = qt[0:128], qt[128:256]
        qsend[2 * q] = jnp.where(low, up, half_swap(dn)).astype(BF16)
        qsend[2 * q + 1] = jnp.where(low, half_swap(up), dn).astype(BF16)
    qrecv[y] = qsend[y]

    def q_copy(k):
        dy = lax.rem(y + k, NY)
        return remote(qsend.at[dy], qrecv.at[y], qs, qr, z * NY + dy, tp)

    for k in (2, 1, 3):
        q_copy(k).start()
    phase("g")
    g = dot(hid[0:TOK, :], wqg[:, TOK:])
    gbuf[...] = g.astype(BF16).reshape(NX, NC, OUTR, TOK)
    g_copy = remote(gbuf.at[:, 1 - core], gother, gs, gr, sp, partner)
    g_copy.start()
    drain(wo, lsem.at[5])
    w_copy = remote(wo, wo2, ws, wr, sp, partner)
    w_copy.start()

    phase("kq_wait")
    drain(zgrecv.at[pl.ds(0, NZ - 1)], zgr)
    total = zgrecv[0]
    for k in range(1, NZ):
        total = total + zgrecv[k]
    mgsend[...] = total
    mgrecv[group] = total

    def mg_copy(k):
        g = lax.rem(group + k, NY * NTP)
        dy, dt = lax.div(g, NTP), lax.rem(g, NTP)
        return remote(mgsend, mgrecv.at[group], mgs, mgr, z * NY + dy, dt)

    def mg_start(k, c):
        mg_copy(k).start()
        return c

    lax.fori_loop(1, NY * NTP, mg_start, 0)

    up_src = kvext.at[pl.ds(4 * TOK, TOK), :]
    dn_src = kvext.at[pl.ds(TOK, TOK), :]
    up_dst = kvext.at[pl.ds(0, TOK), :]
    dn_dst = kvext.at[pl.ds(5 * TOK, TOK), :]
    up_copy = remote(up_src, up_dst, hs.at[0], hr.at[0], jnp.minimum(z + 1, NZ - 1) * NY + y, tp)
    dn_copy = remote(dn_src, dn_dst, hs.at[1], hr.at[1], jnp.maximum(z - 1, 0) * NY + y, tp)

    @pl.when(y != 3)
    def _():
        k_in(3).wait_recv()

    @pl.when(z < NZ - 1)
    def _():
        up_copy.start()

    @pl.when(y != 0)
    def _():
        k_in(0).wait_recv()

    @pl.when(z > 0)
    def _():
        dn_copy.start()

    @pl.when(y != 1)
    def _():
        k_in(1).wait_recv()

    @pl.when(y != 2)
    def _():
        k_in(2).wait_recv()

    phase("gates")
    g_copy.wait_recv()
    for part in range(2):
        g = (gbuf[:, core] if part == 0 else gother[...]).astype(F32)
        sgate[:, :, TOK * part : TOK * part + TOK] = g * (1.0 / (1.0 + jnp.exp(-g)))
    phase("q_wait")
    drain(qrecv.at[pl.ds(0, NY - 1)], qr)
    phase("c_wait")
    drain(ctxkv.at[pl.ds(0, CTX - NY * CTXL)], cr)
    first = 1 - lax.div(x, 2)
    beside = x + 1 - 2 * lax.rem(x, 2)
    source = core * NY + y

    def r_copy(a, b, h):
        return remote(
            rsend.at[a, b, h], rrecv.at[a, source], rs, rr.at[a], z * NY + b, x * NC + h
        )

    def pair(a, b):
        p = 2 * b + a
        xq = qrecv[b].astype(F32)
        qp = jnp.where(low, jnp.where(a == 1, half_swap(xq), xq), 0.0).astype(BF16)
        base = jnp.clip(row0 + 2 * p - 4, 0, LAST_START) - row0 + 4
        rows = pl.ds(pl.multiple_of(base * GRID_W, GRID_W), 10 * GRID_W)
        t = jnp.where(p < 2, p, jnp.where(p < 6, 2, p - 3))
        sc_ctx = dot_nt(qp, ctxkv[...])
        kvw = kvext[rows, :]
        sc_win = dot_nt(qp, kvw) + btab[t]
        top = jnp.maximum(
            jnp.max(sc_ctx, axis=1, keepdims=True), jnp.max(sc_win, axis=1, keepdims=True)
        )
        e_ctx = jnp.exp(sc_ctx - top)
        e_win = jnp.exp(sc_win - top)
        den = jnp.sum(e_ctx, axis=1, keepdims=True) + jnp.sum(e_win, axis=1, keepdims=True)
        o = dot(e_ctx.astype(BF16), ctxkv[...]) + dot(e_win.astype(BF16), kvw)
        o = o * (1.0 / den)
        for h in range(NC):
            r0, r1 = o[OUTR * h : OUTR * h + OUTR], o[64 + OUTR * h : 64 + OUTR * h + OUTR]
            rsend[a, b, h] = jnp.where(low, half_swap(r0), r1).astype(BF16)

    def pairs(a, *blocks):
        for b in blocks:
            pair(a, b)
        for b in blocks:
            for h in range(NC):
                here = (b == y) & (h == core)

                @pl.when(here)
                def _():
                    rrecv[a, source] = rsend[a, b, h]

                @pl.when(jnp.logical_not(here))
                def _():
                    r_copy(a, b, h).start()

    def p_copy(i):
        return remote(psend.at[i], precv.at[x], ps, pr, sp, i * NC + core)

    def finish(a):
        phase("r_wait")
        drain(rrecv.at[a, pl.ds(0, NC * NY - 1)], rr.at[a])
        phase("project")
        for part in range(2):
            src = (core if part == 0 else 1 - core) * NY
            for q in range(2):
                x0, x1 = rrecv[a, src + 2 * q].astype(F32), rrecv[a, src + 2 * q + 1].astype(F32)
                cols = slice(TOK * part + 128 * q, TOK * part + 128 * q + 128)
                up = jnp.where(low, x0, half_swap(x1)) * sgate[2 * a, :, cols]
                dn = jnp.where(low, half_swap(x0), x1) * sgate[2 * a + 1, :, cols]
                gated[0:OUTR, cols] = up.astype(BF16)
                gated[OUTR : 2 * OUTR, cols] = dn.astype(BF16)
        for n in range(4):
            cols = slice(512 * n, 512 * n + 512)
            term = dot(gated[:, :TOK], wo[:, cols]) + dot(gated[:, TOK:], wo2[:, cols])
            psend[2 * a, :, cols] = term[:OUTR].astype(BF16)
            psend[2 * a + 1, :, cols] = term[OUTR:].astype(BF16)

    pairs(first, 1, 2)
    phase("h_wait")

    @pl.when(z > 0)
    def _():
        up_copy.wait_recv()

    @pl.when(z < NZ - 1)
    def _():
        dn_copy.wait_recv()

    phase("attention2")
    pairs(first, 0, 3)
    phase("attention3")
    pairs(1 - first, 1, 2)
    pairs(1 - first, 0, 3)
    phase("w_wait")
    w_copy.wait_recv()
    finish(first)
    p_copy(lax.rem(x + 2, NX)).start()
    p_copy(lax.rem(beside + 2, NX)).start()
    finish(1 - first)
    p_copy(beside).start()

    phase("sent1")
    drain(zrecv.at[pl.ds(0, NZ - 1)], zs)
    drain(zgrecv.at[pl.ds(0, NZ - 1)], zgs)
    drain(mrecv.at[pl.ds(0, NY * NTP - 1)], ms)
    drain(mgrecv.at[pl.ds(0, NY * NTP - 1)], mgs)
    drain(mgrecv.at[pl.ds(0, NY * NTP - 1)], mgr)
    drain(ctxkv.at[pl.ds(0, CTX - NY * CTXL)], cs)
    drain(ctx.at[pl.ds(0, NY - 1), 0], xs)
    drain(ctx.at[pl.ds(0, NY - 1), 0], xps)
    drain(kvext.at[pl.ds(0, (NY - 1) * TOK)], ks)
    drain(qrecv.at[pl.ds(0, NY - 1)], qs)
    w_copy.wait_send()
    g_copy.wait_send()
    for a in range(2):
        drain(rrecv.at[a, pl.ds(0, NC * NY - 1)], rs)

    @pl.when(z < NZ - 1)
    def _():
        up_copy.wait_send()

    @pl.when(z > 0)
    def _():
        dn_copy.wait_send()

    for t in range(NTP):
        total = mgrecv[t] + mgrecv[NTP + t] + mgrecv[2 * NTP + t] + mgrecv[3 * NTP + t]
        mod[4:5, 256 * t : 256 * t + 128] = total[0:1]
        mod[4:5, 256 * t + 128 : 256 * t + 256] = total[1:2]
    phase("p_wait")
    drain(precv.at[pl.ds(0, NX - 1)], pr)
    phase("final")
    branch = psend[x].astype(F32)
    for k in (1, 2, 3):
        branch = branch + precv[lax.rem(x + k, NX)].astype(F32)
    branch = branch.astype(BF16).astype(F32)
    normed = branch * lax.rsqrt(jnp.mean(branch * branch, axis=1, keepdims=True) + EPSILON)
    own = lat[pl.ds(pl.multiple_of(tp * OUTR, OUTR), OUTR), :].astype(F32)
    out_ref[...] = (own + mod[4:5, :] * (normed * mod[6:7, :])).astype(BF16)

    phase("sent")
    drain(precv.at[pl.ds(0, NX - 1)], ps)
    phase(None)


def shards(
    latent,
    context,
    condition,
    context_condition,
    gain_pre,
    gain_post,
    w_shift,
    w_scale,
    w_gate,
    w_query,
    w_key,
    w_value,
    w_silu,
    offset_bias,
    w_out,
):
    in_rows = w_shift.shape[0]
    vmem = pl.BlockSpec(memory_space=pltpu.VMEM)
    hbm = pl.BlockSpec(memory_space=pltpu.HBM)
    dma = pltpu.SemaphoreType.DMA
    operands = (
        condition.reshape(16, 128),
        context_condition.reshape(16, 128),
        gain_pre.reshape(16, 128),
        gain_post.reshape(16, 128),
        jnp.transpose(offset_bias, (1, 0, 2)),
        latent,
        context,
        w_shift,
        w_scale,
        w_gate,
        w_query,
        w_key,
        w_value,
        w_silu,
        w_out,
    )
    operands = [pltpu.with_memory_space_constraint(a, pltpu.HBM) for a in operands]
    return pl.pallas_call(
        kernel,
        name="whole",
        out_shape=jax.ShapeDtypeStruct((OUTR, D), BF16),
        in_specs=[hbm] * 15,
        out_specs=vmem,
        scratch_shapes=[
            pltpu.VMEM((2, 16, 128), BF16),
            pltpu.VMEM((2, 16, 128), F32),
            pltpu.VMEM((2, 16, 128), F32),
            pltpu.VMEM((2 * WIN_ROWS - 1, NY, 2 * WIN_COLS - 1), F32),
            pltpu.VMEM((16, 128), F32),
            pltpu.VMEM((3, in_rows, TOK), BF16),
            pltpu.VMEM((TOK, D), BF16),
            pltpu.VMEM((NY, NC, CTXL // NC, D), BF16),
            pltpu.VMEM((D, 2 * TOK), BF16),
            pltpu.VMEM((D, 128), BF16),
            pltpu.VMEM((D, 2 * TOK), BF16),
            pltpu.VMEM((TOK, D), BF16),
            pltpu.VMEM((TOK, D), BF16),
            pltpu.VMEM((8, 128), F32),
            pltpu.VMEM((NZ, 8, 128), F32),
            pltpu.VMEM((8, 128), F32),
            pltpu.VMEM((NY * NTP, 8, 128), F32),
            pltpu.VMEM((2, 128), F32),
            pltpu.VMEM((NZ, 2, 128), F32),
            pltpu.VMEM((2, 128), F32),
            pltpu.VMEM((NY * NTP, 2, 128), F32),
            pltpu.VMEM((8, D), F32),
            pltpu.VMEM((4, 8, D), F32),
            pltpu.VMEM((len(SPECIAL), 128, 640), F32),
            pltpu.VMEM((TOK, D), BF16),
            pltpu.VMEM((NY * CTXL, D), BF16),
            pltpu.VMEM((TOK, 128), F32),
            pltpu.VMEM((NY * CTXL, 128), F32),
            pltpu.VMEM((CTX, 128), BF16),
            pltpu.VMEM((NY, TOK, 128), BF16),
            pltpu.VMEM((6 * TOK, 128), BF16),
            pltpu.VMEM((NY, 128, 128), BF16),
            pltpu.VMEM((NY, 128, 128), BF16),
            pltpu.VMEM((NX, NC, OUTR, TOK), BF16),
            pltpu.VMEM((NX, OUTR, TOK), BF16),
            pltpu.VMEM((NX, OUTR, NC * TOK), F32),
            pltpu.VMEM((2, NY, NC, OUTR, 128), BF16),
            pltpu.VMEM((2, NC * NY, OUTR, 128), BF16),
            pltpu.VMEM((2 * OUTR, NC * TOK), BF16),
            pltpu.VMEM((NX, OUTR, D), BF16),
            pltpu.VMEM((NX, OUTR, D), BF16),
            dma((9,)),
            dma,
            dma,
            dma,
            dma,
            dma,
            dma,
            dma,
            dma,
            dma,
            dma,
            dma,
            dma,
            dma,
            dma,
            dma,
            dma,
            dma,
            dma((NY,)),
            dma,
            dma,
            dma((2,)),
            dma((2,)),
            dma,
            dma((2,)),
            dma,
            dma,
            dma,
            dma,
        ],
        compiler_params=pltpu.CompilerParams(
            collective_id=0, has_side_effects=True, vmem_limit_bytes=48 << 20
        ),
    )(*operands)


def solution(mesh):
    in_specs = (
        P("sp", None),
        P("sp", None),
        P(),
        P(),
        P(),
        P(),
        P("sp", "tp"),
        P("sp", "tp"),
        P("sp", "tp"),
        P(None, "tp"),
        P(None, "tp"),
        P(None, "tp"),
        P(None, "tp"),
        P("tp", None, None),
        P("tp", None),
    )
    out_specs = P(("sp", "tp"), None)
    return jax.shard_map(shards, mesh=mesh, in_specs=in_specs, out_specs=out_specs, check_vma=False)
```

```python
import functools

import jax
import jax.numpy as jnp
from jax import lax
from jax.experimental import pallas as pl
from jax.experimental.pallas import tpu as pltpu
from jax.sharding import PartitionSpec as P

GRID_W = 64
WIN_ROWS = 8
WIN_COLS = 16
EPSILON = 1e-06
NZ, NY, NX, NC = 8, 4, 4, 2
NTP = NX * NC
D = 2048
HD = 64
TOK = 256
CTXL = 32
CTX = 1024
OUTR = TOK // NTP
LAST_START = NZ * NY * TOK // GRID_W - WIN_ROWS
SPECIAL = (0, 1, 2, 6, 7)
Z_ORDER = (4, 3, 5, 2, 6, 1, 7)
G_ORDER = sorted(
    ((ky, kx, kc) for ky in range(NY) for kx in range(NX) for kc in range(NC)),
    key=lambda k: -min(k[0], NY - k[0]) - min(k[1], NX - k[1]) - k[2] / 2,
)[:-1]
F32 = jnp.float32
BF16 = jnp.bfloat16
NT = (((1,), (1,)), ((), ()))


def dot(a, b):
    return jnp.dot(a, b, preferred_element_type=F32)


def dot_nt(a, b):
    return lax.dot_general(a, b, NT, preferred_element_type=F32)


def remote(src, dst, ssem, rsem, sp, tp):
    return pltpu.make_async_remote_copy(
        src_ref=src,
        dst_ref=dst,
        send_sem=ssem,
        recv_sem=rsem,
        device_id=(sp, tp),
        device_id_type=pl.DeviceIdType.MESH,
    )


class Phases:
    def __init__(self):
        self.scope = None

    def __call__(self, name):
        if self.scope is not None:
            self.scope.__exit__(None, None, None)
        self.scope = None
        if name:
            self.scope = jax.named_scope(name)
            self.scope.__enter__()


def drain(ref, sem):
    pltpu.make_async_copy(ref, ref, sem).wait()


def half_swap(v):
    return pltpu.roll(v, 64, 1)


def kernel(
    cond_h,
    cond2_h,
    gpre_h,
    gpost_h,
    bias_h,
    lat_h,
    ctx_h,
    wsh_h,
    wsc_h,
    wga_h,
    wq_h,
    wk_h,
    wv_h,
    wg_h,
    wo_h,
    out_ref,
    conds,
    condf,
    gains,
    bias,
    biasx,
    wmod,
    lat,
    ctx,
    wkv,
    wy,
    wqg,
    wo,
    wo2,
    zsend,
    zrecv,
    msend,
    mrecv,
    zgsend,
    zgrecv,
    mgsend,
    mgrecv,
    mod,
    spread,
    btab,
    hid,
    hidc,
    rsl,
    rsc,
    ctxkv,
    kvsend,
    kvext,
    qsend,
    qrecv,
    gbuf,
    gother,
    sgate,
    rsend,
    rrecv,
    gated,
    psend,
    precv,
    lsem,
    zs,
    zr,
    ms,
    mr,
    zgs,
    zgr,
    mgs,
    mgr,
    xs,
    xr,
    xps,
    xpr,
    ws,
    wr,
    cs,
    cr,
    ks,
    kr,
    qs,
    qr,
    hs,
    hr,
    rs,
    rr,
    gs,
    gr,
    ps,
    pr,
):
    sp = lax.axis_index("sp")
    tp = lax.axis_index("tp")
    z, y = lax.div(sp, NY), lax.rem(sp, NY)
    x, core = lax.div(tp, NC), lax.rem(tp, NC)
    partner = x * NC + (1 - core)
    group = y * NTP + tp
    lane = lax.broadcasted_iota(jnp.int32, (1, 128), 1)
    low = lane < 64

    phase = Phases()
    phase("loads")
    def load(sem, *moves):
        for a, b in moves:
            pltpu.make_async_copy(a, b, lsem.at[sem]).start()

    load(0, (cond_h, conds.at[0]), (cond2_h, conds.at[1]))
    load(1, (wsh_h, wmod.at[0]), (wsc_h, wmod.at[1]), (wga_h, wmod.at[2]))
    half = CTXL // NC
    load(8, *((ctx_h.at[pl.ds(half * h, half), :], ctx.at[y, h]) for h in range(NC)))
    load(2, (lat_h, lat))
    load(3, (gpre_h, gains.at[0]), (gpost_h, gains.at[1]))
    load(4, (bias_h, bias))
    load(5, (wo_h, wo))
    load(6, (wk_h, wkv.at[:, pl.ds(0, TOK)]), (wv_h, wkv.at[:, pl.ds(TOK, TOK)]))
    load(7, (wq_h, wqg.at[:, pl.ds(0, TOK)]), (wg_h, wqg.at[:, pl.ds(TOK, TOK)]))

    phase("greet")
    barrier = pltpu.get_barrier_semaphore()

    def greet(dsp, dtp):
        pl.semaphore_signal(
            barrier, inc=1, device_id=(dsp, dtp), device_id_type=pl.DeviceIdType.MESH
        )

    for k in Z_ORDER:
        greet(lax.rem(z + k, NZ) * NY + y, tp)

    def group_peer(k):
        dx, dc = lax.rem(x + k[1], NX), 1 - core if k[2] else core
        return z * NY + lax.rem(y + k[0], NY), dx * NC + dc

    for k in G_ORDER:
        greet(*group_peer(k))

    phase("partial")
    drain(conds, lsem.at[0])
    v = conds[...].astype(F32)
    condf[...] = v * (1.0 / (1.0 + jnp.exp(-v)))
    line = jnp.concatenate([condf[i, pl.ds(lax.div(sp, 2), 1), :] for i in range(2)], axis=0)
    line = jnp.where(lax.rem(sp, 2) == 1, half_swap(line), line)[:, :64]
    act = jnp.concatenate([line, jnp.zeros((6, 64), F32)], axis=0).astype(BF16)
    drain(wmod, lsem.at[1])
    sh = dot(act, wmod[0])
    sc = dot(act, wmod[1])
    ga = dot(act, wmod[2])
    zsend[0:2] = sh[0:2, :128]
    zsend[2:4] = sc[0:2, :128]
    zsend[4:6] = sh[0:2, 128:]
    zsend[6:8] = sc[0:2, 128:]
    zgsend[0:1] = ga[0:1, :128]
    zgsend[1:2] = ga[0:1, 128:]
    zrecv[z] = zsend[...]
    zgrecv[z] = zgsend[...]

    phase("barrier")
    pl.semaphore_wait(barrier, NZ - 1 + NY * NTP - 1)

    phase("z_start")
    def z_copy(k):
        dz = lax.rem(z + k, NZ)
        return remote(zsend, zrecv.at[z], zs, zr, dz * NY + y, tp)

    def zg_copy(k):
        dz = lax.rem(z + k, NZ)
        return remote(zgsend, zgrecv.at[z], zgs, zgr, dz * NY + y, tp)

    for k in Z_ORDER:
        z_copy(k).start()
    for k in Z_ORDER:
        zg_copy(k).start()

    def x_copy(k):
        dy = lax.rem(y + k, NY)
        return remote(ctx.at[y, core], ctx.at[y, core], xs, xr, z * NY + dy, tp)

    def x_pass(k):
        rows = ctx.at[lax.rem(y + k, NY), core]
        return remote(rows, rows, xps, xpr, sp, partner)

    drain(ctx.at[0], lsem.at[8])
    for k in (2, 1, 3):
        x_copy(k).start()

    phase("stats")
    drain(lat, lsem.at[2])

    def stats(v):
        r = lax.rsqrt(jnp.mean(v * v, axis=1, keepdims=True) + EPSILON)
        return jnp.broadcast_to(r, (v.shape[0], 128))

    def row_stats(i, c):
        rows = pl.ds(pl.multiple_of(i * 32, 32), 32)
        rsl[rows, :] = stats(lat[rows, :].astype(F32))
        return c

    lax.fori_loop(0, TOK // 32, row_stats, 0)
    drain(gains, lsem.at[3])
    for t in range(16):
        mod[5:6, 128 * t : 128 * t + 128] = gains[0, t : t + 1, :]
        mod[6:7, 128 * t : 128 * t + 128] = gains[1, t : t + 1, :]
    drain(bias, lsem.at[4])
    biasx[...] = jnp.zeros((16, 128), F32)
    for d in range(2 * WIN_ROWS - 1):
        line = bias[d, pl.ds(y, 1), :]
        biasx[d : d + 1, 0:31] = line
        if d > 0:
            biasx[d - 1 : d, 64:95] = line

    phase("z_wait")
    drain(zrecv.at[pl.ds(0, NZ - 1)], zr)
    phase("m_start")
    total = zrecv[0]
    for k in range(1, NZ):
        total = total + zrecv[k]
    msend[...] = total
    mrecv[group] = total

    for k in G_ORDER:
        remote(msend, mrecv.at[group], ms, mr, *group_peer(k)).start()

    phase("tables")
    col = lax.rem(lax.broadcasted_iota(jnp.int32, (64, 128), 1), 64)
    right = lax.div(lax.broadcasted_iota(jnp.int32, (64, 128), 1), 64)
    qcol = lax.broadcasted_iota(jnp.int32, (64, 128), 0)
    first_col = jnp.clip(qcol - WIN_COLS // 2, 0, GRID_W - WIN_COLS)
    in_cols = (col >= first_col) & (col < first_col + WIN_COLS)
    row0 = z * 16

    def table(t, c):
        p = jnp.where(t < 3, t, t + 3)
        base = jnp.clip(row0 + 2 * p - 4, 0, LAST_START)
        for a in range(2):
            row = row0 + 2 * p + a
            off = jnp.clip(row - 4, 0, LAST_START) - base
            d0 = base - row + 7
            for m in range(5):
                line = biasx[pl.ds(d0 + 2 * m, 1), :]
                tile = pltpu.roll(
                    jnp.broadcast_to(line, (64, 128)), 113, 1, stride=1, stride_axis=0
                )
                krow = right + 2 * m
                ok = in_cols & (krow >= off) & (krow < off + WIN_ROWS)
                btab[t, a * 64 : a * 64 + 64, m * 128 : m * 128 + 128] = jnp.where(
                    ok, tile, -jnp.inf
                )
        return c

    lax.fori_loop(0, len(SPECIAL), table, 0)

    @pl.when(z == 0)
    def _():
        kvext[0:TOK] = jnp.zeros((TOK, 128), BF16)

    @pl.when(z == NZ - 1)
    def _():
        kvext[5 * TOK : 6 * TOK] = jnp.zeros((TOK, 128), BF16)

    phase("x_wait")
    drain(ctx.at[pl.ds(0, NY - 1), 0], xr)
    for k in (1, 2, 3):
        x_pass(k).start()

    phase("wy")
    drain(wkv, lsem.at[6])

    def head_columns(i, c):
        rows = pl.ds(pl.multiple_of(i * 256, 256), 256)
        at = 128 * lax.div(y, 2)
        kt = wkv[rows, pl.ds(pl.multiple_of(at, 128), 128)].astype(F32)
        vt = wkv[rows, pl.ds(pl.multiple_of(TOK + at, 128), 128)].astype(F32)
        odd = lax.rem(y, 2) == 1
        wy[rows, :] = jnp.where(
            low, jnp.where(odd, half_swap(kt), kt), jnp.where(odd, vt, half_swap(vt))
        ).astype(BF16)
        return c

    lax.fori_loop(0, D // 256, head_columns, 0)
    phase("x_wait2")
    drain(ctx.at[pl.ds(0, NY - 1), 0], xpr)
    for b in range(NY):
        rows = slice(CTXL * b, CTXL * b + CTXL)
        rsc[rows, :] = stats(ctx[b].reshape(CTXL, D).astype(F32))

    phase("m_wait")
    drain(mrecv.at[pl.ds(0, NY * NTP - 1)], mr)
    phase("mod")
    for t in range(NTP):
        total = mrecv[t] + mrecv[NTP + t] + mrecv[2 * NTP + t] + mrecv[3 * NTP + t]
        lo, hi = 256 * t, 256 * t + 128
        mod[0:4, lo : lo + 128] = total[0:4]
        mod[0:4, hi : hi + 128] = total[4:8]
    mod[2:3, :] = mod[5:6, :] * (1.0 + mod[2:3, :])
    mod[3:4, :] = mod[5:6, :] * (1.0 + mod[3:4, :])

    for i in range(4):
        spread[i] = jnp.broadcast_to(mod[i : i + 1, :], (8, D))

    def hidden(v, r, which):
        n = v.shape[0] // 8
        r = r.reshape(n, 8, 128)
        parts = []
        for t in range(D // 128):
            cols = slice(128 * t, 128 * t + 128)
            u = v[:, cols].astype(F32).reshape(n, 8, 128) * r
            u = u * spread[2 + which, :, cols] + spread[which, :, cols]
            parts.append(u.reshape(8 * n, 128).astype(BF16))
        return jnp.concatenate(parts, axis=1)

    phase("ctx_hidden")
    for b in range(NY):
        rows = slice(CTXL * b, CTXL * b + CTXL)
        hidc[rows, :] = hidden(ctx[b].reshape(CTXL, D), rsc[rows, :], 1)
    phase("ctx_kv")
    here = pl.ds(pl.multiple_of(z * NY * CTXL, NY * CTXL), NY * CTXL)
    ctxkv[here, :] = dot(hidc[...], wy[...]).astype(BF16)

    def c_copy(k):
        dz = lax.rem(z + k, NZ)
        return remote(ctxkv.at[here, :], ctxkv.at[here, :], cs, cr, dz * NY + y, tp)

    for k in Z_ORDER:
        c_copy(k).start()

    phase("hidden_kv")
    for i in range(2):
        rows = slice(128 * i, 128 * i + 128)
        for n in range(4):
            r32 = slice(128 * i + 32 * n, 128 * i + 32 * n + 32)
            hid[r32, :] = hidden(lat[r32, :], rsl[r32, :], 0)
        kv = dot(hid[rows, :], wkv[...])
        for q in range(2):
            kt = kv[:, 128 * q : 128 * q + 128]
            vt = kv[:, 256 + 128 * q : 256 + 128 * q + 128]
            kvsend[2 * q, rows] = jnp.where(low, kt, half_swap(vt)).astype(BF16)
            kvsend[2 * q + 1, rows] = jnp.where(low, half_swap(kt), vt).astype(BF16)
    mine = pl.ds(pl.multiple_of((1 + y) * TOK, TOK), TOK)
    kvext[mine, :] = kvsend[y]

    def k_copy(k):
        dy = lax.rem(y + k, NY)
        return remote(kvsend.at[dy], kvext.at[mine, :], ks, kr.at[y], z * NY + dy, tp)

    def k_in(dy):
        rows = pl.ds(pl.multiple_of((1 + dy) * TOK, TOK), TOK)
        return remote(kvsend.at[y], kvext.at[rows, :], ks, kr.at[dy], z * NY + dy, tp)

    for k in (2, 1, 3):
        k_copy(k).start()

    phase("qg")
    drain(wqg, lsem.at[7])
    qg = dot(hid[0:TOK, :], wqg[:, 0:TOK])
    for q in range(2):
        qt = qg[:, 128 * q : 128 * q + 128] * (HD**-0.5)
        up, dn = qt[0:128], qt[128:256]
        qsend[2 * q] = jnp.where(low, up, half_swap(dn)).astype(BF16)
        qsend[2 * q + 1] = jnp.where(low, half_swap(up), dn).astype(BF16)
    qrecv[y] = qsend[y]

    def q_copy(k):
        dy = lax.rem(y + k, NY)
        return remote(qsend.at[dy], qrecv.at[y], qs, qr, z * NY + dy, tp)

    for k in (2, 1, 3):
        q_copy(k).start()
    phase("g")
    g = dot(hid[0:TOK, :], wqg[:, TOK:])
    gbuf[...] = g.astype(BF16).reshape(NX, NC, OUTR, TOK)
    g_copy = remote(gbuf.at[:, 1 - core], gother, gs, gr, sp, partner)
    g_copy.start()
    drain(wo, lsem.at[5])
    w_copy = remote(wo, wo2, ws, wr, sp, partner)
    w_copy.start()

    phase("kq_wait")
    drain(zgrecv.at[pl.ds(0, NZ - 1)], zgr)
    total = zgrecv[0]
    for k in range(1, NZ):
        total = total + zgrecv[k]
    mgsend[...] = total
    mgrecv[group] = total

    for k in G_ORDER:
        remote(mgsend, mgrecv.at[group], mgs, mgr, *group_peer(k)).start()

    up_src = kvext.at[pl.ds(4 * TOK, TOK), :]
    dn_src = kvext.at[pl.ds(TOK, TOK), :]
    up_dst = kvext.at[pl.ds(0, TOK), :]
    dn_dst = kvext.at[pl.ds(5 * TOK, TOK), :]
    up_copy = remote(up_src, up_dst, hs.at[0], hr.at[0], jnp.minimum(z + 1, NZ - 1) * NY + y, tp)
    dn_copy = remote(dn_src, dn_dst, hs.at[1], hr.at[1], jnp.maximum(z - 1, 0) * NY + y, tp)

    @pl.when(y != 3)
    def _():
        k_in(3).wait_recv()

    @pl.when(z < NZ - 1)
    def _():
        up_copy.start()

    @pl.when(y != 0)
    def _():
        k_in(0).wait_recv()

    @pl.when(z > 0)
    def _():
        dn_copy.start()

    @pl.when(y != 1)
    def _():
        k_in(1).wait_recv()

    @pl.when(y != 2)
    def _():
        k_in(2).wait_recv()

    phase("gates")
    g_copy.wait_recv()
    for part in range(2):
        g = (gbuf[:, core] if part == 0 else gother[...]).astype(F32)
        sgate[:, :, TOK * part : TOK * part + TOK] = g * (1.0 / (1.0 + jnp.exp(-g)))
    phase("q_wait")
    drain(qrecv.at[pl.ds(0, NY - 1)], qr)
    phase("c_wait")
    drain(ctxkv.at[pl.ds(0, CTX - NY * CTXL)], cr)
    phase("attention")
    first = 1 - lax.div(x, 2)
    beside = x + 1 - 2 * lax.rem(x, 2)
    source = core * NY + y

    def r_copy(a, b, h):
        return remote(
            rsend.at[a, b, h], rrecv.at[a, source], rs, rr.at[a], z * NY + b, x * NC + h
        )

    def pairs(a, *blocks):
        queries, windows = [], []
        for b in blocks:
            p = 2 * b + a
            xq = qrecv[b].astype(F32)
            queries.append(
                jnp.where(low, jnp.where(a == 1, half_swap(xq), xq), 0.0).astype(BF16)
            )
            base = jnp.clip(row0 + 2 * p - 4, 0, LAST_START) - row0 + 4
            rows = pl.ds(pl.multiple_of(base * GRID_W, GRID_W), 10 * GRID_W)
            windows.append((rows, jnp.where(p < 2, p, jnp.where(p < 6, 2, p - 3))))
        sc_ctx = dot_nt(jnp.concatenate(queries, axis=0), ctxkv[...])
        sc_win = jnp.concatenate(
            [dot_nt(qp, kvext[rows, :]) + btab[t] for qp, (rows, t) in zip(queries, windows)],
            axis=0,
        )
        top = jnp.maximum(
            jnp.max(sc_ctx, axis=1, keepdims=True), jnp.max(sc_win, axis=1, keepdims=True)
        )
        e_ctx = jnp.exp(sc_ctx - top)
        e_win = jnp.exp(sc_win - top)
        den = jnp.sum(e_ctx, axis=1, keepdims=True) + jnp.sum(e_win, axis=1, keepdims=True)
        e_win = e_win.astype(BF16)
        o_all = dot(e_ctx.astype(BF16), ctxkv[...])
        for i, (b, (rows, t)) in enumerate(zip(blocks, windows)):
            part = slice(128 * i, 128 * i + 128)
            o = (o_all[part] + dot(e_win[part], kvext[rows, :])) * (1.0 / den[part])
            for h in range(NC):
                r0, r1 = o[OUTR * h : OUTR * h + OUTR], o[64 + OUTR * h : 64 + OUTR * h + OUTR]
                rsend[a, b, h] = jnp.where(low, half_swap(r0), r1).astype(BF16)
        for b in blocks:
            for h in range(NC):
                here = (b == y) & (h == core)

                @pl.when(here)
                def _():
                    rrecv[a, source] = rsend[a, b, h]

                @pl.when(jnp.logical_not(here))
                def _():
                    r_copy(a, b, h).start()

    def p_copy(i):
        return remote(psend.at[i], precv.at[x], ps, pr, sp, i * NC + core)

    def finish(a):
        phase("r_wait")
        drain(rrecv.at[a, pl.ds(0, NC * NY - 1)], rr.at[a])
        phase("project")
        for part in range(2):
            src = (core if part == 0 else 1 - core) * NY
            for q in range(2):
                x0, x1 = rrecv[a, src + 2 * q].astype(F32), rrecv[a, src + 2 * q + 1].astype(F32)
                cols = slice(TOK * part + 128 * q, TOK * part + 128 * q + 128)
                up = jnp.where(low, x0, half_swap(x1)) * sgate[2 * a, :, cols]
                dn = jnp.where(low, half_swap(x0), x1) * sgate[2 * a + 1, :, cols]
                gated[0:OUTR, cols] = up.astype(BF16)
                gated[OUTR : 2 * OUTR, cols] = dn.astype(BF16)
        for n in range(4):
            cols = slice(512 * n, 512 * n + 512)
            term = dot(gated[:, :TOK], wo[:, cols]) + dot(gated[:, TOK:], wo2[:, cols])
            psend[2 * a, :, cols] = term[:OUTR].astype(BF16)
            psend[2 * a + 1, :, cols] = term[OUTR:].astype(BF16)

    pairs(first, 1, 2)
    phase("h_wait")

    @pl.when(z > 0)
    def _():
        up_copy.wait_recv()

    @pl.when(z < NZ - 1)
    def _():
        dn_copy.wait_recv()

    phase("attention2")
    pairs(first, 0, 3)
    phase("attention3")
    pairs(1 - first, 0, 3)
    pairs(1 - first, 1, 2)
    phase("w_wait")
    w_copy.wait_recv()
    finish(first)
    p_copy(lax.rem(x + 2, NX)).start()
    p_copy(lax.rem(beside + 2, NX)).start()
    finish(1 - first)
    p_copy(beside).start()

    phase("sent1")
    drain(zrecv.at[pl.ds(0, NZ - 1)], zs)
    drain(zgrecv.at[pl.ds(0, NZ - 1)], zgs)
    drain(mrecv.at[pl.ds(0, NY * NTP - 1)], ms)
    drain(mgrecv.at[pl.ds(0, NY * NTP - 1)], mgs)
    drain(mgrecv.at[pl.ds(0, NY * NTP - 1)], mgr)
    drain(ctxkv.at[pl.ds(0, CTX - NY * CTXL)], cs)
    drain(ctx.at[pl.ds(0, NY - 1), 0], xs)
    drain(ctx.at[pl.ds(0, NY - 1), 0], xps)
    drain(kvext.at[pl.ds(0, (NY - 1) * TOK)], ks)
    drain(qrecv.at[pl.ds(0, NY - 1)], qs)
    w_copy.wait_send()
    g_copy.wait_send()
    for a in range(2):
        drain(rrecv.at[a, pl.ds(0, NC * NY - 1)], rs)

    @pl.when(z < NZ - 1)
    def _():
        up_copy.wait_send()

    @pl.when(z > 0)
    def _():
        dn_copy.wait_send()

    for t in range(NTP):
        total = mgrecv[t] + mgrecv[NTP + t] + mgrecv[2 * NTP + t] + mgrecv[3 * NTP + t]
        mod[4:5, 256 * t : 256 * t + 128] = total[0:1]
        mod[4:5, 256 * t + 128 : 256 * t + 256] = total[1:2]
    phase("p_wait")
    drain(precv.at[pl.ds(0, NX - 1)], pr)
    phase("final")
    branch = psend[x].astype(F32)
    for k in (1, 2, 3):
        branch = branch + precv[lax.rem(x + k, NX)].astype(F32)
    branch = branch.astype(BF16).astype(F32)
    normed = branch * lax.rsqrt(jnp.mean(branch * branch, axis=1, keepdims=True) + EPSILON)
    own = lat[pl.ds(pl.multiple_of(tp * OUTR, OUTR), OUTR), :].astype(F32)
    out_ref[...] = (own + mod[4:5, :] * (normed * mod[6:7, :])).astype(BF16)

    phase("sent")
    drain(precv.at[pl.ds(0, NX - 1)], ps)
    phase(None)


def shards(
    latent,
    context,
    condition,
    context_condition,
    gain_pre,
    gain_post,
    w_shift,
    w_scale,
    w_gate,
    w_query,
    w_key,
    w_value,
    w_silu,
    offset_bias,
    w_out,
):
    in_rows = w_shift.shape[0]
    vmem = pl.BlockSpec(memory_space=pltpu.VMEM)
    hbm = pl.BlockSpec(memory_space=pltpu.HBM)
    dma = pltpu.SemaphoreType.DMA
    operands = (
        condition.reshape(16, 128),
        context_condition.reshape(16, 128),
        gain_pre.reshape(16, 128),
        gain_post.reshape(16, 128),
        jnp.transpose(offset_bias, (1, 0, 2)),
        latent,
        context,
        w_shift,
        w_scale,
        w_gate,
        w_query,
        w_key,
        w_value,
        w_silu,
        w_out,
    )
    operands = [pltpu.with_memory_space_constraint(a, pltpu.HBM) for a in operands]
    return pl.pallas_call(
        kernel,
        name="whole",
        out_shape=jax.ShapeDtypeStruct((OUTR, D), BF16),
        in_specs=[hbm] * 15,
        out_specs=vmem,
        scratch_shapes=[
            pltpu.VMEM((2, 16, 128), BF16),
            pltpu.VMEM((2, 16, 128), F32),
            pltpu.VMEM((2, 16, 128), F32),
            pltpu.VMEM((2 * WIN_ROWS - 1, NY, 2 * WIN_COLS - 1), F32),
            pltpu.VMEM((16, 128), F32),
            pltpu.VMEM((3, in_rows, TOK), BF16),
            pltpu.VMEM((TOK, D), BF16),
            pltpu.VMEM((NY, NC, CTXL // NC, D), BF16),
            pltpu.VMEM((D, 2 * TOK), BF16),
            pltpu.VMEM((D, 128), BF16),
            pltpu.VMEM((D, 2 * TOK), BF16),
            pltpu.VMEM((TOK, D), BF16),
            pltpu.VMEM((TOK, D), BF16),
            pltpu.VMEM((8, 128), F32),
            pltpu.VMEM((NZ, 8, 128), F32),
            pltpu.VMEM((8, 128), F32),
            pltpu.VMEM((NY * NTP, 8, 128), F32),
            pltpu.VMEM((2, 128), F32),
            pltpu.VMEM((NZ, 2, 128), F32),
            pltpu.VMEM((2, 128), F32),
            pltpu.VMEM((NY * NTP, 2, 128), F32),
            pltpu.VMEM((8, D), F32),
            pltpu.VMEM((4, 8, D), F32),
            pltpu.VMEM((len(SPECIAL), 128, 640), F32),
            pltpu.VMEM((TOK, D), BF16),
            pltpu.VMEM((NY * CTXL, D), BF16),
            pltpu.VMEM((TOK, 128), F32),
            pltpu.VMEM((NY * CTXL, 128), F32),
            pltpu.VMEM((CTX, 128), BF16),
            pltpu.VMEM((NY, TOK, 128), BF16),
            pltpu.VMEM((6 * TOK, 128), BF16),
            pltpu.VMEM((NY, 128, 128), BF16),
            pltpu.VMEM((NY, 128, 128), BF16),
            pltpu.VMEM((NX, NC, OUTR, TOK), BF16),
            pltpu.VMEM((NX, OUTR, TOK), BF16),
            pltpu.VMEM((NX, OUTR, NC * TOK), F32),
            pltpu.VMEM((2, NY, NC, OUTR, 128), BF16),
            pltpu.VMEM((2, NC * NY, OUTR, 128), BF16),
            pltpu.VMEM((2 * OUTR, NC * TOK), BF16),
            pltpu.VMEM((NX, OUTR, D), BF16),
            pltpu.VMEM((NX, OUTR, D), BF16),
            dma((9,)),
            dma,
            dma,
            dma,
            dma,
            dma,
            dma,
            dma,
            dma,
            dma,
            dma,
            dma,
            dma,
            dma,
            dma,
            dma,
            dma,
            dma,
            dma((NY,)),
            dma,
            dma,
            dma((2,)),
            dma((2,)),
            dma,
            dma((2,)),
            dma,
            dma,
            dma,
            dma,
        ],
        compiler_params=pltpu.CompilerParams(
            collective_id=0, has_side_effects=True, vmem_limit_bytes=48 << 20
        ),
    )(*operands)


def solution(mesh):
    in_specs = (
        P("sp", None),
        P("sp", None),
        P(),
        P(),
        P(),
        P(),
        P("sp", "tp"),
        P("sp", "tp"),
        P("sp", "tp"),
        P(None, "tp"),
        P(None, "tp"),
        P(None, "tp"),
        P(None, "tp"),
        P("tp", None, None),
        P("tp", None),
    )
    out_specs = P(("sp", "tp"), None)
    return jax.shard_map(shards, mesh=mesh, in_specs=in_specs, out_specs=out_specs, check_vma=False)
```

```python
import functools

import jax
import jax.numpy as jnp
from jax import lax
from jax.experimental import pallas as pl
from jax.experimental.pallas import tpu as pltpu
from jax.sharding import PartitionSpec as P

GRID_W = 64
WIN_ROWS = 8
WIN_COLS = 16
EPSILON = 1e-06
NZ, NY, NX, NC = 8, 4, 4, 2
NTP = NX * NC
D = 2048
HD = 64
TOK = 256
CTXL = 32
CTX = 1024
OUTR = TOK // NTP
LAST_START = NZ * NY * TOK // GRID_W - WIN_ROWS
TABLES = 8
WIN = WIN_ROWS * GRID_W
Z_ORDER = (4, 3, 5, 2, 6, 1, 7)
G_ORDER = sorted(
    ((ky, kx, kc) for ky in range(NY) for kx in range(NX) for kc in range(NC)),
    key=lambda k: -min(k[0], NY - k[0]) - min(k[1], NX - k[1]) - k[2] / 2,
)[:-1]
F32 = jnp.float32
BF16 = jnp.bfloat16
NT = (((1,), (1,)), ((), ()))


def dot(a, b):
    return jnp.dot(a, b, preferred_element_type=F32)


def dot_nt(a, b):
    return lax.dot_general(a, b, NT, preferred_element_type=F32)


def remote(src, dst, ssem, rsem, sp, tp):
    return pltpu.make_async_remote_copy(
        src_ref=src,
        dst_ref=dst,
        send_sem=ssem,
        recv_sem=rsem,
        device_id=(sp, tp),
        device_id_type=pl.DeviceIdType.MESH,
    )


class Phases:
    def __init__(self):
        self.scope = None

    def __call__(self, name):
        if self.scope is not None:
            self.scope.__exit__(None, None, None)
        self.scope = None
        if name:
            self.scope = jax.named_scope(name)
            self.scope.__enter__()


def drain(ref, sem):
    pltpu.make_async_copy(ref, ref, sem).wait()


def half_swap(v):
    return pltpu.roll(v, 64, 1)


def kernel(
    cond_h,
    cond2_h,
    gpre_h,
    gpost_h,
    bias_h,
    lat_h,
    ctx_h,
    wsh_h,
    wsc_h,
    wga_h,
    wq_h,
    wk_h,
    wv_h,
    wg_h,
    wo_h,
    out_ref,
    conds,
    condf,
    gains,
    bias,
    biasx,
    wmod,
    lat,
    ctx,
    wkv,
    wy,
    wqg,
    wo,
    wo2,
    zsend,
    zrecv,
    msend,
    mrecv,
    zgsend,
    zgrecv,
    mgsend,
    mgrecv,
    mod,
    spread,
    btab,
    hid,
    hidc,
    rsl,
    rsc,
    ctxkv,
    kvsend,
    kvext,
    qsend,
    qrecv,
    gbuf,
    gother,
    sgate,
    rsend,
    rrecv,
    gated,
    psend,
    hop,
    precv,
    lsem,
    zs,
    zr,
    ms,
    mr,
    zgs,
    zgr,
    mgs,
    mgr,
    xs,
    xr,
    xps,
    xpr,
    ws,
    wr,
    cs,
    cr,
    ks,
    kr,
    qs,
    qr,
    hs,
    hr,
    rs,
    rr,
    gs,
    gr,
    hp,
    ps,
    pr,
):
    sp = lax.axis_index("sp")
    tp = lax.axis_index("tp")
    z, y = lax.div(sp, NY), lax.rem(sp, NY)
    x, core = lax.div(tp, NC), lax.rem(tp, NC)
    partner = x * NC + (1 - core)
    group = y * NTP + tp
    lane = lax.broadcasted_iota(jnp.int32, (1, 128), 1)
    low = lane < 64

    phase = Phases()
    phase("loads")
    def load(sem, *moves):
        for a, b in moves:
            pltpu.make_async_copy(a, b, lsem.at[sem]).start()

    load(0, (cond_h, conds.at[0]), (cond2_h, conds.at[1]))
    load(1, (wsh_h, wmod.at[0]), (wsc_h, wmod.at[1]), (wga_h, wmod.at[2]))
    half = CTXL // NC
    load(8, *((ctx_h.at[pl.ds(half * h, half), :], ctx.at[y, h]) for h in range(NC)))
    load(2, (lat_h, lat))
    load(3, (gpre_h, gains.at[0]), (gpost_h, gains.at[1]))
    load(4, (bias_h, bias))
    load(5, (wo_h, wo))
    load(6, (wk_h, wkv.at[:, pl.ds(0, TOK)]), (wv_h, wkv.at[:, pl.ds(TOK, TOK)]))
    load(7, (wq_h, wqg.at[:, pl.ds(0, TOK)]), (wg_h, wqg.at[:, pl.ds(TOK, TOK)]))

    phase("greet")
    barrier = pltpu.get_barrier_semaphore()

    def greet(dsp, dtp):
        pl.semaphore_signal(
            barrier, inc=1, device_id=(dsp, dtp), device_id_type=pl.DeviceIdType.MESH
        )

    for k in Z_ORDER:
        greet(lax.rem(z + k, NZ) * NY + y, tp)

    def group_peer(k):
        dx, dc = lax.rem(x + k[1], NX), 1 - core if k[2] else core
        return z * NY + lax.rem(y + k[0], NY), dx * NC + dc

    for k in G_ORDER:
        greet(*group_peer(k))

    phase("partial")
    drain(conds, lsem.at[0])
    v = conds[...].astype(F32)
    condf[...] = v * (1.0 / (1.0 + jnp.exp(-v)))
    line = jnp.concatenate([condf[i, pl.ds(lax.div(sp, 2), 1), :] for i in range(2)], axis=0)
    line = jnp.where(lax.rem(sp, 2) == 1, half_swap(line), line)[:, :64]
    act = jnp.concatenate([line, jnp.zeros((6, 64), F32)], axis=0).astype(BF16)
    drain(wmod, lsem.at[1])
    sh = dot(act, wmod[0])
    sc = dot(act, wmod[1])
    ga = dot(act, wmod[2])
    zsend[0:2] = sh[0:2, :128]
    zsend[2:4] = sc[0:2, :128]
    zsend[4:6] = sh[0:2, 128:]
    zsend[6:8] = sc[0:2, 128:]
    zgsend[0:1] = ga[0:1, :128]
    zgsend[1:2] = ga[0:1, 128:]
    zrecv[z] = zsend[...]
    zgrecv[z] = zgsend[...]

    phase("barrier")
    pl.semaphore_wait(barrier, NZ - 1 + NY * NTP - 1)

    phase("z_start")
    def z_copy(k):
        dz = lax.rem(z + k, NZ)
        return remote(zsend, zrecv.at[z], zs, zr, dz * NY + y, tp)

    def zg_copy(k):
        dz = lax.rem(z + k, NZ)
        return remote(zgsend, zgrecv.at[z], zgs, zgr, dz * NY + y, tp)

    for k in Z_ORDER:
        z_copy(k).start()
    for k in Z_ORDER:
        zg_copy(k).start()

    def x_copy(k):
        dy = lax.rem(y + k, NY)
        return remote(ctx.at[y, core], ctx.at[y, core], xs, xr, z * NY + dy, tp)

    def x_pass(k):
        rows = ctx.at[lax.rem(y + k, NY), core]
        return remote(rows, rows, xps, xpr, sp, partner)

    drain(ctx.at[0], lsem.at[8])
    for k in (2, 1, 3):
        x_copy(k).start()

    phase("stats")
    drain(lat, lsem.at[2])

    def stats(v):
        r = lax.rsqrt(jnp.mean(v * v, axis=1, keepdims=True) + EPSILON)
        return jnp.broadcast_to(r, (v.shape[0], 128))

    def row_stats(i, c):
        rows = pl.ds(pl.multiple_of(i * 32, 32), 32)
        rsl[rows, :] = stats(lat[rows, :].astype(F32))
        return c

    lax.fori_loop(0, TOK // 32, row_stats, 0)
    drain(gains, lsem.at[3])
    for t in range(16):
        mod[5:6, 128 * t : 128 * t + 128] = gains[0, t : t + 1, :]
        mod[6:7, 128 * t : 128 * t + 128] = gains[1, t : t + 1, :]
    drain(bias, lsem.at[4])
    biasx[...] = jnp.zeros((16, 128), F32)
    for d in range(2 * WIN_ROWS - 1):
        line = bias[d, pl.ds(y, 1), :]
        biasx[d : d + 1, 0:31] = line
        if d > 0:
            biasx[d - 1 : d, 64:95] = line

    phase("z_wait")
    drain(zrecv.at[pl.ds(0, NZ - 1)], zr)
    phase("m_start")
    total = zrecv[0]
    for k in range(1, NZ):
        total = total + zrecv[k]
    msend[...] = total
    mrecv[group] = total

    for k in G_ORDER:
        remote(msend, mrecv.at[group], ms, mr, *group_peer(k)).start()

    phase("tables")
    col = lax.rem(lax.broadcasted_iota(jnp.int32, (64, 128), 1), 64)
    qcol = lax.broadcasted_iota(jnp.int32, (64, 128), 0)
    first_col = jnp.clip(qcol - WIN_COLS // 2, 0, GRID_W - WIN_COLS)
    in_cols = (col >= first_col) & (col < first_col + WIN_COLS)
    row0 = z * 16

    def table(t, c):
        row = row0 + jnp.where(t < 5, t, t + 8)
        d0 = jnp.clip(row - 4, 0, LAST_START) - row + 7
        for m in range(WIN_ROWS // 2):
            line = biasx[pl.ds(d0 + 2 * m, 1), :]
            tile = pltpu.roll(
                jnp.broadcast_to(line, (64, 128)), 113, 1, stride=1, stride_axis=0
            )
            btab[t, :, m * 128 : m * 128 + 128] = jnp.where(in_cols, tile, -jnp.inf)
        return c

    lax.fori_loop(0, TABLES, table, 0)

    @pl.when(z == 0)
    def _():
        kvext[0:TOK] = jnp.zeros((TOK, 128), BF16)

    @pl.when(z == NZ - 1)
    def _():
        kvext[5 * TOK : 6 * TOK] = jnp.zeros((TOK, 128), BF16)

    phase("x_wait")
    drain(ctx.at[pl.ds(0, NY - 1), 0], xr)
    for k in (1, 2, 3):
        x_pass(k).start()

    phase("wy")
    drain(wkv, lsem.at[6])

    def head_columns(i, c):
        rows = pl.ds(pl.multiple_of(i * 256, 256), 256)
        at = 128 * lax.div(y, 2)
        kt = wkv[rows, pl.ds(pl.multiple_of(at, 128), 128)].astype(F32)
        vt = wkv[rows, pl.ds(pl.multiple_of(TOK + at, 128), 128)].astype(F32)
        odd = lax.rem(y, 2) == 1
        wy[rows, :] = jnp.where(
            low, jnp.where(odd, half_swap(kt), kt), jnp.where(odd, vt, half_swap(vt))
        ).astype(BF16)
        return c

    lax.fori_loop(0, D // 256, head_columns, 0)
    phase("x_wait2")
    drain(ctx.at[pl.ds(0, NY - 1), 0], xpr)
    for b in range(NY):
        rows = slice(CTXL * b, CTXL * b + CTXL)
        rsc[rows, :] = stats(ctx[b].reshape(CTXL, D).astype(F32))

    phase("m_wait")
    drain(mrecv.at[pl.ds(0, NY * NTP - 1)], mr)
    phase("mod")
    for t in range(NTP):
        total = mrecv[t] + mrecv[NTP + t] + mrecv[2 * NTP + t] + mrecv[3 * NTP + t]
        lo, hi = 256 * t, 256 * t + 128
        mod[0:4, lo : lo + 128] = total[0:4]
        mod[0:4, hi : hi + 128] = total[4:8]
    mod[2:3, :] = mod[5:6, :] * (1.0 + mod[2:3, :])
    mod[3:4, :] = mod[5:6, :] * (1.0 + mod[3:4, :])

    for i in range(4):
        spread[i] = jnp.broadcast_to(mod[i : i + 1, :], (8, D))

    def hidden(v, r, which):
        n = v.shape[0] // 8
        r = r.reshape(n, 8, 128)
        parts = []
        for t in range(D // 128):
            cols = slice(128 * t, 128 * t + 128)
            u = v[:, cols].astype(F32).reshape(n, 8, 128) * r
            u = u * spread[2 + which, :, cols] + spread[which, :, cols]
            parts.append(u.reshape(8 * n, 128).astype(BF16))
        return jnp.concatenate(parts, axis=1)

    phase("ctx_hidden")
    for b in range(NY):
        rows = slice(CTXL * b, CTXL * b + CTXL)
        hidc[rows, :] = hidden(ctx[b].reshape(CTXL, D), rsc[rows, :], 1)
    phase("ctx_kv")
    here = pl.ds(pl.multiple_of(z * NY * CTXL, NY * CTXL), NY * CTXL)
    ctxkv[here, :] = dot(hidc[...], wy[...]).astype(BF16)

    def c_copy(k):
        dz = lax.rem(z + k, NZ)
        return remote(ctxkv.at[here, :], ctxkv.at[here, :], cs, cr, dz * NY + y, tp)

    for k in Z_ORDER:
        c_copy(k).start()

    phase("hidden_kv")
    for i in range(2):
        rows = slice(128 * i, 128 * i + 128)
        for n in range(4):
            r32 = slice(128 * i + 32 * n, 128 * i + 32 * n + 32)
            hid[r32, :] = hidden(lat[r32, :], rsl[r32, :], 0)
        kv = dot(hid[rows, :], wkv[...])
        for q in range(2):
            kt = kv[:, 128 * q : 128 * q + 128]
            vt = kv[:, 256 + 128 * q : 256 + 128 * q + 128]
            kvsend[2 * q, rows] = jnp.where(low, kt, half_swap(vt)).astype(BF16)
            kvsend[2 * q + 1, rows] = jnp.where(low, half_swap(kt), vt).astype(BF16)
    mine = pl.ds(pl.multiple_of((1 + y) * TOK, TOK), TOK)
    kvext[mine, :] = kvsend[y]

    def k_copy(k):
        dy = lax.rem(y + k, NY)
        return remote(kvsend.at[dy], kvext.at[mine, :], ks, kr.at[y], z * NY + dy, tp)

    def k_in(dy):
        rows = pl.ds(pl.multiple_of((1 + dy) * TOK, TOK), TOK)
        return remote(kvsend.at[y], kvext.at[rows, :], ks, kr.at[dy], z * NY + dy, tp)

    for k in (2, 1, 3):
        k_copy(k).start()

    phase("qg")
    drain(wqg, lsem.at[7])
    qg = dot(hid[0:TOK, :], wqg[:, 0:TOK])
    for q in range(2):
        qt = qg[:, 128 * q : 128 * q + 128] * (HD**-0.5)
        up, dn = qt[0:128], qt[128:256]
        qsend[2 * q] = jnp.where(low, up, half_swap(dn)).astype(BF16)
        qsend[2 * q + 1] = jnp.where(low, half_swap(up), dn).astype(BF16)
    qrecv[y] = qsend[y]

    def q_copy(k):
        dy = lax.rem(y + k, NY)
        return remote(qsend.at[dy], qrecv.at[y], qs, qr, z * NY + dy, tp)

    for k in (2, 1, 3):
        q_copy(k).start()
    phase("g")
    g = dot(hid[0:TOK, :], wqg[:, TOK:])
    gbuf[...] = g.astype(BF16).reshape(NX, NC, OUTR, TOK)
    g_copy = remote(gbuf.at[:, 1 - core], gother, gs, gr, sp, partner)
    g_copy.start()
    drain(wo, lsem.at[5])
    w_copy = remote(wo, wo2, ws, wr, sp, partner)
    w_copy.start()

    phase("kq_wait")
    drain(zgrecv.at[pl.ds(0, NZ - 1)], zgr)
    total = zgrecv[0]
    for k in range(1, NZ):
        total = total + zgrecv[k]
    mgsend[...] = total
    mgrecv[group] = total

    for k in G_ORDER:
        remote(mgsend, mgrecv.at[group], mgs, mgr, *group_peer(k)).start()

    up_src = kvext.at[pl.ds(4 * TOK, TOK), :]
    dn_src = kvext.at[pl.ds(TOK, TOK), :]
    up_dst = kvext.at[pl.ds(0, TOK), :]
    dn_dst = kvext.at[pl.ds(5 * TOK, TOK), :]
    up_copy = remote(up_src, up_dst, hs.at[0], hr.at[0], jnp.minimum(z + 1, NZ - 1) * NY + y, tp)
    dn_copy = remote(dn_src, dn_dst, hs.at[1], hr.at[1], jnp.maximum(z - 1, 0) * NY + y, tp)

    @pl.when(y != 3)
    def _():
        k_in(3).wait_recv()

    @pl.when(z < NZ - 1)
    def _():
        up_copy.start()

    @pl.when(y != 0)
    def _():
        k_in(0).wait_recv()

    @pl.when(z > 0)
    def _():
        dn_copy.start()

    @pl.when(y != 1)
    def _():
        k_in(1).wait_recv()

    @pl.when(y != 2)
    def _():
        k_in(2).wait_recv()

    phase("gates")
    g_copy.wait_recv()
    for part in range(2):
        g = (gbuf[:, core] if part == 0 else gother[...]).astype(F32)
        sgate[:, :, TOK * part : TOK * part + TOK] = g * (1.0 / (1.0 + jnp.exp(-g)))
    phase("q_wait")
    drain(qrecv.at[pl.ds(0, NY - 1)], qr)
    phase("c_wait")
    drain(ctxkv.at[pl.ds(0, CTX - NY * CTXL)], cr)
    phase("attention")
    across = lax.rem(x + 2, NX)
    plus, minus = lax.rem(x + 1, NX), lax.rem(x + NX - 1, NX)
    source = core * NY + y
    fold = OUTR // 2

    def r_copy(i, b, h):
        return remote(
            rsend.at[i, b, h], rrecv.at[i, source], rs, rr.at[i], z * NY + b, x * NC + h
        )

    def attend(i, *blocks):
        queries, windows = [], []
        for b in blocks:
            xq = qrecv[b, pl.ds(pl.multiple_of(64 * lax.rem(i, 2), 64), 64), :].astype(F32)
            queries.append(jnp.where(low, jnp.where(i > 1, half_swap(xq), xq), 0.0).astype(BF16))
            row = 4 * b + i
            base = jnp.clip(row0 + row - 4, 0, LAST_START) - row0 + 4
            keys = pl.ds(pl.multiple_of(base * GRID_W, GRID_W), WIN)
            windows.append((keys, jnp.where(row < 4, row, jnp.where(row < 13, 4, row - 8))))
        sc_ctx = dot_nt(jnp.concatenate(queries, axis=0), ctxkv[...])
        sc_win = jnp.concatenate(
            [dot_nt(qp, kvext[keys, :]) + btab[t] for qp, (keys, t) in zip(queries, windows)],
            axis=0,
        )
        top = jnp.maximum(
            jnp.max(sc_ctx, axis=1, keepdims=True), jnp.max(sc_win, axis=1, keepdims=True)
        )
        e_ctx = jnp.exp(sc_ctx - top)
        e_win = jnp.exp(sc_win - top)
        den = jnp.sum(e_ctx, axis=1, keepdims=True) + jnp.sum(e_win, axis=1, keepdims=True)
        e_win = e_win.astype(BF16)
        o_all = dot(e_ctx.astype(BF16), ctxkv[...])
        for n, (b, (keys, t)) in enumerate(zip(blocks, windows)):
            part = slice(64 * n, 64 * n + 64)
            o = (o_all[part] + dot(e_win[part], kvext[keys, :])) * (1.0 / den[part])
            for h in range(NC):
                r0 = o[OUTR * h : OUTR * h + fold]
                r1 = o[OUTR * h + fold : OUTR * h + OUTR]
                rsend[i, b, h] = jnp.where(low, half_swap(r0), r1).astype(BF16)
        for b in blocks:
            for h in range(NC):
                here = (b == y) & (h == core)

                @pl.when(here)
                def _():
                    rrecv[i, source] = rsend[i, b, h]

                @pl.when(jnp.logical_not(here))
                def _():
                    r_copy(i, b, h).start()

    def project(i, name, *steps):
        phase("r_wait_" + name)
        drain(rrecv.at[i, pl.ds(0, NC * NY - 1)], rr.at[i])
        phase("project_" + name)
        for part in range(2):
            src = (core if part == 0 else 1 - core) * NY
            for q in range(2):
                x0, x1 = rrecv[i, src + 2 * q].astype(F32), rrecv[i, src + 2 * q + 1].astype(F32)
                cols = slice(TOK * part + 128 * q, TOK * part + 128 * q + 128)
                up = jnp.where(low, x0, half_swap(x1)) * sgate[i, 0:fold, cols]
                dn = jnp.where(low, half_swap(x0), x1) * sgate[i, fold:OUTR, cols]
                gated[0:fold, cols] = up.astype(BF16)
                gated[fold:OUTR, cols] = dn.astype(BF16)
        for pieces, then in steps:
            for n in pieces:
                cols = slice(512 * n, 512 * n + 512)
                term = dot(gated[:, :TOK], wo[:, cols]) + dot(gated[:, TOK:], wo2[:, cols])
                psend[i, :, cols] = term.astype(BF16)
            then()

    def to_neighbour(src, up, dst, sem):
        remote(src, dst, ps, sem, sp, (plus if up else minus) * NC + core).start()

    def send_across(*pieces):
        for n in pieces:
            src = psend.at[across, :, pl.ds(512 * n, 512)]
            to_neighbour(src, n < 2, hop.at[n], hp.at[n])

    def send_on(up, at, width):
        cols = pl.ds(at, width)
        src = psend.at[plus if up else minus, :, cols]
        to_neighbour(src, up, precv.at[0 if up else 1, :, cols], pr)

    attend(across, 1, 2)
    phase("h_wait")

    @pl.when(z > 0)
    def _():
        up_copy.wait_recv()

    @pl.when(z < NZ - 1)
    def _():
        dn_copy.wait_recv()

    phase("attention2")
    attend(across, 0, 3)
    phase("attention3")
    attend(plus, 0, 3, 1, 2)
    phase("attention4")
    attend(minus, 0, 3, 1, 2)
    phase("attention5")
    attend(x, 0, 3, 1, 2)
    w_copy.wait_recv()
    project(
        across,
        "across",
        ((0, 2), lambda: send_across(0, 2)),
        ((1, 3), lambda: send_across(1, 3)),
    )
    project(plus, "plus", ((2, 3, 0, 1), lambda: send_on(True, D // 2, D // 2)))
    project(minus, "minus", ((0, 1, 2, 3), lambda: send_on(False, 0, D // 2)))
    for n in (0, 2, 1, 3):
        phase(f"hop{n}")
        up, cols = n < 2, slice(512 * n, 512 * n + 512)
        drain(hop.at[n], hp.at[n])
        to = plus if up else minus
        psend[to, :, cols] = (psend[to, :, cols].astype(F32) + hop[n].astype(F32)).astype(BF16)
        send_on(up, 512 * n, 512)

    project(x, "own", ((0, 1, 2, 3), lambda: None))

    phase("sent1")
    drain(zrecv.at[pl.ds(0, NZ - 1)], zs)
    drain(zgrecv.at[pl.ds(0, NZ - 1)], zgs)
    drain(mrecv.at[pl.ds(0, NY * NTP - 1)], ms)
    drain(mgrecv.at[pl.ds(0, NY * NTP - 1)], mgs)
    drain(mgrecv.at[pl.ds(0, NY * NTP - 1)], mgr)
    drain(ctxkv.at[pl.ds(0, CTX - NY * CTXL)], cs)
    drain(ctx.at[pl.ds(0, NY - 1), 0], xs)
    drain(ctx.at[pl.ds(0, NY - 1), 0], xps)
    drain(kvext.at[pl.ds(0, (NY - 1) * TOK)], ks)
    drain(qrecv.at[pl.ds(0, NY - 1)], qs)
    w_copy.wait_send()
    g_copy.wait_send()
    for i in range(NX):
        drain(rrecv.at[i, pl.ds(0, NC * NY - 1)], rs)

    @pl.when(z < NZ - 1)
    def _():
        up_copy.wait_send()

    @pl.when(z > 0)
    def _():
        dn_copy.wait_send()

    for t in range(NTP):
        total = mgrecv[t] + mgrecv[NTP + t] + mgrecv[2 * NTP + t] + mgrecv[3 * NTP + t]
        mod[4:5, 256 * t : 256 * t + 128] = total[0:1]
        mod[4:5, 256 * t + 128 : 256 * t + 256] = total[1:2]
    phase("p_wait")
    drain(precv, pr)
    phase("final")
    branch = psend[x].astype(F32) + precv[0].astype(F32) + precv[1].astype(F32)
    branch = branch.astype(BF16).astype(F32)
    normed = branch * lax.rsqrt(jnp.mean(branch * branch, axis=1, keepdims=True) + EPSILON)
    own = lat[pl.ds(pl.multiple_of(tp * OUTR, OUTR), OUTR), :].astype(F32)
    out_ref[...] = (own + mod[4:5, :] * (normed * mod[6:7, :])).astype(BF16)

    phase("sent")
    drain(psend.at[pl.ds(0, NX - 1)], ps)
    phase(None)


def shards(
    latent,
    context,
    condition,
    context_condition,
    gain_pre,
    gain_post,
    w_shift,
    w_scale,
    w_gate,
    w_query,
    w_key,
    w_value,
    w_silu,
    offset_bias,
    w_out,
):
    in_rows = w_shift.shape[0]
    vmem = pl.BlockSpec(memory_space=pltpu.VMEM)
    hbm = pl.BlockSpec(memory_space=pltpu.HBM)
    dma = pltpu.SemaphoreType.DMA
    operands = (
        condition.reshape(16, 128),
        context_condition.reshape(16, 128),
        gain_pre.reshape(16, 128),
        gain_post.reshape(16, 128),
        jnp.transpose(offset_bias, (1, 0, 2)),
        latent,
        context,
        w_shift,
        w_scale,
        w_gate,
        w_query,
        w_key,
        w_value,
        w_silu,
        w_out,
    )
    operands = [pltpu.with_memory_space_constraint(a, pltpu.HBM) for a in operands]
    return pl.pallas_call(
        kernel,
        name="whole",
        out_shape=jax.ShapeDtypeStruct((OUTR, D), BF16),
        in_specs=[hbm] * 15,
        out_specs=vmem,
        scratch_shapes=[
            pltpu.VMEM((2, 16, 128), BF16),
            pltpu.VMEM((2, 16, 128), F32),
            pltpu.VMEM((2, 16, 128), F32),
            pltpu.VMEM((2 * WIN_ROWS - 1, NY, 2 * WIN_COLS - 1), F32),
            pltpu.VMEM((16, 128), F32),
            pltpu.VMEM((3, in_rows, TOK), BF16),
            pltpu.VMEM((TOK, D), BF16),
            pltpu.VMEM((NY, NC, CTXL // NC, D), BF16),
            pltpu.VMEM((D, 2 * TOK), BF16),
            pltpu.VMEM((D, 128), BF16),
            pltpu.VMEM((D, 2 * TOK), BF16),
            pltpu.VMEM((TOK, D), BF16),
            pltpu.VMEM((TOK, D), BF16),
            pltpu.VMEM((8, 128), F32),
            pltpu.VMEM((NZ, 8, 128), F32),
            pltpu.VMEM((8, 128), F32),
            pltpu.VMEM((NY * NTP, 8, 128), F32),
            pltpu.VMEM((2, 128), F32),
            pltpu.VMEM((NZ, 2, 128), F32),
            pltpu.VMEM((2, 128), F32),
            pltpu.VMEM((NY * NTP, 2, 128), F32),
            pltpu.VMEM((8, D), F32),
            pltpu.VMEM((4, 8, D), F32),
            pltpu.VMEM((TABLES, GRID_W, WIN), F32),
            pltpu.VMEM((TOK, D), BF16),
            pltpu.VMEM((NY * CTXL, D), BF16),
            pltpu.VMEM((TOK, 128), F32),
            pltpu.VMEM((NY * CTXL, 128), F32),
            pltpu.VMEM((CTX, 128), BF16),
            pltpu.VMEM((NY, TOK, 128), BF16),
            pltpu.VMEM((6 * TOK, 128), BF16),
            pltpu.VMEM((NY, 128, 128), BF16),
            pltpu.VMEM((NY, 128, 128), BF16),
            pltpu.VMEM((NX, NC, OUTR, TOK), BF16),
            pltpu.VMEM((NX, OUTR, TOK), BF16),
            pltpu.VMEM((NX, OUTR, NC * TOK), F32),
            pltpu.VMEM((NX, NY, NC, OUTR // 2, 128), BF16),
            pltpu.VMEM((NX, NC * NY, OUTR // 2, 128), BF16),
            pltpu.VMEM((OUTR, NC * TOK), BF16),
            pltpu.VMEM((NX, OUTR, D), BF16),
            pltpu.VMEM((4, OUTR, D // 4), BF16),
            pltpu.VMEM((2, OUTR, D), BF16),
            dma((9,)),
            dma,
            dma,
            dma,
            dma,
            dma,
            dma,
            dma,
            dma,
            dma,
            dma,
            dma,
            dma,
            dma,
            dma,
            dma,
            dma,
            dma,
            dma((NY,)),
            dma,
            dma,
            dma((2,)),
            dma((2,)),
            dma,
            dma((NX,)),
            dma,
            dma,
            dma((4,)),
            dma,
            dma,
        ],
        compiler_params=pltpu.CompilerParams(
            collective_id=0, has_side_effects=True, vmem_limit_bytes=48 << 20
        ),
    )(*operands)


def solution(mesh):
    in_specs = (
        P("sp", None),
        P("sp", None),
        P(),
        P(),
        P(),
        P(),
        P("sp", "tp"),
        P("sp", "tp"),
        P("sp", "tp"),
        P(None, "tp"),
        P(None, "tp"),
        P(None, "tp"),
        P(None, "tp"),
        P("tp", None, None),
        P("tp", None),
    )
    out_specs = P(("sp", "tp"), None)
    return jax.shard_map(shards, mesh=mesh, in_specs=in_specs, out_specs=out_specs, check_vma=False)
```

```python
import functools

import jax
import jax.numpy as jnp
from jax import lax
from jax.experimental import pallas as pl
from jax.experimental.pallas import tpu as pltpu
from jax.sharding import PartitionSpec as P

GRID_W = 64
WIN_ROWS = 8
WIN_COLS = 16
EPSILON = 1e-06
NZ, NY, NX, NC = 8, 4, 4, 2
NTP = NX * NC
D = 2048
HD = 64
TOK = 256
CTXL = 32
CTX = 1024
OUTR = TOK // NTP
LAST_START = NZ * NY * TOK // GRID_W - WIN_ROWS
TABLES = 8
WIN = WIN_ROWS * GRID_W
Z_ORDER = (4, 3, 5, 2, 6, 1, 7)
G_ORDER = sorted(
    ((ky, kx, kc) for ky in range(NY) for kx in range(NX) for kc in range(NC)),
    key=lambda k: -min(k[0], NY - k[0]) - min(k[1], NX - k[1]) - k[2] / 2,
)[:-1]
F32 = jnp.float32
BF16 = jnp.bfloat16
NT = (((1,), (1,)), ((), ()))


def dot(a, b):
    return jnp.dot(a, b, preferred_element_type=F32)


def dot_nt(a, b):
    return lax.dot_general(a, b, NT, preferred_element_type=F32)


def remote(src, dst, ssem, rsem, sp, tp):
    return pltpu.make_async_remote_copy(
        src_ref=src,
        dst_ref=dst,
        send_sem=ssem,
        recv_sem=rsem,
        device_id=(sp, tp),
        device_id_type=pl.DeviceIdType.MESH,
    )


class Phases:
    def __init__(self):
        self.scope = None

    def __call__(self, name):
        if self.scope is not None:
            self.scope.__exit__(None, None, None)
        self.scope = None
        if name:
            self.scope = jax.named_scope(name)
            self.scope.__enter__()


def drain(ref, sem):
    pltpu.make_async_copy(ref, ref, sem).wait()


def half_swap(v):
    return pltpu.roll(v, 64, 1)


def kernel(
    cond_h,
    cond2_h,
    gpre_h,
    gpost_h,
    bias_h,
    lat_h,
    ctx_h,
    wsh_h,
    wsc_h,
    wga_h,
    wq_h,
    wk_h,
    wv_h,
    wg_h,
    wo_h,
    out_ref,
    conds,
    condf,
    gains,
    bias,
    biasx,
    wmod,
    lat,
    ctx,
    wkv,
    wy,
    wqg,
    wo,
    wo2,
    zsend,
    zrecv,
    msend,
    mrecv,
    zgsend,
    zgrecv,
    mgsend,
    mgrecv,
    mod,
    spread,
    btab,
    hid,
    hidc,
    rsl,
    rsc,
    ctxkv,
    kvsend,
    kvext,
    qsend,
    qrecv,
    gbuf,
    gother,
    sgate,
    rsend,
    rrecv,
    gated,
    psend,
    hop,
    precv,
    lsem,
    zs,
    zr,
    ms,
    mr,
    zgs,
    zgr,
    mgs,
    mgr,
    xs,
    xr,
    xps,
    xpr,
    ws,
    wr,
    cs,
    cr,
    ks,
    kr,
    qs,
    qr,
    hs,
    hr,
    rs,
    rr,
    gs,
    gr,
    hp,
    ps,
    pr,
):
    sp = lax.axis_index("sp")
    tp = lax.axis_index("tp")
    z, y = lax.div(sp, NY), lax.rem(sp, NY)
    x, core = lax.div(tp, NC), lax.rem(tp, NC)
    partner = x * NC + (1 - core)
    group = y * NTP + tp
    lane = lax.broadcasted_iota(jnp.int32, (1, 128), 1)
    low = lane < 64

    phase = Phases()
    phase("loads")
    def load(sem, *moves):
        for a, b in moves:
            pltpu.make_async_copy(a, b, lsem.at[sem]).start()

    load(0, (cond_h, conds.at[0]), (cond2_h, conds.at[1]))
    load(1, (wsh_h, wmod.at[0]), (wsc_h, wmod.at[1]), (wga_h, wmod.at[2]))
    half = CTXL // NC
    load(8, *((ctx_h.at[pl.ds(half * h, half), :], ctx.at[y, h]) for h in range(NC)))
    load(2, (lat_h, lat))
    load(3, (gpre_h, gains.at[0]), (gpost_h, gains.at[1]))
    load(4, (bias_h, bias))
    load(5, (wo_h, wo))
    load(6, (wk_h, wkv.at[:, pl.ds(0, TOK)]), (wv_h, wkv.at[:, pl.ds(TOK, TOK)]))
    load(7, (wq_h, wqg.at[:, pl.ds(0, TOK)]), (wg_h, wqg.at[:, pl.ds(TOK, TOK)]))

    phase("greet")
    barrier = pltpu.get_barrier_semaphore()

    def greet(dsp, dtp):
        pl.semaphore_signal(
            barrier, inc=1, device_id=(dsp, dtp), device_id_type=pl.DeviceIdType.MESH
        )

    for k in Z_ORDER:
        greet(lax.rem(z + k, NZ) * NY + y, tp)

    def group_peer(k):
        dx, dc = lax.rem(x + k[1], NX), 1 - core if k[2] else core
        return z * NY + lax.rem(y + k[0], NY), dx * NC + dc

    for k in G_ORDER:
        greet(*group_peer(k))

    phase("partial")
    drain(conds, lsem.at[0])
    v = conds[...].astype(F32)
    condf[...] = v * (1.0 / (1.0 + jnp.exp(-v)))
    line = jnp.concatenate([condf[i, pl.ds(lax.div(sp, 2), 1), :] for i in range(2)], axis=0)
    line = jnp.where(lax.rem(sp, 2) == 1, half_swap(line), line)[:, :64]
    act = jnp.concatenate([line, jnp.zeros((6, 64), F32)], axis=0).astype(BF16)
    drain(wmod, lsem.at[1])
    sh = dot(act, wmod[0])
    sc = dot(act, wmod[1])
    ga = dot(act, wmod[2])
    zsend[0:2] = sh[0:2, :128]
    zsend[2:4] = sc[0:2, :128]
    zsend[4:6] = sh[0:2, 128:]
    zsend[6:8] = sc[0:2, 128:]
    zgsend[0:1] = ga[0:1, :128]
    zgsend[1:2] = ga[0:1, 128:]
    zrecv[z] = zsend[...]
    zgrecv[z] = zgsend[...]

    phase("barrier")
    pl.semaphore_wait(barrier, NZ - 1 + NY * NTP - 1)

    phase("z_start")
    def z_copy(k):
        dz = lax.rem(z + k, NZ)
        return remote(zsend, zrecv.at[z], zs, zr, dz * NY + y, tp)

    def zg_copy(k):
        dz = lax.rem(z + k, NZ)
        return remote(zgsend, zgrecv.at[z], zgs, zgr, dz * NY + y, tp)

    for k in Z_ORDER:
        z_copy(k).start()
    for k in Z_ORDER:
        zg_copy(k).start()

    def x_copy(k):
        dy = lax.rem(y + k, NY)
        return remote(ctx.at[y, core], ctx.at[y, core], xs, xr, z * NY + dy, tp)

    def x_pass(k):
        rows = ctx.at[lax.rem(y + k, NY), core]
        return remote(rows, rows, xps, xpr, sp, partner)

    drain(ctx.at[0], lsem.at[8])
    for k in (2, 1, 3):
        x_copy(k).start()

    phase("stats")
    drain(lat, lsem.at[2])

    def stats(v):
        r = lax.rsqrt(jnp.mean(v * v, axis=1, keepdims=True) + EPSILON)
        return jnp.broadcast_to(r, (v.shape[0], 128))

    def row_stats(i, c):
        rows = pl.ds(pl.multiple_of(i * 32, 32), 32)
        rsl[rows, :] = stats(lat[rows, :].astype(F32))
        return c

    lax.fori_loop(0, TOK // 32, row_stats, 0)
    drain(gains, lsem.at[3])
    for t in range(16):
        mod[5:6, 128 * t : 128 * t + 128] = gains[0, t : t + 1, :]
        mod[6:7, 128 * t : 128 * t + 128] = gains[1, t : t + 1, :]
    drain(bias, lsem.at[4])
    biasx[...] = jnp.zeros((16, 128), F32)
    for d in range(2 * WIN_ROWS - 1):
        line = bias[d, pl.ds(y, 1), :]
        biasx[d : d + 1, 0:31] = line
        if d > 0:
            biasx[d - 1 : d, 64:95] = line

    phase("z_wait")
    drain(zrecv.at[pl.ds(0, NZ - 1)], zr)
    phase("m_start")
    total = zrecv[0]
    for k in range(1, NZ):
        total = total + zrecv[k]
    msend[...] = total
    mrecv[group] = total

    for k in G_ORDER:
        remote(msend, mrecv.at[group], ms, mr, *group_peer(k)).start()

    phase("tables")
    col = lax.rem(lax.broadcasted_iota(jnp.int32, (64, 128), 1), 64)
    qcol = lax.broadcasted_iota(jnp.int32, (64, 128), 0)
    first_col = jnp.clip(qcol - WIN_COLS // 2, 0, GRID_W - WIN_COLS)
    in_cols = (col >= first_col) & (col < first_col + WIN_COLS)
    row0 = z * 16

    def table(t, c):
        row = row0 + jnp.where(t < 5, t, t + 8)
        d0 = jnp.clip(row - 4, 0, LAST_START) - row + 7
        for m in range(WIN_ROWS // 2):
            line = biasx[pl.ds(d0 + 2 * m, 1), :]
            tile = pltpu.roll(
                jnp.broadcast_to(line, (64, 128)), 113, 1, stride=1, stride_axis=0
            )
            btab[t, :, m * 128 : m * 128 + 128] = jnp.where(in_cols, tile, -jnp.inf)
        return c

    lax.fori_loop(0, TABLES, table, 0)

    @pl.when(z == 0)
    def _():
        kvext[0:TOK] = jnp.zeros((TOK, 128), BF16)

    @pl.when(z == NZ - 1)
    def _():
        kvext[5 * TOK : 6 * TOK] = jnp.zeros((TOK, 128), BF16)

    phase("x_wait")
    drain(ctx.at[pl.ds(0, NY - 1), 0], xr)
    for k in (1, 2, 3):
        x_pass(k).start()

    phase("wy")
    drain(wkv, lsem.at[6])

    def head_columns(i, c):
        rows = pl.ds(pl.multiple_of(i * 256, 256), 256)
        at = 128 * lax.div(y, 2)
        kt = wkv[rows, pl.ds(pl.multiple_of(at, 128), 128)].astype(F32)
        vt = wkv[rows, pl.ds(pl.multiple_of(TOK + at, 128), 128)].astype(F32)
        odd = lax.rem(y, 2) == 1
        wy[rows, :] = jnp.where(
            low, jnp.where(odd, half_swap(kt), kt), jnp.where(odd, vt, half_swap(vt))
        ).astype(BF16)
        return c

    lax.fori_loop(0, D // 256, head_columns, 0)
    phase("x_wait2")
    drain(ctx.at[pl.ds(0, NY - 1), 0], xpr)
    for b in range(NY):
        rows = slice(CTXL * b, CTXL * b + CTXL)
        rsc[rows, :] = stats(ctx[b].reshape(CTXL, D).astype(F32))

    phase("m_wait")
    drain(mrecv.at[pl.ds(0, NY * NTP - 1)], mr)
    phase("mod")
    for t in range(NTP):
        total = mrecv[t] + mrecv[NTP + t] + mrecv[2 * NTP + t] + mrecv[3 * NTP + t]
        lo, hi = 256 * t, 256 * t + 128
        mod[0:4, lo : lo + 128] = total[0:4]
        mod[0:4, hi : hi + 128] = total[4:8]
    mod[2:3, :] = mod[5:6, :] * (1.0 + mod[2:3, :])
    mod[3:4, :] = mod[5:6, :] * (1.0 + mod[3:4, :])

    for i in range(4):
        spread[i] = jnp.broadcast_to(mod[i : i + 1, :], (8, D))

    def hidden(v, r, which):
        n = v.shape[0] // 8
        r = r.reshape(n, 8, 128)
        parts = []
        for t in range(D // 128):
            cols = slice(128 * t, 128 * t + 128)
            u = v[:, cols].astype(F32).reshape(n, 8, 128) * r
            u = u * spread[2 + which, :, cols] + spread[which, :, cols]
            parts.append(u.reshape(8 * n, 128).astype(BF16))
        return jnp.concatenate(parts, axis=1)

    phase("ctx_hidden")
    for b in range(NY):
        rows = slice(CTXL * b, CTXL * b + CTXL)
        hidc[rows, :] = hidden(ctx[b].reshape(CTXL, D), rsc[rows, :], 1)
    phase("ctx_kv")
    here = pl.ds(pl.multiple_of(z * NY * CTXL, NY * CTXL), NY * CTXL)
    ctxkv[here, :] = dot(hidc[...], wy[...]).astype(BF16)

    def c_copy(k):
        dz = lax.rem(z + k, NZ)
        return remote(ctxkv.at[here, :], ctxkv.at[here, :], cs, cr, dz * NY + y, tp)

    for k in Z_ORDER:
        c_copy(k).start()

    phase("hidden_kv")

    def k_copy(k, i):
        dy = lax.rem(y + k, NY)
        at = pl.ds(pl.multiple_of((1 + y) * TOK + 128 * i, 128), 128)
        src = kvsend.at[dy, pl.ds(128 * i, 128), :]
        return remote(src, kvext.at[at, :], ks, kr.at[y], z * NY + dy, tp)

    for i in range(2):
        rows = slice(128 * i, 128 * i + 128)
        for n in range(4):
            r32 = slice(128 * i + 32 * n, 128 * i + 32 * n + 32)
            hid[r32, :] = hidden(lat[r32, :], rsl[r32, :], 0)
        kv = dot(hid[rows, :], wkv[...])
        for q in range(2):
            kt = kv[:, 128 * q : 128 * q + 128]
            vt = kv[:, 256 + 128 * q : 256 + 128 * q + 128]
            kvsend[2 * q, rows] = jnp.where(low, kt, half_swap(vt)).astype(BF16)
            kvsend[2 * q + 1, rows] = jnp.where(low, half_swap(kt), vt).astype(BF16)
        for k in (2, 1, 3):
            k_copy(k, i).start()
        kvext[pl.ds(pl.multiple_of((1 + y) * TOK + 128 * i, 128), 128), :] = kvsend[y, rows]

    def k_in(dy):
        rows = pl.ds(pl.multiple_of((1 + dy) * TOK, TOK), TOK)
        return remote(kvsend.at[y], kvext.at[rows, :], ks, kr.at[dy], z * NY + dy, tp)


    phase("qg")
    drain(wqg, lsem.at[7])
    qg = dot(hid[0:TOK, :], wqg[:, 0:TOK])
    for q in range(2):
        qt = qg[:, 128 * q : 128 * q + 128] * (HD**-0.5)
        up, dn = qt[0:128], qt[128:256]
        qsend[2 * q] = jnp.where(low, up, half_swap(dn)).astype(BF16)
        qsend[2 * q + 1] = jnp.where(low, half_swap(up), dn).astype(BF16)
    qrecv[y] = qsend[y]

    def q_copy(k):
        dy = lax.rem(y + k, NY)
        return remote(qsend.at[dy], qrecv.at[y], qs, qr, z * NY + dy, tp)

    for k in (2, 1, 3):
        q_copy(k).start()
    phase("g")
    g = dot(hid[0:TOK, :], wqg[:, TOK:])
    gbuf[...] = g.astype(BF16).reshape(NX, NC, OUTR, TOK)
    g_copy = remote(gbuf.at[:, 1 - core], gother, gs, gr, sp, partner)
    g_copy.start()
    drain(wo, lsem.at[5])
    w_copy = remote(wo, wo2, ws, wr, sp, partner)
    w_copy.start()

    phase("kq_wait")
    drain(zgrecv.at[pl.ds(0, NZ - 1)], zgr)
    total = zgrecv[0]
    for k in range(1, NZ):
        total = total + zgrecv[k]
    mgsend[...] = total
    mgrecv[group] = total

    for k in G_ORDER:
        remote(mgsend, mgrecv.at[group], mgs, mgr, *group_peer(k)).start()

    up_src = kvext.at[pl.ds(4 * TOK, TOK), :]
    dn_src = kvext.at[pl.ds(TOK, TOK), :]
    up_dst = kvext.at[pl.ds(0, TOK), :]
    dn_dst = kvext.at[pl.ds(5 * TOK, TOK), :]
    up_copy = remote(up_src, up_dst, hs.at[0], hr.at[0], jnp.minimum(z + 1, NZ - 1) * NY + y, tp)
    dn_copy = remote(dn_src, dn_dst, hs.at[1], hr.at[1], jnp.maximum(z - 1, 0) * NY + y, tp)

    @pl.when(y != 3)
    def _():
        k_in(3).wait_recv()

    @pl.when(z < NZ - 1)
    def _():
        up_copy.start()

    @pl.when(y != 0)
    def _():
        k_in(0).wait_recv()

    @pl.when(z > 0)
    def _():
        dn_copy.start()

    @pl.when(y != 1)
    def _():
        k_in(1).wait_recv()

    @pl.when(y != 2)
    def _():
        k_in(2).wait_recv()

    phase("gates")
    g_copy.wait_recv()
    for part in range(2):
        g = (gbuf[:, core] if part == 0 else gother[...]).astype(F32)
        sgate[:, :, TOK * part : TOK * part + TOK] = g * (1.0 / (1.0 + jnp.exp(-g)))
    phase("q_wait")
    drain(qrecv.at[pl.ds(0, NY - 1)], qr)
    phase("c_wait")
    drain(ctxkv.at[pl.ds(0, CTX - NY * CTXL)], cr)
    phase("attention")
    across = lax.rem(x + 2, NX)
    plus, minus = lax.rem(x + 1, NX), lax.rem(x + NX - 1, NX)
    source = core * NY + y
    fold = OUTR // 2

    def r_copy(i, b, h):
        return remote(
            rsend.at[i, b, h], rrecv.at[i, source], rs, rr.at[i], z * NY + b, x * NC + h
        )

    def attend(i, *blocks):
        queries, windows = [], []
        for b in blocks:
            xq = qrecv[b, pl.ds(pl.multiple_of(64 * lax.rem(i, 2), 64), 64), :].astype(F32)
            queries.append(jnp.where(low, jnp.where(i > 1, half_swap(xq), xq), 0.0).astype(BF16))
            row = 4 * b + i
            base = jnp.clip(row0 + row - 4, 0, LAST_START) - row0 + 4
            keys = pl.ds(pl.multiple_of(base * GRID_W, GRID_W), WIN)
            windows.append((keys, jnp.where(row < 4, row, jnp.where(row < 13, 4, row - 8))))
        sc_ctx = dot_nt(jnp.concatenate(queries, axis=0), ctxkv[...])
        sc_win = jnp.concatenate(
            [dot_nt(qp, kvext[keys, :]) + btab[t] for qp, (keys, t) in zip(queries, windows)],
            axis=0,
        )
        top = jnp.maximum(
            jnp.max(sc_ctx, axis=1, keepdims=True), jnp.max(sc_win, axis=1, keepdims=True)
        )
        e_ctx = jnp.exp(sc_ctx - top)
        e_win = jnp.exp(sc_win - top)
        den = jnp.sum(e_ctx, axis=1, keepdims=True) + jnp.sum(e_win, axis=1, keepdims=True)
        e_win = e_win.astype(BF16)
        o_all = dot(e_ctx.astype(BF16), ctxkv[...])
        for n, (b, (keys, t)) in enumerate(zip(blocks, windows)):
            part = slice(64 * n, 64 * n + 64)
            o = (o_all[part] + dot(e_win[part], kvext[keys, :])) * (1.0 / den[part])
            for h in range(NC):
                r0 = o[OUTR * h : OUTR * h + fold]
                r1 = o[OUTR * h + fold : OUTR * h + OUTR]
                rsend[i, b, h] = jnp.where(low, half_swap(r0), r1).astype(BF16)
        for b in blocks:
            for h in range(NC):
                here = (b == y) & (h == core)

                @pl.when(here)
                def _():
                    rrecv[i, source] = rsend[i, b, h]

                @pl.when(jnp.logical_not(here))
                def _():
                    r_copy(i, b, h).start()

    def gate(i, name, at):
        phase("r_wait_" + name)
        drain(rrecv.at[i, pl.ds(0, NC * NY - 1)], rr.at[i])
        phase("project_" + name)
        for part in range(2):
            src = (core if part == 0 else 1 - core) * NY
            for q in range(2):
                x0, x1 = rrecv[i, src + 2 * q].astype(F32), rrecv[i, src + 2 * q + 1].astype(F32)
                cols = slice(TOK * part + 128 * q, TOK * part + 128 * q + 128)
                up = jnp.where(low, x0, half_swap(x1)) * sgate[i, 0:fold, cols]
                dn = jnp.where(low, half_swap(x0), x1) * sgate[i, fold:OUTR, cols]
                gated[at : at + fold, cols] = up.astype(BF16)
                gated[at + fold : at + OUTR, cols] = dn.astype(BF16)

    def project(targets, at, *pieces):
        rows = slice(at, at + OUTR * len(targets))
        for n in pieces:
            cols = slice(512 * n, 512 * n + 512)
            term = dot(gated[rows, :TOK], wo[:, cols]) + dot(gated[rows, TOK:], wo2[:, cols])
            for m, i in enumerate(targets):
                psend[i, :, cols] = term[OUTR * m : OUTR * m + OUTR].astype(BF16)

    def to_neighbour(src, up, dst, sem):
        remote(src, dst, ps, sem, sp, (plus if up else minus) * NC + core).start()

    def send_across(*pieces):
        for n in pieces:
            src = psend.at[across, :, pl.ds(512 * n, 512)]
            to_neighbour(src, n < 2, hop.at[n], hp.at[n])

    def send_on(up, at, width):
        cols = pl.ds(at, width)
        src = psend.at[plus if up else minus, :, cols]
        to_neighbour(src, up, precv.at[0 if up else 1, :, cols], pr)

    attend(across, 1, 2)
    phase("h_wait")

    @pl.when(z > 0)
    def _():
        up_copy.wait_recv()

    @pl.when(z < NZ - 1)
    def _():
        dn_copy.wait_recv()

    phase("attention2")
    attend(across, 0, 3)
    phase("attention3")
    attend(plus, 0, 3, 1, 2)
    phase("attention4")
    attend(minus, 0, 3, 1, 2)
    phase("attention5")
    attend(x, 0, 3, 1, 2)
    w_copy.wait_recv()
    gate(across, "across", 0)
    project((across,), 0, 0, 2)
    send_across(0, 2)
    project((across,), 0, 1, 3)
    send_across(1, 3)
    gate(plus, "plus", OUTR)
    project((plus,), OUTR, 2, 3)
    send_on(True, D // 2, D // 2)
    gate(minus, "minus", 2 * OUTR)
    project((plus, minus), OUTR, 0, 1)
    send_on(False, 0, D // 2)

    def add_and_send(n):
        phase(f"hop{n}")
        up, cols = n < 2, slice(512 * n, 512 * n + 512)
        drain(hop.at[n], hp.at[n])
        to = plus if up else minus
        psend[to, :, cols] = (psend[to, :, cols].astype(F32) + hop[n].astype(F32)).astype(BF16)
        send_on(up, 512 * n, 512)

    phase("rest")
    project((minus,), 2 * OUTR, 2, 3)
    for n in (0, 2, 1, 3):
        add_and_send(n)
    gate(x, "own", 0)
    project((x,), 0, 0, 1, 2, 3)

    phase("sent1")
    drain(zrecv.at[pl.ds(0, NZ - 1)], zs)
    drain(zgrecv.at[pl.ds(0, NZ - 1)], zgs)
    drain(mrecv.at[pl.ds(0, NY * NTP - 1)], ms)
    drain(mgrecv.at[pl.ds(0, NY * NTP - 1)], mgs)
    drain(mgrecv.at[pl.ds(0, NY * NTP - 1)], mgr)
    drain(ctxkv.at[pl.ds(0, CTX - NY * CTXL)], cs)
    drain(ctx.at[pl.ds(0, NY - 1), 0], xs)
    drain(ctx.at[pl.ds(0, NY - 1), 0], xps)
    drain(kvext.at[pl.ds(0, (NY - 1) * TOK)], ks)
    drain(qrecv.at[pl.ds(0, NY - 1)], qs)
    w_copy.wait_send()
    g_copy.wait_send()
    for i in range(NX):
        drain(rrecv.at[i, pl.ds(0, NC * NY - 1)], rs)

    @pl.when(z < NZ - 1)
    def _():
        up_copy.wait_send()

    @pl.when(z > 0)
    def _():
        dn_copy.wait_send()

    for t in range(NTP):
        total = mgrecv[t] + mgrecv[NTP + t] + mgrecv[2 * NTP + t] + mgrecv[3 * NTP + t]
        mod[4:5, 256 * t : 256 * t + 128] = total[0:1]
        mod[4:5, 256 * t + 128 : 256 * t + 256] = total[1:2]
    phase("p_wait")
    drain(precv, pr)
    phase("final")
    branch = psend[x].astype(F32) + precv[0].astype(F32) + precv[1].astype(F32)
    branch = branch.astype(BF16).astype(F32)
    normed = branch * lax.rsqrt(jnp.mean(branch * branch, axis=1, keepdims=True) + EPSILON)
    own = lat[pl.ds(pl.multiple_of(tp * OUTR, OUTR), OUTR), :].astype(F32)
    out_ref[...] = (own + mod[4:5, :] * (normed * mod[6:7, :])).astype(BF16)

    phase("sent")
    drain(psend.at[pl.ds(0, NX - 1)], ps)
    phase(None)


def shards(
    latent,
    context,
    condition,
    context_condition,
    gain_pre,
    gain_post,
    w_shift,
    w_scale,
    w_gate,
    w_query,
    w_key,
    w_value,
    w_silu,
    offset_bias,
    w_out,
):
    in_rows = w_shift.shape[0]
    vmem = pl.BlockSpec(memory_space=pltpu.VMEM)
    hbm = pl.BlockSpec(memory_space=pltpu.HBM)
    dma = pltpu.SemaphoreType.DMA
    operands = (
        condition.reshape(16, 128),
        context_condition.reshape(16, 128),
        gain_pre.reshape(16, 128),
        gain_post.reshape(16, 128),
        jnp.transpose(offset_bias, (1, 0, 2)),
        latent,
        context,
        w_shift,
        w_scale,
        w_gate,
        w_query,
        w_key,
        w_value,
        w_silu,
        w_out,
    )
    operands = [pltpu.with_memory_space_constraint(a, pltpu.HBM) for a in operands]
    return pl.pallas_call(
        kernel,
        name="whole",
        out_shape=jax.ShapeDtypeStruct((OUTR, D), BF16),
        in_specs=[hbm] * 15,
        out_specs=vmem,
        scratch_shapes=[
            pltpu.VMEM((2, 16, 128), BF16),
            pltpu.VMEM((2, 16, 128), F32),
            pltpu.VMEM((2, 16, 128), F32),
            pltpu.VMEM((2 * WIN_ROWS - 1, NY, 2 * WIN_COLS - 1), F32),
            pltpu.VMEM((16, 128), F32),
            pltpu.VMEM((3, in_rows, TOK), BF16),
            pltpu.VMEM((TOK, D), BF16),
            pltpu.VMEM((NY, NC, CTXL // NC, D), BF16),
            pltpu.VMEM((D, 2 * TOK), BF16),
            pltpu.VMEM((D, 128), BF16),
            pltpu.VMEM((D, 2 * TOK), BF16),
            pltpu.VMEM((TOK, D), BF16),
            pltpu.VMEM((TOK, D), BF16),
            pltpu.VMEM((8, 128), F32),
            pltpu.VMEM((NZ, 8, 128), F32),
            pltpu.VMEM((8, 128), F32),
            pltpu.VMEM((NY * NTP, 8, 128), F32),
            pltpu.VMEM((2, 128), F32),
            pltpu.VMEM((NZ, 2, 128), F32),
            pltpu.VMEM((2, 128), F32),
            pltpu.VMEM((NY * NTP, 2, 128), F32),
            pltpu.VMEM((8, D), F32),
            pltpu.VMEM((4, 8, D), F32),
            pltpu.VMEM((TABLES, GRID_W, WIN), F32),
            pltpu.VMEM((TOK, D), BF16),
            pltpu.VMEM((NY * CTXL, D), BF16),
            pltpu.VMEM((TOK, 128), F32),
            pltpu.VMEM((NY * CTXL, 128), F32),
            pltpu.VMEM((CTX, 128), BF16),
            pltpu.VMEM((NY, TOK, 128), BF16),
            pltpu.VMEM((6 * TOK, 128), BF16),
            pltpu.VMEM((NY, 128, 128), BF16),
            pltpu.VMEM((NY, 128, 128), BF16),
            pltpu.VMEM((NX, NC, OUTR, TOK), BF16),
            pltpu.VMEM((NX, OUTR, TOK), BF16),
            pltpu.VMEM((NX, OUTR, NC * TOK), F32),
            pltpu.VMEM((NX, NY, NC, OUTR // 2, 128), BF16),
            pltpu.VMEM((NX, NC * NY, OUTR // 2, 128), BF16),
            pltpu.VMEM((3 * OUTR, NC * TOK), BF16),
            pltpu.VMEM((NX, OUTR, D), BF16),
            pltpu.VMEM((4, OUTR, D // 4), BF16),
            pltpu.VMEM((2, OUTR, D), BF16),
            dma((9,)),
            dma,
            dma,
            dma,
            dma,
            dma,
            dma,
            dma,
            dma,
            dma,
            dma,
            dma,
            dma,
            dma,
            dma,
            dma,
            dma,
            dma,
            dma((NY,)),
            dma,
            dma,
            dma((2,)),
            dma((2,)),
            dma,
            dma((NX,)),
            dma,
            dma,
            dma((4,)),
            dma,
            dma,
        ],
        compiler_params=pltpu.CompilerParams(
            collective_id=0, has_side_effects=True, vmem_limit_bytes=48 << 20
        ),
    )(*operands)


def solution(mesh):
    in_specs = (
        P("sp", None),
        P("sp", None),
        P(),
        P(),
        P(),
        P(),
        P("sp", "tp"),
        P("sp", "tp"),
        P("sp", "tp"),
        P(None, "tp"),
        P(None, "tp"),
        P(None, "tp"),
        P(None, "tp"),
        P("tp", None, None),
        P("tp", None),
    )
    out_specs = P(("sp", "tp"), None)
    return jax.shard_map(shards, mesh=mesh, in_specs=in_specs, out_specs=out_specs, check_vma=False)
```

```python
import functools

import jax
import jax.numpy as jnp
from jax import lax
from jax.experimental import pallas as pl
from jax.experimental.pallas import tpu as pltpu
from jax.sharding import PartitionSpec as P

GRID_W = 64
WIN_ROWS = 8
WIN_COLS = 16
EPSILON = 1e-06
NZ, NY, NX, NC = 8, 4, 4, 2
NTP = NX * NC
D = 2048
HD = 64
TOK = 256
CTXL = 32
CTX = 1024
OUTR = TOK // NTP
LAST_START = NZ * NY * TOK // GRID_W - WIN_ROWS
TABLES = 8
WIN = WIN_ROWS * GRID_W
Z_ORDER = (4, 3, 5, 2, 6, 1, 7)
G_ORDER = sorted(
    ((ky, kx, kc) for ky in range(NY) for kx in range(NX) for kc in range(NC)),
    key=lambda k: -min(k[0], NY - k[0]) - min(k[1], NX - k[1]) - k[2] / 2,
)[:-1]
F32 = jnp.float32
BF16 = jnp.bfloat16
NT = (((1,), (1,)), ((), ()))


def dot(a, b):
    return jnp.dot(a, b, preferred_element_type=F32)


def dot_nt(a, b):
    return lax.dot_general(a, b, NT, preferred_element_type=F32)


def remote(src, dst, ssem, rsem, sp, tp):
    return pltpu.make_async_remote_copy(
        src_ref=src,
        dst_ref=dst,
        send_sem=ssem,
        recv_sem=rsem,
        device_id=(sp, tp),
        device_id_type=pl.DeviceIdType.MESH,
    )


class Phases:
    def __init__(self):
        self.scope = None

    def __call__(self, name):
        if self.scope is not None:
            self.scope.__exit__(None, None, None)
        self.scope = None
        if name:
            self.scope = jax.named_scope(name)
            self.scope.__enter__()


def drain(ref, sem):
    pltpu.make_async_copy(ref, ref, sem).wait()


def half_swap(v):
    return pltpu.roll(v, 64, 1)


def kernel(
    cond_h,
    cond2_h,
    gpre_h,
    gpost_h,
    bias_h,
    lat_h,
    ctx_h,
    wsh_h,
    wsc_h,
    wga_h,
    wq_h,
    wk_h,
    wv_h,
    wg_h,
    wo_h,
    out_ref,
    conds,
    condf,
    gains,
    bias,
    biasx,
    wmod,
    lat,
    ctx,
    wkv,
    wy,
    wqg,
    wo,
    wo2,
    zsend,
    zrecv,
    msend,
    mrecv,
    zgsend,
    zgrecv,
    mgsend,
    mgrecv,
    mod,
    spread,
    btab,
    hid,
    hidc,
    rsl,
    rsc,
    ctxkv,
    kvsend,
    kvext,
    qsend,
    qrecv,
    gbuf,
    gother,
    sgate,
    rsend,
    rrecv,
    gated,
    psend,
    hop,
    precv,
    lsem,
    zs,
    zr,
    ms,
    mr,
    zgs,
    zgr,
    mgs,
    mgr,
    xs,
    xr,
    xps,
    xpr,
    ws,
    wr,
    cs,
    cr,
    ks,
    kr,
    qs,
    qr,
    hs,
    hr,
    rs,
    rr,
    gs,
    gr,
    hp,
    ps,
    pr,
):
    sp = lax.axis_index("sp")
    tp = lax.axis_index("tp")
    z, y = lax.div(sp, NY), lax.rem(sp, NY)
    x, core = lax.div(tp, NC), lax.rem(tp, NC)
    partner = x * NC + (1 - core)
    group = y * NTP + tp
    lane = lax.broadcasted_iota(jnp.int32, (1, 128), 1)
    low = lane < 64

    phase = Phases()
    phase("loads")
    def load(sem, *moves):
        for a, b in moves:
            pltpu.make_async_copy(a, b, lsem.at[sem]).start()

    load(0, (cond_h, conds.at[0]), (cond2_h, conds.at[1]))
    load(1, (wsh_h, wmod.at[0]), (wsc_h, wmod.at[1]), (wga_h, wmod.at[2]))
    half = CTXL // NC
    load(8, *((ctx_h.at[pl.ds(half * h, half), :], ctx.at[y, h]) for h in range(NC)))
    load(2, (lat_h, lat))
    load(3, (gpre_h, gains.at[0]), (gpost_h, gains.at[1]))
    load(4, (bias_h, bias))
    load(5, (wo_h, wo))
    load(6, (wk_h, wkv.at[:, pl.ds(0, TOK)]), (wv_h, wkv.at[:, pl.ds(TOK, TOK)]))
    load(7, (wq_h, wqg.at[:, pl.ds(0, TOK)]), (wg_h, wqg.at[:, pl.ds(TOK, TOK)]))

    phase("greet")
    barrier = pltpu.get_barrier_semaphore()

    def greet(dsp, dtp):
        pl.semaphore_signal(
            barrier, inc=1, device_id=(dsp, dtp), device_id_type=pl.DeviceIdType.MESH
        )

    for k in Z_ORDER:
        greet(lax.rem(z + k, NZ) * NY + y, tp)

    def group_peer(k):
        dx, dc = lax.rem(x + k[1], NX), 1 - core if k[2] else core
        return z * NY + lax.rem(y + k[0], NY), dx * NC + dc

    for k in G_ORDER:
        greet(*group_peer(k))

    phase("partial")
    drain(conds, lsem.at[0])
    v = conds[...].astype(F32)
    condf[...] = v * (1.0 / (1.0 + jnp.exp(-v)))
    line = jnp.concatenate([condf[i, pl.ds(lax.div(sp, 2), 1), :] for i in range(2)], axis=0)
    line = jnp.where(lax.rem(sp, 2) == 1, half_swap(line), line)[:, :64]
    act = jnp.concatenate([line, jnp.zeros((6, 64), F32)], axis=0).astype(BF16)
    drain(wmod, lsem.at[1])
    sh = dot(act, wmod[0])
    sc = dot(act, wmod[1])
    ga = dot(act, wmod[2])
    zsend[0:2] = sh[0:2, :128]
    zsend[2:4] = sc[0:2, :128]
    zsend[4:6] = sh[0:2, 128:]
    zsend[6:8] = sc[0:2, 128:]
    zgsend[0:1] = ga[0:1, :128]
    zgsend[1:2] = ga[0:1, 128:]
    zrecv[z] = zsend[...]
    zgrecv[z] = zgsend[...]

    phase("barrier")
    pl.semaphore_wait(barrier, NZ - 1 + NY * NTP - 1)

    phase("z_start")
    def z_copy(k):
        dz = lax.rem(z + k, NZ)
        return remote(zsend, zrecv.at[z], zs, zr, dz * NY + y, tp)

    def zg_copy(k):
        dz = lax.rem(z + k, NZ)
        return remote(zgsend, zgrecv.at[z], zgs, zgr, dz * NY + y, tp)

    for k in Z_ORDER:
        z_copy(k).start()
    for k in Z_ORDER:
        zg_copy(k).start()

    def x_copy(k):
        dy = lax.rem(y + k, NY)
        return remote(ctx.at[y, core], ctx.at[y, core], xs, xr, z * NY + dy, tp)

    def x_pass(k):
        rows = ctx.at[lax.rem(y + k, NY), core]
        return remote(rows, rows, xps, xpr, sp, partner)

    drain(ctx.at[0], lsem.at[8])
    for k in (2, 1, 3):
        x_copy(k).start()

    phase("stats")
    drain(lat, lsem.at[2])

    def stats(v):
        r = lax.rsqrt(jnp.mean(v * v, axis=1, keepdims=True) + EPSILON)
        return jnp.broadcast_to(r, (v.shape[0], 128))

    def row_stats(i, c):
        rows = pl.ds(pl.multiple_of(i * 32, 32), 32)
        rsl[rows, :] = stats(lat[rows, :].astype(F32))
        return c

    lax.fori_loop(0, TOK // 32, row_stats, 0)
    drain(gains, lsem.at[3])
    for t in range(16):
        mod[5:6, 128 * t : 128 * t + 128] = gains[0, t : t + 1, :]
        mod[6:7, 128 * t : 128 * t + 128] = gains[1, t : t + 1, :]
    drain(bias, lsem.at[4])
    biasx[...] = jnp.zeros((16, 128), F32)
    for d in range(2 * WIN_ROWS - 1):
        line = bias[d, pl.ds(y, 1), :]
        biasx[d : d + 1, 0:31] = line
        if d > 0:
            biasx[d - 1 : d, 64:95] = line

    phase("z_wait")
    drain(zrecv.at[pl.ds(0, NZ - 1)], zr)
    phase("m_start")
    total = zrecv[0]
    for k in range(1, NZ):
        total = total + zrecv[k]
    msend[...] = total
    mrecv[group] = total

    for k in G_ORDER:
        remote(msend, mrecv.at[group], ms, mr, *group_peer(k)).start()

    phase("tables")
    col = lax.rem(lax.broadcasted_iota(jnp.int32, (64, 128), 1), 64)
    qcol = lax.broadcasted_iota(jnp.int32, (64, 128), 0)
    first_col = jnp.clip(qcol - WIN_COLS // 2, 0, GRID_W - WIN_COLS)
    in_cols = (col >= first_col) & (col < first_col + WIN_COLS)
    row0 = z * 16

    def table(t, c):
        row = row0 + jnp.where(t < 5, t, t + 8)
        d0 = jnp.clip(row - 4, 0, LAST_START) - row + 7
        for m in range(WIN_ROWS // 2):
            line = biasx[pl.ds(d0 + 2 * m, 1), :]
            tile = pltpu.roll(
                jnp.broadcast_to(line, (64, 128)), 113, 1, stride=1, stride_axis=0
            )
            btab[t, :, m * 128 : m * 128 + 128] = jnp.where(in_cols, tile, -jnp.inf)
        return c

    lax.fori_loop(0, TABLES, table, 0)

    @pl.when(z == 0)
    def _():
        kvext[0:TOK] = jnp.zeros((TOK, 128), BF16)

    @pl.when(z == NZ - 1)
    def _():
        kvext[5 * TOK : 6 * TOK] = jnp.zeros((TOK, 128), BF16)

    phase("x_wait")
    drain(ctx.at[pl.ds(0, NY - 1), 0], xr)
    for k in (1, 2, 3):
        x_pass(k).start()

    phase("wy")
    drain(wkv, lsem.at[6])

    def head_columns(i, c):
        rows = pl.ds(pl.multiple_of(i * 256, 256), 256)
        at = 128 * lax.div(y, 2)
        kt = wkv[rows, pl.ds(pl.multiple_of(at, 128), 128)].astype(F32)
        vt = wkv[rows, pl.ds(pl.multiple_of(TOK + at, 128), 128)].astype(F32)
        odd = lax.rem(y, 2) == 1
        wy[rows, :] = jnp.where(
            low, jnp.where(odd, half_swap(kt), kt), jnp.where(odd, vt, half_swap(vt))
        ).astype(BF16)
        return c

    lax.fori_loop(0, D // 256, head_columns, 0)
    phase("x_wait2")
    drain(ctx.at[pl.ds(0, NY - 1), 0], xpr)
    for b in range(NY):
        rows = slice(CTXL * b, CTXL * b + CTXL)
        rsc[rows, :] = stats(ctx[b].reshape(CTXL, D).astype(F32))

    phase("m_wait")
    drain(mrecv.at[pl.ds(0, NY * NTP - 1)], mr)
    phase("mod")
    for t in range(NTP):
        total = mrecv[t] + mrecv[NTP + t] + mrecv[2 * NTP + t] + mrecv[3 * NTP + t]
        lo, hi = 256 * t, 256 * t + 128
        mod[0:4, lo : lo + 128] = total[0:4]
        mod[0:4, hi : hi + 128] = total[4:8]
    mod[2:3, :] = mod[5:6, :] * (1.0 + mod[2:3, :])
    mod[3:4, :] = mod[5:6, :] * (1.0 + mod[3:4, :])

    for i in range(4):
        spread[i] = jnp.broadcast_to(mod[i : i + 1, :], (8, D))

    def hidden(v, r, which):
        n = v.shape[0] // 8
        r = r.reshape(n, 8, 128)
        parts = []
        for t in range(D // 128):
            cols = slice(128 * t, 128 * t + 128)
            u = v[:, cols].astype(F32).reshape(n, 8, 128) * r
            u = u * spread[2 + which, :, cols] + spread[which, :, cols]
            parts.append(u.reshape(8 * n, 128).astype(BF16))
        return jnp.concatenate(parts, axis=1)

    phase("ctx_hidden")
    for b in range(NY):
        rows = slice(CTXL * b, CTXL * b + CTXL)
        hidc[rows, :] = hidden(ctx[b].reshape(CTXL, D), rsc[rows, :], 1)
    phase("ctx_kv")
    here = pl.ds(pl.multiple_of(z * NY * CTXL, NY * CTXL), NY * CTXL)
    ctxkv[here, :] = dot(hidc[...], wy[...]).astype(BF16)

    def c_copy(k):
        dz = lax.rem(z + k, NZ)
        return remote(ctxkv.at[here, :], ctxkv.at[here, :], cs, cr, dz * NY + y, tp)

    for k in Z_ORDER:
        c_copy(k).start()

    phase("hidden_kv")

    def k_copy(k, i):
        dy = lax.rem(y + k, NY)
        at = pl.ds(pl.multiple_of((1 + y) * TOK + 128 * i, 128), 128)
        src = kvsend.at[dy, pl.ds(128 * i, 128), :]
        return remote(src, kvext.at[at, :], ks, kr.at[y], z * NY + dy, tp)

    for i in range(2):
        rows = slice(128 * i, 128 * i + 128)
        for n in range(4):
            r32 = slice(128 * i + 32 * n, 128 * i + 32 * n + 32)
            hid[r32, :] = hidden(lat[r32, :], rsl[r32, :], 0)
        kv = dot(hid[rows, :], wkv[...])
        for q in range(2):
            kt = kv[:, 128 * q : 128 * q + 128]
            vt = kv[:, 256 + 128 * q : 256 + 128 * q + 128]
            kvsend[2 * q, rows] = jnp.where(low, kt, half_swap(vt)).astype(BF16)
            kvsend[2 * q + 1, rows] = jnp.where(low, half_swap(kt), vt).astype(BF16)
        for k in (2, 1, 3):
            k_copy(k, i).start()
        kvext[pl.ds(pl.multiple_of((1 + y) * TOK + 128 * i, 128), 128), :] = kvsend[y, rows]

    def k_in(dy):
        rows = pl.ds(pl.multiple_of((1 + dy) * TOK, TOK), TOK)
        return remote(kvsend.at[y], kvext.at[rows, :], ks, kr.at[dy], z * NY + dy, tp)


    phase("qg")
    drain(wqg, lsem.at[7])
    qg = dot(hid[0:TOK, :], wqg[:, 0:TOK])
    for q in range(2):
        qt = qg[:, 128 * q : 128 * q + 128] * (HD**-0.5)
        up, dn = qt[0:128], qt[128:256]
        qsend[2 * q] = jnp.where(low, up, half_swap(dn)).astype(BF16)
        qsend[2 * q + 1] = jnp.where(low, half_swap(up), dn).astype(BF16)
    qrecv[y] = qsend[y]

    def q_copy(k):
        dy = lax.rem(y + k, NY)
        return remote(qsend.at[dy], qrecv.at[y], qs, qr, z * NY + dy, tp)

    for k in (2, 1, 3):
        q_copy(k).start()
    phase("g")
    g = dot(hid[0:TOK, :], wqg[:, TOK:])
    gbuf[...] = g.astype(BF16).reshape(NX, NC, OUTR, TOK)
    g_copy = remote(gbuf.at[:, 1 - core], gother, gs, gr, sp, partner)
    g_copy.start()
    drain(wo, lsem.at[5])
    w_copy = remote(wo, wo2, ws, wr, sp, partner)
    w_copy.start()

    phase("kq_wait")
    drain(zgrecv.at[pl.ds(0, NZ - 1)], zgr)
    total = zgrecv[0]
    for k in range(1, NZ):
        total = total + zgrecv[k]
    mgsend[...] = total
    mgrecv[group] = total

    for k in G_ORDER:
        remote(mgsend, mgrecv.at[group], mgs, mgr, *group_peer(k)).start()

    up_src = kvext.at[pl.ds(4 * TOK, TOK), :]
    dn_src = kvext.at[pl.ds(TOK, TOK), :]
    up_dst = kvext.at[pl.ds(0, TOK), :]
    dn_dst = kvext.at[pl.ds(5 * TOK, TOK), :]
    up_copy = remote(up_src, up_dst, hs.at[0], hr.at[0], jnp.minimum(z + 1, NZ - 1) * NY + y, tp)
    dn_copy = remote(dn_src, dn_dst, hs.at[1], hr.at[1], jnp.maximum(z - 1, 0) * NY + y, tp)

    @pl.when((y == NY - 1) & (z < NZ - 1))
    def _():
        up_copy.start()

    @pl.when((y == 0) & (z > 0))
    def _():
        dn_copy.start()

    @pl.when(y == 1)
    def _():
        k_in(0).wait_recv()

    @pl.when((y == 1) & (z > 0))
    def _():
        dn_copy.start()

    @pl.when(y != NY - 1)
    def _():
        k_in(3).wait_recv()

    @pl.when((y != NY - 1) & (z < NZ - 1))
    def _():
        up_copy.start()

    @pl.when(y > 1)
    def _():
        k_in(0).wait_recv()

    @pl.when((y > 1) & (z > 0))
    def _():
        dn_copy.start()

    @pl.when(y != 1)
    def _():
        k_in(1).wait_recv()

    @pl.when(y != 2)
    def _():
        k_in(2).wait_recv()

    phase("gates")
    g_copy.wait_recv()
    for part in range(2):
        g = (gbuf[:, core] if part == 0 else gother[...]).astype(F32)
        sgate[:, :, TOK * part : TOK * part + TOK] = g * (1.0 / (1.0 + jnp.exp(-g)))
    phase("q_wait")
    drain(qrecv.at[pl.ds(0, NY - 1)], qr)
    phase("c_wait")
    drain(ctxkv.at[pl.ds(0, CTX - NY * CTXL)], cr)
    phase("attention")
    across = lax.rem(x + 2, NX)
    plus, minus = lax.rem(x + 1, NX), lax.rem(x + NX - 1, NX)
    source = core * NY + y
    fold = OUTR // 2

    def r_copy(i, b, h):
        return remote(
            rsend.at[i, b, h], rrecv.at[i, source], rs, rr.at[i], z * NY + b, x * NC + h
        )

    def attend(i, *blocks):
        queries, windows = [], []
        for b in blocks:
            xq = qrecv[b, pl.ds(pl.multiple_of(64 * lax.rem(i, 2), 64), 64), :].astype(F32)
            queries.append(jnp.where(low, jnp.where(i > 1, half_swap(xq), xq), 0.0).astype(BF16))
            row = 4 * b + i
            base = jnp.clip(row0 + row - 4, 0, LAST_START) - row0 + 4
            keys = pl.ds(pl.multiple_of(base * GRID_W, GRID_W), WIN)
            windows.append((keys, jnp.where(row < 4, row, jnp.where(row < 13, 4, row - 8))))
        sc_ctx = dot_nt(jnp.concatenate(queries, axis=0), ctxkv[...])
        sc_win = jnp.concatenate(
            [dot_nt(qp, kvext[keys, :]) + btab[t] for qp, (keys, t) in zip(queries, windows)],
            axis=0,
        )
        top = jnp.maximum(
            jnp.max(sc_ctx, axis=1, keepdims=True), jnp.max(sc_win, axis=1, keepdims=True)
        )
        e_ctx = jnp.exp(sc_ctx - top)
        e_win = jnp.exp(sc_win - top)
        den = jnp.sum(e_ctx, axis=1, keepdims=True) + jnp.sum(e_win, axis=1, keepdims=True)
        e_win = e_win.astype(BF16)
        o_all = dot(e_ctx.astype(BF16), ctxkv[...])
        for n, (b, (keys, t)) in enumerate(zip(blocks, windows)):
            part = slice(64 * n, 64 * n + 64)
            o = (o_all[part] + dot(e_win[part], kvext[keys, :])) * (1.0 / den[part])
            for h in range(NC):
                r0 = o[OUTR * h : OUTR * h + fold]
                r1 = o[OUTR * h + fold : OUTR * h + OUTR]
                rsend[i, b, h] = jnp.where(low, half_swap(r0), r1).astype(BF16)
        for b in blocks:
            for h in range(NC):
                here = (b == y) & (h == core)

                @pl.when(here)
                def _():
                    rrecv[i, source] = rsend[i, b, h]

                @pl.when(jnp.logical_not(here))
                def _():
                    r_copy(i, b, h).start()

    def gate(i, name, at):
        phase("r_wait_" + name)
        drain(rrecv.at[i, pl.ds(0, NC * NY - 1)], rr.at[i])
        phase("project_" + name)
        for part in range(2):
            src = (core if part == 0 else 1 - core) * NY
            for q in range(2):
                x0, x1 = rrecv[i, src + 2 * q].astype(F32), rrecv[i, src + 2 * q + 1].astype(F32)
                cols = slice(TOK * part + 128 * q, TOK * part + 128 * q + 128)
                up = jnp.where(low, x0, half_swap(x1)) * sgate[i, 0:fold, cols]
                dn = jnp.where(low, half_swap(x0), x1) * sgate[i, fold:OUTR, cols]
                gated[at : at + fold, cols] = up.astype(BF16)
                gated[at + fold : at + OUTR, cols] = dn.astype(BF16)

    def project(targets, at, *pieces):
        rows = slice(at, at + OUTR * len(targets))
        for n in pieces:
            cols = slice(512 * n, 512 * n + 512)
            term = dot(gated[rows, :TOK], wo[:, cols]) + dot(gated[rows, TOK:], wo2[:, cols])
            for m, i in enumerate(targets):
                psend[i, :, cols] = term[OUTR * m : OUTR * m + OUTR].astype(BF16)

    def to_neighbour(src, up, dst, sem):
        remote(src, dst, ps, sem, sp, (plus if up else minus) * NC + core).start()

    def send_across(*pieces):
        for n in pieces:
            src = psend.at[across, :, pl.ds(512 * n, 512)]
            to_neighbour(src, n < 2, hop.at[n], hp.at[n])

    def send_on(up, at, width):
        cols = pl.ds(at, width)
        src = psend.at[plus if up else minus, :, cols]
        to_neighbour(src, up, precv.at[0 if up else 1, :, cols], pr)

    attend(across, 1, 2)
    phase("h_wait")

    @pl.when(z > 0)
    def _():
        up_copy.wait_recv()

    @pl.when(z < NZ - 1)
    def _():
        dn_copy.wait_recv()

    phase("attention2")
    attend(across, 0, 3)
    phase("attention3")
    attend(plus, 0, 3, 1, 2)
    phase("attention4")
    attend(minus, 0, 3, 1, 2)
    phase("attention5")
    attend(x, 0, 3, 1, 2)
    w_copy.wait_recv()
    gate(across, "across", 0)
    project((across,), 0, 0, 2)
    send_across(0, 2)
    project((across,), 0, 1, 3)
    send_across(1, 3)
    gate(plus, "plus", OUTR)
    project((plus,), OUTR, 2, 3)
    send_on(True, D // 2, D // 2)
    gate(minus, "minus", 2 * OUTR)
    project((plus, minus), OUTR, 0, 1)
    send_on(False, 0, D // 2)

    def add_and_send(m, n):
        phase(f"hop{m}")
        cols = pl.ds(pl.multiple_of(512 * n, 512), 512)
        drain(hop.at[n], hp.at[n])
        up = n < 2
        to = jnp.where(up, plus, minus)
        psend[to, :, cols] = (psend[to, :, cols].astype(F32) + hop[n].astype(F32)).astype(BF16)
        dst = precv.at[jnp.where(up, 0, 1), :, cols]
        remote(psend.at[to, :, cols], dst, ps, pr, sp, to * NC + core).start()

    phase("rest")
    project((minus,), 2 * OUTR, 2, 3)
    for m, (inner, first, last) in enumerate(((0, 2, 0), (2, 3, 1), (1, 0, 2), (3, 1, 3))):
        add_and_send(m, jnp.where(x == 0, first, jnp.where(x == NX - 1, last, inner)))
    gate(x, "own", 0)
    project((x,), 0, 0, 1, 2, 3)

    phase("sent1")
    drain(zrecv.at[pl.ds(0, NZ - 1)], zs)
    drain(zgrecv.at[pl.ds(0, NZ - 1)], zgs)
    drain(mrecv.at[pl.ds(0, NY * NTP - 1)], ms)
    drain(mgrecv.at[pl.ds(0, NY * NTP - 1)], mgs)
    drain(mgrecv.at[pl.ds(0, NY * NTP - 1)], mgr)
    drain(ctxkv.at[pl.ds(0, CTX - NY * CTXL)], cs)
    drain(ctx.at[pl.ds(0, NY - 1), 0], xs)
    drain(ctx.at[pl.ds(0, NY - 1), 0], xps)
    drain(kvext.at[pl.ds(0, (NY - 1) * TOK)], ks)
    drain(qrecv.at[pl.ds(0, NY - 1)], qs)
    w_copy.wait_send()
    g_copy.wait_send()
    for i in range(NX):
        drain(rrecv.at[i, pl.ds(0, NC * NY - 1)], rs)

    @pl.when(z < NZ - 1)
    def _():
        up_copy.wait_send()

    @pl.when(z > 0)
    def _():
        dn_copy.wait_send()

    for t in range(NTP):
        total = mgrecv[t] + mgrecv[NTP + t] + mgrecv[2 * NTP + t] + mgrecv[3 * NTP + t]
        mod[4:5, 256 * t : 256 * t + 128] = total[0:1]
        mod[4:5, 256 * t + 128 : 256 * t + 256] = total[1:2]
    phase("p_wait")
    drain(precv, pr)
    phase("final")
    branch = psend[x].astype(F32) + precv[0].astype(F32) + precv[1].astype(F32)
    branch = branch.astype(BF16).astype(F32)
    normed = branch * lax.rsqrt(jnp.mean(branch * branch, axis=1, keepdims=True) + EPSILON)
    own = lat[pl.ds(pl.multiple_of(tp * OUTR, OUTR), OUTR), :].astype(F32)
    out_ref[...] = (own + mod[4:5, :] * (normed * mod[6:7, :])).astype(BF16)

    phase("sent")
    drain(psend.at[pl.ds(0, NX - 1)], ps)
    phase(None)


def shards(
    latent,
    context,
    condition,
    context_condition,
    gain_pre,
    gain_post,
    w_shift,
    w_scale,
    w_gate,
    w_query,
    w_key,
    w_value,
    w_silu,
    offset_bias,
    w_out,
):
    in_rows = w_shift.shape[0]
    vmem = pl.BlockSpec(memory_space=pltpu.VMEM)
    hbm = pl.BlockSpec(memory_space=pltpu.HBM)
    dma = pltpu.SemaphoreType.DMA
    operands = (
        condition.reshape(16, 128),
        context_condition.reshape(16, 128),
        gain_pre.reshape(16, 128),
        gain_post.reshape(16, 128),
        jnp.transpose(offset_bias, (1, 0, 2)),
        latent,
        context,
        w_shift,
        w_scale,
        w_gate,
        w_query,
        w_key,
        w_value,
        w_silu,
        w_out,
    )
    operands = [pltpu.with_memory_space_constraint(a, pltpu.HBM) for a in operands]
    return pl.pallas_call(
        kernel,
        name="whole",
        out_shape=jax.ShapeDtypeStruct((OUTR, D), BF16),
        in_specs=[hbm] * 15,
        out_specs=vmem,
        scratch_shapes=[
            pltpu.VMEM((2, 16, 128), BF16),
            pltpu.VMEM((2, 16, 128), F32),
            pltpu.VMEM((2, 16, 128), F32),
            pltpu.VMEM((2 * WIN_ROWS - 1, NY, 2 * WIN_COLS - 1), F32),
            pltpu.VMEM((16, 128), F32),
            pltpu.VMEM((3, in_rows, TOK), BF16),
            pltpu.VMEM((TOK, D), BF16),
            pltpu.VMEM((NY, NC, CTXL // NC, D), BF16),
            pltpu.VMEM((D, 2 * TOK), BF16),
            pltpu.VMEM((D, 128), BF16),
            pltpu.VMEM((D, 2 * TOK), BF16),
            pltpu.VMEM((TOK, D), BF16),
            pltpu.VMEM((TOK, D), BF16),
            pltpu.VMEM((8, 128), F32),
            pltpu.VMEM((NZ, 8, 128), F32),
            pltpu.VMEM((8, 128), F32),
            pltpu.VMEM((NY * NTP, 8, 128), F32),
            pltpu.VMEM((2, 128), F32),
            pltpu.VMEM((NZ, 2, 128), F32),
            pltpu.VMEM((2, 128), F32),
            pltpu.VMEM((NY * NTP, 2, 128), F32),
            pltpu.VMEM((8, D), F32),
            pltpu.VMEM((4, 8, D), F32),
            pltpu.VMEM((TABLES, GRID_W, WIN), F32),
            pltpu.VMEM((TOK, D), BF16),
            pltpu.VMEM((NY * CTXL, D), BF16),
            pltpu.VMEM((TOK, 128), F32),
            pltpu.VMEM((NY * CTXL, 128), F32),
            pltpu.VMEM((CTX, 128), BF16),
            pltpu.VMEM((NY, TOK, 128), BF16),
            pltpu.VMEM((6 * TOK, 128), BF16),
            pltpu.VMEM((NY, 128, 128), BF16),
            pltpu.VMEM((NY, 128, 128), BF16),
            pltpu.VMEM((NX, NC, OUTR, TOK), BF16),
            pltpu.VMEM((NX, OUTR, TOK), BF16),
            pltpu.VMEM((NX, OUTR, NC * TOK), F32),
            pltpu.VMEM((NX, NY, NC, OUTR // 2, 128), BF16),
            pltpu.VMEM((NX, NC * NY, OUTR // 2, 128), BF16),
            pltpu.VMEM((3 * OUTR, NC * TOK), BF16),
            pltpu.VMEM((NX, OUTR, D), BF16),
            pltpu.VMEM((4, OUTR, D // 4), BF16),
            pltpu.VMEM((2, OUTR, D), BF16),
            dma((9,)),
            dma,
            dma,
            dma,
            dma,
            dma,
            dma,
            dma,
            dma,
            dma,
            dma,
            dma,
            dma,
            dma,
            dma,
            dma,
            dma,
            dma,
            dma((NY,)),
            dma,
            dma,
            dma((2,)),
            dma((2,)),
            dma,
            dma((NX,)),
            dma,
            dma,
            dma((4,)),
            dma,
            dma,
        ],
        compiler_params=pltpu.CompilerParams(
            collective_id=0, has_side_effects=True, vmem_limit_bytes=48 << 20
        ),
    )(*operands)


def solution(mesh):
    in_specs = (
        P("sp", None),
        P("sp", None),
        P(),
        P(),
        P(),
        P(),
        P("sp", "tp"),
        P("sp", "tp"),
        P("sp", "tp"),
        P(None, "tp"),
        P(None, "tp"),
        P(None, "tp"),
        P(None, "tp"),
        P("tp", None, None),
        P("tp", None),
    )
    out_specs = P(("sp", "tp"), None)
    return jax.shard_map(shards, mesh=mesh, in_specs=in_specs, out_specs=out_specs, check_vma=False)
```

```python
import functools

import jax
import jax.numpy as jnp
from jax import lax
from jax.experimental import pallas as pl
from jax.experimental.pallas import tpu as pltpu
from jax.sharding import PartitionSpec as P

GRID_W = 64
WIN_ROWS = 8
WIN_COLS = 16
EPSILON = 1e-06
NZ, NY, NX, NC = 8, 4, 4, 2
NTP = NX * NC
D = 2048
HD = 64
TOK = 256
CTXL = 32
CTX = 1024
OUTR = TOK // NTP
LAST_START = NZ * NY * TOK // GRID_W - WIN_ROWS
TABLES = 8
WIN = WIN_ROWS * GRID_W
Z_ORDER = (4, 3, 5, 2, 6, 1, 7)
G_ORDER = sorted(
    ((ky, kx, kc) for ky in range(NY) for kx in range(NX) for kc in range(NC)),
    key=lambda k: -min(k[0], NY - k[0]) - min(k[1], NX - k[1]) - k[2] / 2,
)[:-1]
F32 = jnp.float32
BF16 = jnp.bfloat16
NT = (((1,), (1,)), ((), ()))


def dot(a, b):
    return jnp.dot(a, b, preferred_element_type=F32)


def dot_nt(a, b):
    return lax.dot_general(a, b, NT, preferred_element_type=F32)


def remote(src, dst, ssem, rsem, sp, tp):
    return pltpu.make_async_remote_copy(
        src_ref=src,
        dst_ref=dst,
        send_sem=ssem,
        recv_sem=rsem,
        device_id=(sp, tp),
        device_id_type=pl.DeviceIdType.MESH,
    )


class Phases:
    def __init__(self):
        self.scope = None

    def __call__(self, name):
        if self.scope is not None:
            self.scope.__exit__(None, None, None)
        self.scope = None
        if name:
            self.scope = jax.named_scope(name)
            self.scope.__enter__()


def drain(ref, sem):
    pltpu.make_async_copy(ref, ref, sem).wait()


def half_swap(v):
    return pltpu.roll(v, 64, 1)


def kernel(
    cond_h,
    cond2_h,
    gpre_h,
    gpost_h,
    bias_h,
    lat_h,
    ctx_h,
    wsh_h,
    wsc_h,
    wga_h,
    wq_h,
    wk_h,
    wv_h,
    wg_h,
    wo_h,
    out_ref,
    conds,
    condf,
    gains,
    bias,
    biasx,
    wmod,
    lat,
    ctx,
    wkv,
    wy,
    wqg,
    wo,
    wo2,
    zsend,
    zrecv,
    msend,
    mrecv,
    zgsend,
    zgrecv,
    mgsend,
    mgrecv,
    mod,
    spread,
    btab,
    hid,
    hidc,
    rsl,
    rsc,
    ctxkv,
    kvsend,
    kvext,
    qsend,
    qrecv,
    gbuf,
    gother,
    sgate,
    rsend,
    rrecv,
    gated,
    psend,
    hop,
    precv,
    lsem,
    zs,
    zr,
    ms,
    mr,
    zgs,
    zgr,
    mgs,
    mgr,
    xs,
    xr,
    xps,
    xpr,
    ws,
    wr,
    cs,
    cr,
    ks,
    kr,
    qs,
    qr,
    hs,
    hr,
    rs,
    rr,
    gs,
    gr,
    hp,
    ps,
    pr,
):
    sp = lax.axis_index("sp")
    tp = lax.axis_index("tp")
    z, y = lax.div(sp, NY), lax.rem(sp, NY)
    x, core = lax.div(tp, NC), lax.rem(tp, NC)
    partner = x * NC + (1 - core)
    group = y * NTP + tp
    lane = lax.broadcasted_iota(jnp.int32, (1, 128), 1)
    low = lane < 64

    phase = Phases()
    phase("loads")
    def load(sem, *moves):
        for a, b in moves:
            pltpu.make_async_copy(a, b, lsem.at[sem]).start()

    load(0, (cond_h, conds.at[0]), (cond2_h, conds.at[1]))
    load(1, (wsh_h, wmod.at[0]), (wsc_h, wmod.at[1]), (wga_h, wmod.at[2]))
    half = CTXL // NC
    load(8, *((ctx_h.at[pl.ds(half * h, half), :], ctx.at[y, h]) for h in range(NC)))
    load(2, (lat_h, lat))
    load(3, (gpre_h, gains.at[0]), (gpost_h, gains.at[1]))
    load(4, (bias_h, bias))
    load(5, (wo_h, wo))
    load(6, (wk_h, wkv.at[:, pl.ds(0, TOK)]), (wv_h, wkv.at[:, pl.ds(TOK, TOK)]))
    load(7, (wq_h, wqg.at[:, pl.ds(0, TOK)]), (wg_h, wqg.at[:, pl.ds(TOK, TOK)]))

    phase("greet")
    barrier = pltpu.get_barrier_semaphore()

    def greet(dsp, dtp):
        pl.semaphore_signal(
            barrier, inc=1, device_id=(dsp, dtp), device_id_type=pl.DeviceIdType.MESH
        )

    for k in Z_ORDER:
        greet(lax.rem(z + k, NZ) * NY + y, tp)

    def group_peer(k):
        dx, dc = lax.rem(x + k[1], NX), 1 - core if k[2] else core
        return z * NY + lax.rem(y + k[0], NY), dx * NC + dc

    for k in G_ORDER:
        greet(*group_peer(k))

    phase("partial")
    drain(conds, lsem.at[0])
    v = conds[...].astype(F32)
    condf[...] = v * (1.0 / (1.0 + jnp.exp(-v)))
    line = jnp.concatenate([condf[i, pl.ds(lax.div(sp, 2), 1), :] for i in range(2)], axis=0)
    line = jnp.where(lax.rem(sp, 2) == 1, half_swap(line), line)[:, :64]
    act = jnp.concatenate([line, jnp.zeros((6, 64), F32)], axis=0).astype(BF16)
    drain(wmod, lsem.at[1])
    sh = dot(act, wmod[0])
    sc = dot(act, wmod[1])
    ga = dot(act, wmod[2])
    zsend[0:2] = sh[0:2, :128]
    zsend[2:4] = sc[0:2, :128]
    zsend[4:6] = sh[0:2, 128:]
    zsend[6:8] = sc[0:2, 128:]
    zgsend[0:1] = ga[0:1, :128]
    zgsend[1:2] = ga[0:1, 128:]
    zrecv[z] = zsend[...]
    zgrecv[z] = zgsend[...]

    phase("barrier")
    pl.semaphore_wait(barrier, NZ - 1 + NY * NTP - 1)

    phase("z_start")
    def z_copy(k):
        dz = lax.rem(z + k, NZ)
        return remote(zsend, zrecv.at[z], zs, zr, dz * NY + y, tp)

    def zg_copy(k):
        dz = lax.rem(z + k, NZ)
        return remote(zgsend, zgrecv.at[z], zgs, zgr, dz * NY + y, tp)

    for k in Z_ORDER:
        z_copy(k).start()
    for k in Z_ORDER:
        zg_copy(k).start()

    def x_copy(k):
        dy = lax.rem(y + k, NY)
        return remote(ctx.at[y, core], ctx.at[y, core], xs, xr, z * NY + dy, tp)

    def x_pass(k):
        rows = ctx.at[lax.rem(y + k, NY), core]
        return remote(rows, rows, xps, xpr, sp, partner)

    drain(ctx.at[0], lsem.at[8])
    for k in (2, 1, 3):
        x_copy(k).start()

    phase("stats")
    drain(lat, lsem.at[2])

    def stats(v):
        r = lax.rsqrt(jnp.mean(v * v, axis=1, keepdims=True) + EPSILON)
        return jnp.broadcast_to(r, (v.shape[0], 128))

    def row_stats(i, c):
        rows = pl.ds(pl.multiple_of(i * 32, 32), 32)
        rsl[rows, :] = stats(lat[rows, :].astype(F32))
        return c

    lax.fori_loop(0, TOK // 32, row_stats, 0)
    drain(gains, lsem.at[3])
    for t in range(16):
        mod[5:6, 128 * t : 128 * t + 128] = gains[0, t : t + 1, :]
        mod[6:7, 128 * t : 128 * t + 128] = gains[1, t : t + 1, :]
    drain(bias, lsem.at[4])
    biasx[...] = jnp.zeros((16, 128), F32)
    for d in range(2 * WIN_ROWS - 1):
        line = bias[d, pl.ds(y, 1), :]
        biasx[d : d + 1, 0:31] = line
        if d > 0:
            biasx[d - 1 : d, 64:95] = line

    phase("z_wait")
    drain(zrecv.at[pl.ds(0, NZ - 1)], zr)
    phase("m_start")
    total = zrecv[0]
    for k in range(1, NZ):
        total = total + zrecv[k]
    msend[...] = total
    mrecv[group] = total

    for k in G_ORDER:
        remote(msend, mrecv.at[group], ms, mr, *group_peer(k)).start()

    phase("tables")
    col = lax.rem(lax.broadcasted_iota(jnp.int32, (64, 128), 1), 64)
    qcol = lax.broadcasted_iota(jnp.int32, (64, 128), 0)
    first_col = jnp.clip(qcol - WIN_COLS // 2, 0, GRID_W - WIN_COLS)
    in_cols = (col >= first_col) & (col < first_col + WIN_COLS)
    row0 = z * 16

    def table(t, c):
        row = row0 + jnp.where(t < 5, t, t + 8)
        d0 = jnp.clip(row - 4, 0, LAST_START) - row + 7
        for m in range(WIN_ROWS // 2):
            line = biasx[pl.ds(d0 + 2 * m, 1), :]
            tile = pltpu.roll(
                jnp.broadcast_to(line, (64, 128)), 113, 1, stride=1, stride_axis=0
            )
            btab[t, :, m * 128 : m * 128 + 128] = jnp.where(in_cols, tile, -jnp.inf)
        return c

    lax.fori_loop(0, TABLES, table, 0)

    @pl.when(z == 0)
    def _():
        kvext[0:TOK] = jnp.zeros((TOK, 128), BF16)

    @pl.when(z == NZ - 1)
    def _():
        kvext[5 * TOK : 6 * TOK] = jnp.zeros((TOK, 128), BF16)

    phase("x_wait")
    drain(ctx.at[pl.ds(0, NY - 1), 0], xr)
    for k in (1, 2, 3):
        x_pass(k).start()

    phase("wy")
    drain(wkv, lsem.at[6])

    def head_columns(i, c):
        rows = pl.ds(pl.multiple_of(i * 256, 256), 256)
        at = 128 * lax.div(y, 2)
        kt = wkv[rows, pl.ds(pl.multiple_of(at, 128), 128)].astype(F32)
        vt = wkv[rows, pl.ds(pl.multiple_of(TOK + at, 128), 128)].astype(F32)
        odd = lax.rem(y, 2) == 1
        wy[rows, :] = jnp.where(
            low, jnp.where(odd, half_swap(kt), kt), jnp.where(odd, vt, half_swap(vt))
        ).astype(BF16)
        return c

    lax.fori_loop(0, D // 256, head_columns, 0)
    phase("x_wait2")
    drain(ctx.at[pl.ds(0, NY - 1), 0], xpr)
    for b in range(NY):
        rows = slice(CTXL * b, CTXL * b + CTXL)
        rsc[rows, :] = stats(ctx[b].reshape(CTXL, D).astype(F32))

    phase("m_wait")
    drain(mrecv.at[pl.ds(0, NY * NTP - 1)], mr)
    phase("mod")
    for t in range(NTP):
        total = mrecv[t] + mrecv[NTP + t] + mrecv[2 * NTP + t] + mrecv[3 * NTP + t]
        lo, hi = 256 * t, 256 * t + 128
        mod[0:4, lo : lo + 128] = total[0:4]
        mod[0:4, hi : hi + 128] = total[4:8]
    mod[2:3, :] = mod[5:6, :] * (1.0 + mod[2:3, :])
    mod[3:4, :] = mod[5:6, :] * (1.0 + mod[3:4, :])

    for i in range(4):
        spread[i] = jnp.broadcast_to(mod[i : i + 1, :], (8, D))

    def hidden(v, r, which):
        n = v.shape[0] // 8
        r = r.reshape(n, 8, 128)
        parts = []
        for t in range(D // 128):
            cols = slice(128 * t, 128 * t + 128)
            u = v[:, cols].astype(F32).reshape(n, 8, 128) * r
            u = u * spread[2 + which, :, cols] + spread[which, :, cols]
            parts.append(u.reshape(8 * n, 128).astype(BF16))
        return jnp.concatenate(parts, axis=1)

    phase("ctx_hidden")
    for b in range(NY):
        rows = slice(CTXL * b, CTXL * b + CTXL)
        hidc[rows, :] = hidden(ctx[b].reshape(CTXL, D), rsc[rows, :], 1)
    phase("ctx_kv")
    here = pl.ds(pl.multiple_of(z * NY * CTXL, NY * CTXL), NY * CTXL)
    ctxkv[here, :] = dot(hidc[...], wy[...]).astype(BF16)

    def c_copy(k):
        dz = lax.rem(z + k, NZ)
        return remote(ctxkv.at[here, :], ctxkv.at[here, :], cs, cr, dz * NY + y, tp)

    for k in Z_ORDER:
        c_copy(k).start()

    phase("hidden_kv")

    def k_copy(k, i):
        dy = lax.rem(y + k, NY)
        at = pl.ds(pl.multiple_of((1 + y) * TOK + 128 * i, 128), 128)
        src = kvsend.at[dy, pl.ds(128 * i, 128), :]
        return remote(src, kvext.at[at, :], ks, kr.at[y], z * NY + dy, tp)

    for i in range(2):
        rows = slice(128 * i, 128 * i + 128)
        for n in range(4):
            r32 = slice(128 * i + 32 * n, 128 * i + 32 * n + 32)
            hid[r32, :] = hidden(lat[r32, :], rsl[r32, :], 0)
        kv = dot(hid[rows, :], wkv[...])
        for q in range(2):
            kt = kv[:, 128 * q : 128 * q + 128]
            vt = kv[:, 256 + 128 * q : 256 + 128 * q + 128]
            kvsend[2 * q, rows] = jnp.where(low, kt, half_swap(vt)).astype(BF16)
            kvsend[2 * q + 1, rows] = jnp.where(low, half_swap(kt), vt).astype(BF16)
        for k in (2, 1, 3):
            k_copy(k, i).start()
        kvext[pl.ds(pl.multiple_of((1 + y) * TOK + 128 * i, 128), 128), :] = kvsend[y, rows]

    def k_in(dy):
        rows = pl.ds(pl.multiple_of((1 + dy) * TOK, TOK), TOK)
        return remote(kvsend.at[y], kvext.at[rows, :], ks, kr.at[dy], z * NY + dy, tp)


    phase("qg")
    drain(wqg, lsem.at[7])
    qg = dot(hid[0:TOK, :], wqg[:, 0:TOK])
    for q in range(2):
        qt = qg[:, 128 * q : 128 * q + 128] * (HD**-0.5)
        up, dn = qt[0:128], qt[128:256]
        qsend[2 * q] = jnp.where(low, up, half_swap(dn)).astype(BF16)
        qsend[2 * q + 1] = jnp.where(low, half_swap(up), dn).astype(BF16)
    qrecv[y] = qsend[y]

    def q_copy(k):
        dy = lax.rem(y + k, NY)
        return remote(qsend.at[dy], qrecv.at[y], qs, qr, z * NY + dy, tp)

    for k in (2, 1, 3):
        q_copy(k).start()
    phase("g")
    g = dot(hid[0:TOK, :], wqg[:, TOK:])
    gbuf[...] = g.astype(BF16).reshape(NX, NC, OUTR, TOK)
    g_copy = remote(gbuf.at[:, 1 - core], gother, gs, gr, sp, partner)
    g_copy.start()
    drain(wo, lsem.at[5])
    w_copy = remote(wo, wo2, ws, wr, sp, partner)

    phase("kq_wait")
    drain(zgrecv.at[pl.ds(0, NZ - 1)], zgr)
    total = zgrecv[0]
    for k in range(1, NZ):
        total = total + zgrecv[k]
    mgsend[...] = total
    mgrecv[group] = total

    for k in G_ORDER:
        remote(mgsend, mgrecv.at[group], mgs, mgr, *group_peer(k)).start()

    up_src = kvext.at[pl.ds(4 * TOK, TOK), :]
    dn_src = kvext.at[pl.ds(TOK, TOK), :]
    up_dst = kvext.at[pl.ds(0, TOK), :]
    dn_dst = kvext.at[pl.ds(5 * TOK, TOK), :]
    up_copy = remote(up_src, up_dst, hs.at[0], hr.at[0], jnp.minimum(z + 1, NZ - 1) * NY + y, tp)
    dn_copy = remote(dn_src, dn_dst, hs.at[1], hr.at[1], jnp.maximum(z - 1, 0) * NY + y, tp)

    @pl.when((y == NY - 1) & (z < NZ - 1))
    def _():
        up_copy.start()

    @pl.when((y == 0) & (z > 0))
    def _():
        dn_copy.start()

    @pl.when(y == 1)
    def _():
        k_in(0).wait_recv()

    @pl.when((y == 1) & (z > 0))
    def _():
        dn_copy.start()

    @pl.when(y != NY - 1)
    def _():
        k_in(3).wait_recv()

    @pl.when((y != NY - 1) & (z < NZ - 1))
    def _():
        up_copy.start()

    @pl.when(y > 1)
    def _():
        k_in(0).wait_recv()

    @pl.when((y > 1) & (z > 0))
    def _():
        dn_copy.start()

    @pl.when(y != 1)
    def _():
        k_in(1).wait_recv()

    @pl.when(y != 2)
    def _():
        k_in(2).wait_recv()

    phase("gates")
    g_copy.wait_recv()
    for part in range(2):
        g = (gbuf[:, core] if part == 0 else gother[...]).astype(F32)
        sgate[:, :, TOK * part : TOK * part + TOK] = g * (1.0 / (1.0 + jnp.exp(-g)))
    w_copy.start()
    phase("q_wait")
    drain(qrecv.at[pl.ds(0, NY - 1)], qr)
    phase("c_wait")
    drain(ctxkv.at[pl.ds(0, CTX - NY * CTXL)], cr)
    phase("attention")
    across = lax.rem(x + 2, NX)
    plus, minus = lax.rem(x + 1, NX), lax.rem(x + NX - 1, NX)
    source = core * NY + y
    fold = OUTR // 2

    def r_copy(i, b, h):
        return remote(
            rsend.at[i, b, h], rrecv.at[i, source], rs, rr.at[i], z * NY + b, x * NC + h
        )

    def attend(i, *blocks):
        queries, windows = [], []
        for b in blocks:
            xq = qrecv[b, pl.ds(pl.multiple_of(64 * lax.rem(i, 2), 64), 64), :].astype(F32)
            queries.append(jnp.where(low, jnp.where(i > 1, half_swap(xq), xq), 0.0).astype(BF16))
            row = 4 * b + i
            base = jnp.clip(row0 + row - 4, 0, LAST_START) - row0 + 4
            keys = pl.ds(pl.multiple_of(base * GRID_W, GRID_W), WIN)
            windows.append((keys, jnp.where(row < 4, row, jnp.where(row < 13, 4, row - 8))))
        sc_ctx = dot_nt(jnp.concatenate(queries, axis=0), ctxkv[...])
        sc_win = jnp.concatenate(
            [dot_nt(qp, kvext[keys, :]) + btab[t] for qp, (keys, t) in zip(queries, windows)],
            axis=0,
        )
        top = jnp.maximum(
            jnp.max(sc_ctx, axis=1, keepdims=True), jnp.max(sc_win, axis=1, keepdims=True)
        )
        e_ctx = jnp.exp(sc_ctx - top)
        e_win = jnp.exp(sc_win - top)
        den = jnp.sum(e_ctx, axis=1, keepdims=True) + jnp.sum(e_win, axis=1, keepdims=True)
        e_win = e_win.astype(BF16)
        o_all = dot(e_ctx.astype(BF16), ctxkv[...])
        for n, (b, (keys, t)) in enumerate(zip(blocks, windows)):
            part = slice(64 * n, 64 * n + 64)
            o = (o_all[part] + dot(e_win[part], kvext[keys, :])) * (1.0 / den[part])
            for h in range(NC):
                r0 = o[OUTR * h : OUTR * h + fold]
                r1 = o[OUTR * h + fold : OUTR * h + OUTR]
                rsend[i, b, h] = jnp.where(low, half_swap(r0), r1).astype(BF16)
        for b in blocks:
            for h in range(NC):
                here = (b == y) & (h == core)

                @pl.when(here)
                def _():
                    rrecv[i, source] = rsend[i, b, h]

                @pl.when(jnp.logical_not(here))
                def _():
                    r_copy(i, b, h).start()

    def gate(i, name, at):
        phase("r_wait_" + name)
        drain(rrecv.at[i, pl.ds(0, NC * NY - 1)], rr.at[i])
        phase("project_" + name)
        for part in range(2):
            src = (core if part == 0 else 1 - core) * NY
            for q in range(2):
                x0, x1 = rrecv[i, src + 2 * q].astype(F32), rrecv[i, src + 2 * q + 1].astype(F32)
                cols = slice(TOK * part + 128 * q, TOK * part + 128 * q + 128)
                up = jnp.where(low, x0, half_swap(x1)) * sgate[i, 0:fold, cols]
                dn = jnp.where(low, half_swap(x0), x1) * sgate[i, fold:OUTR, cols]
                gated[at : at + fold, cols] = up.astype(BF16)
                gated[at + fold : at + OUTR, cols] = dn.astype(BF16)

    def project(targets, at, *pieces):
        rows = slice(at, at + OUTR * len(targets))
        for n in pieces:
            cols = slice(512 * n, 512 * n + 512)
            term = dot(gated[rows, :TOK], wo[:, cols]) + dot(gated[rows, TOK:], wo2[:, cols])
            for m, i in enumerate(targets):
                psend[i, :, cols] = term[OUTR * m : OUTR * m + OUTR].astype(BF16)

    def to_neighbour(src, up, dst, sem):
        remote(src, dst, ps, sem, sp, (plus if up else minus) * NC + core).start()

    def send_across(*pieces):
        for n in pieces:
            src = psend.at[across, :, pl.ds(512 * n, 512)]
            to_neighbour(src, n < 2, hop.at[n], hp.at[n])

    def send_on(up, at, width):
        cols = pl.ds(at, width)
        src = psend.at[plus if up else minus, :, cols]
        to_neighbour(src, up, precv.at[0 if up else 1, :, cols], pr)

    attend(across, 1, 2)
    phase("h_wait")

    @pl.when(z > 0)
    def _():
        up_copy.wait_recv()

    @pl.when(z < NZ - 1)
    def _():
        dn_copy.wait_recv()

    phase("attention2")
    attend(across, 0, 3)
    phase("attention3")
    attend(plus, 0, 3, 1, 2)
    phase("attention4")
    attend(minus, 0, 3, 1, 2)
    phase("attention5")
    attend(x, 0, 3, 1, 2)
    w_copy.wait_recv()
    gate(across, "across", 0)
    project((across,), 0, 0, 2)
    send_across(0, 2)
    project((across,), 0, 1, 3)
    send_across(1, 3)
    gate(plus, "plus", OUTR)
    project((plus,), OUTR, 2, 3)
    send_on(True, D // 2, D // 2)
    gate(minus, "minus", 2 * OUTR)
    project((plus, minus), OUTR, 0, 1)
    send_on(False, 0, D // 2)

    def add_and_send(m, n):
        phase(f"hop{m}")
        cols = pl.ds(pl.multiple_of(512 * n, 512), 512)
        drain(hop.at[n], hp.at[n])
        up = n < 2
        to = jnp.where(up, plus, minus)
        psend[to, :, cols] = (psend[to, :, cols].astype(F32) + hop[n].astype(F32)).astype(BF16)
        dst = precv.at[jnp.where(up, 0, 1), :, cols]
        remote(psend.at[to, :, cols], dst, ps, pr, sp, to * NC + core).start()

    phase("rest")
    project((minus,), 2 * OUTR, 2, 3)
    for m, (inner, first, last) in enumerate(((0, 2, 0), (2, 3, 1), (1, 0, 2), (3, 1, 3))):
        add_and_send(m, jnp.where(x == 0, first, jnp.where(x == NX - 1, last, inner)))
    gate(x, "own", 0)
    project((x,), 0, 0, 1, 2, 3)

    phase("sent1")
    drain(zrecv.at[pl.ds(0, NZ - 1)], zs)
    drain(zgrecv.at[pl.ds(0, NZ - 1)], zgs)
    drain(mrecv.at[pl.ds(0, NY * NTP - 1)], ms)
    drain(mgrecv.at[pl.ds(0, NY * NTP - 1)], mgs)
    drain(mgrecv.at[pl.ds(0, NY * NTP - 1)], mgr)
    drain(ctxkv.at[pl.ds(0, CTX - NY * CTXL)], cs)
    drain(ctx.at[pl.ds(0, NY - 1), 0], xs)
    drain(ctx.at[pl.ds(0, NY - 1), 0], xps)
    drain(kvext.at[pl.ds(0, (NY - 1) * TOK)], ks)
    drain(qrecv.at[pl.ds(0, NY - 1)], qs)
    w_copy.wait_send()
    g_copy.wait_send()
    for i in range(NX):
        drain(rrecv.at[i, pl.ds(0, NC * NY - 1)], rs)

    @pl.when(z < NZ - 1)
    def _():
        up_copy.wait_send()

    @pl.when(z > 0)
    def _():
        dn_copy.wait_send()

    for t in range(NTP):
        total = mgrecv[t] + mgrecv[NTP + t] + mgrecv[2 * NTP + t] + mgrecv[3 * NTP + t]
        mod[4:5, 256 * t : 256 * t + 128] = total[0:1]
        mod[4:5, 256 * t + 128 : 256 * t + 256] = total[1:2]
    phase("p_wait")
    drain(precv, pr)
    phase("final")
    branch = psend[x].astype(F32) + precv[0].astype(F32) + precv[1].astype(F32)
    branch = branch.astype(BF16).astype(F32)
    normed = branch * lax.rsqrt(jnp.mean(branch * branch, axis=1, keepdims=True) + EPSILON)
    own = lat[pl.ds(pl.multiple_of(tp * OUTR, OUTR), OUTR), :].astype(F32)
    out_ref[...] = (own + mod[4:5, :] * (normed * mod[6:7, :])).astype(BF16)

    phase("sent")
    drain(psend.at[pl.ds(0, NX - 1)], ps)
    phase(None)


def shards(
    latent,
    context,
    condition,
    context_condition,
    gain_pre,
    gain_post,
    w_shift,
    w_scale,
    w_gate,
    w_query,
    w_key,
    w_value,
    w_silu,
    offset_bias,
    w_out,
):
    in_rows = w_shift.shape[0]
    vmem = pl.BlockSpec(memory_space=pltpu.VMEM)
    hbm = pl.BlockSpec(memory_space=pltpu.HBM)
    dma = pltpu.SemaphoreType.DMA
    operands = (
        condition.reshape(16, 128),
        context_condition.reshape(16, 128),
        gain_pre.reshape(16, 128),
        gain_post.reshape(16, 128),
        jnp.transpose(offset_bias, (1, 0, 2)),
        latent,
        context,
        w_shift,
        w_scale,
        w_gate,
        w_query,
        w_key,
        w_value,
        w_silu,
        w_out,
    )
    operands = [pltpu.with_memory_space_constraint(a, pltpu.HBM) for a in operands]
    return pl.pallas_call(
        kernel,
        name="whole",
        out_shape=jax.ShapeDtypeStruct((OUTR, D), BF16),
        in_specs=[hbm] * 15,
        out_specs=vmem,
        scratch_shapes=[
            pltpu.VMEM((2, 16, 128), BF16),
            pltpu.VMEM((2, 16, 128), F32),
            pltpu.VMEM((2, 16, 128), F32),
            pltpu.VMEM((2 * WIN_ROWS - 1, NY, 2 * WIN_COLS - 1), F32),
            pltpu.VMEM((16, 128), F32),
            pltpu.VMEM((3, in_rows, TOK), BF16),
            pltpu.VMEM((TOK, D), BF16),
            pltpu.VMEM((NY, NC, CTXL // NC, D), BF16),
            pltpu.VMEM((D, 2 * TOK), BF16),
            pltpu.VMEM((D, 128), BF16),
            pltpu.VMEM((D, 2 * TOK), BF16),
            pltpu.VMEM((TOK, D), BF16),
            pltpu.VMEM((TOK, D), BF16),
            pltpu.VMEM((8, 128), F32),
            pltpu.VMEM((NZ, 8, 128), F32),
            pltpu.VMEM((8, 128), F32),
            pltpu.VMEM((NY * NTP, 8, 128), F32),
            pltpu.VMEM((2, 128), F32),
            pltpu.VMEM((NZ, 2, 128), F32),
            pltpu.VMEM((2, 128), F32),
            pltpu.VMEM((NY * NTP, 2, 128), F32),
            pltpu.VMEM((8, D), F32),
            pltpu.VMEM((4, 8, D), F32),
            pltpu.VMEM((TABLES, GRID_W, WIN), F32),
            pltpu.VMEM((TOK, D), BF16),
            pltpu.VMEM((NY * CTXL, D), BF16),
            pltpu.VMEM((TOK, 128), F32),
            pltpu.VMEM((NY * CTXL, 128), F32),
            pltpu.VMEM((CTX, 128), BF16),
            pltpu.VMEM((NY, TOK, 128), BF16),
            pltpu.VMEM((6 * TOK, 128), BF16),
            pltpu.VMEM((NY, 128, 128), BF16),
            pltpu.VMEM((NY, 128, 128), BF16),
            pltpu.VMEM((NX, NC, OUTR, TOK), BF16),
            pltpu.VMEM((NX, OUTR, TOK), BF16),
            pltpu.VMEM((NX, OUTR, NC * TOK), F32),
            pltpu.VMEM((NX, NY, NC, OUTR // 2, 128), BF16),
            pltpu.VMEM((NX, NC * NY, OUTR // 2, 128), BF16),
            pltpu.VMEM((3 * OUTR, NC * TOK), BF16),
            pltpu.VMEM((NX, OUTR, D), BF16),
            pltpu.VMEM((4, OUTR, D // 4), BF16),
            pltpu.VMEM((2, OUTR, D), BF16),
            dma((9,)),
            dma,
            dma,
            dma,
            dma,
            dma,
            dma,
            dma,
            dma,
            dma,
            dma,
            dma,
            dma,
            dma,
            dma,
            dma,
            dma,
            dma,
            dma((NY,)),
            dma,
            dma,
            dma((2,)),
            dma((2,)),
            dma,
            dma((NX,)),
            dma,
            dma,
            dma((4,)),
            dma,
            dma,
        ],
        compiler_params=pltpu.CompilerParams(
            collective_id=0, has_side_effects=True, vmem_limit_bytes=48 << 20
        ),
    )(*operands)


def solution(mesh):
    in_specs = (
        P("sp", None),
        P("sp", None),
        P(),
        P(),
        P(),
        P(),
        P("sp", "tp"),
        P("sp", "tp"),
        P("sp", "tp"),
        P(None, "tp"),
        P(None, "tp"),
        P(None, "tp"),
        P(None, "tp"),
        P("tp", None, None),
        P("tp", None),
    )
    out_specs = P(("sp", "tp"), None)
    return jax.shard_map(shards, mesh=mesh, in_specs=in_specs, out_specs=out_specs, check_vma=False)
```
